32 devices in a mesh: ep: 16 (over z, y, x), tp: 2 (over core).
Axes of the slice: x: 2, y: 2, z: 4, core: 2. Of those that a mesh axis runs over, the one named last changes fastest.
Arguments:
- tokens: bfloat16 [512, 2048], P('ep', 'tp')
- norm1_gain: float32 [2048], P('tp'), may hold values from 0.1 to 1.9
- w_query: bfloat16 [2048, 1024], P('tp'), may hold values from -0.125 to 0.125
- w_key: bfloat16 [2048, 128], P('tp'), may hold values from -0.125 to 0.125
- w_value: bfloat16 [2048, 128], P('tp'), may hold values from -0.125 to 0.125
- head_bias: float32 [16], P('tp'), may hold values from -7 to -1.5
- key_cache: bfloat16 [512, 1024, 128], P('ep', None, 'tp'), may hold values from -6 to 6
- value_cache: bfloat16 [512, 1024, 128], P('ep', None, 'tp'), may hold values from -6 to 6
- seq_lengths: int32 [512], P('ep'), may hold values from 1 to 1024, as said below
- w_out: bfloat16 [1024, 2048], P('tp'), may hold values from -0.375 to 0.375
- norm2_gain: float32 [2048], P('tp'), may hold values from 0.5 to 8
- route_ids: int32 [512, 4], P('ep'), may hold values from 0 to 15, all different within a row; in each aligned block of 32 rows (0 to 31, 32 to 63, ...) at most 16 rows name the same one
- route_logits: float32 [512, 4], P('ep'), may hold values from -6 to 6
- expert_gate: bfloat16 [16, 2048, 2048], P('ep', None, 'tp'), may hold values from -0.125 to 0.125
- expert_up: bfloat16 [16, 2048, 2048], P('ep', None, 'tp'), may hold values from -0.125 to 0.125
- expert_down: bfloat16 [16, 2048, 2048], P('ep', 'tp'), may hold values from -0.125 to 0.125
Outputs:
- mixed_out: bfloat16 [512, 2048], P('ep', 'tp')
- new_key: bfloat16 [512, 128], P('ep', 'tp')
- new_value: bfloat16 [512, 128], P('ep', 'tp')
The draws below stay inside these ranges and needn't reach their ends.
Inputs may be any that keep to these rules, and one draw needn't show every extreme that they name: A sequence attends to its first seq_lengths cache positions; in every draw some sequence has exactly 1024. `route_ids`: each row names 4 different experts. Among the rows of one device no expert is named more than 16 times, and in every draw some expert is named exactly 16 times by some device's rows.
All inputs are finite; a program needn't handle non-finite values.
Results may differ from the reference program's by a relative error of at most 0.028.
Values may be sent and summed in bfloat16 or wider, within the bound.
A program may use at most 128 MiB of HBM per device.

```python
import math
import jax
import jax.numpy as jnp
import numpy as np
from jax import lax

D = 2048
HEAD = 64
Q_HEADS = 16
KV_HEADS = 2
FF = 2048
TOPK = 4
MAXLEN = 1024
SEQ_DEV = 32
QW = 1024
KV_W = 128
EXPERTS = 16
TOKENS = 512
CAP = 16
N_EP = 16
N_TP = 2


def draw_tokens(key, part):
    keys = jax.random.split(jax.random.fold_in(key, 11), 3)
    base = jax.random.normal(keys[0], (TOKENS, D), jnp.float32)
    ramp = 3.0 ** (jnp.arange(D, dtype=jnp.float32) / (D - 1)) / jnp.sqrt(3.0)
    rough = jnp.exp(jax.random.uniform(keys[1], (D,), jnp.float32, -0.5, 0.5))
    row_scale = jnp.exp(jax.random.uniform(keys[2], (TOKENS, 1), jnp.float32, -1.15, 1.15))
    return (base * ramp * rough * row_scale).astype(jnp.bfloat16)


def draw_seq_lengths(key, part):
    keys = jax.random.split(jax.random.fold_in(key, 23), 2)
    lengths = jax.random.randint(keys[0], (TOKENS,), 1, MAXLEN + 1, dtype=jnp.int32)
    chosen = jax.random.randint(keys[1], (), 0, TOKENS, dtype=jnp.int32)
    return jnp.where(jnp.arange(TOKENS, dtype=jnp.int32) == chosen, MAXLEN, lengths).astype(jnp.int32)


def block_levels(key, dims, shards, smallest, largest):
    loudness = 1.0
    for position, blocks in shards:
        draws = jax.random.uniform(jax.random.fold_in(jax.random.fold_in(key, 6), position), (blocks,), jnp.float32, smallest / len(shards), largest / len(shards))
        loudness = loudness * jnp.repeat(jnp.exp(draws), dims[position] // blocks).reshape((-1,) + (1,) * (len(dims) - 1 - position))
    return loudness


def deal_out(own_key, own, number, rows, number_of, top, limit, lean):
    ranking = jax.random.permutation(own_key, number_of)
    packed, usual = portions_of(number_of, rows * top, limit, lean, True), portions_of(number_of, rows * top, limit, lean, False)
    places = jnp.arange(number_of)

    def named(sizes, turn):
        used = int((sizes > 0).sum())
        fixed = max(1, used // 4)
        moved = fixed + (places - fixed + turn * (used - fixed)) % max(1, number_of - fixed)
        return jnp.zeros((number_of,), jnp.int32).at[ranking[jnp.where(places < fixed, places, moved)]].set(jnp.asarray(sizes, jnp.int32))

    sizes = jnp.where(number % 4 == 0, named(packed, number // 4), named(usual, number - number // 4 - 1))
    mixed = jax.random.permutation(jax.random.fold_in(own, 3), number_of)
    giver, taker = mixed[0:number_of // 2 * 2:2], mixed[1:number_of // 2 * 2:2]
    room = jnp.minimum(sizes[giver] - 1, limit - sizes[taker]) // 2
    room = jnp.where((giver == ranking[0]) | (taker == ranking[0]) | (sizes[taker] == 0), 0, jnp.maximum(room, 0))
    moved = jax.random.randint(jax.random.fold_in(own, 4), (number_of // 2,), 0, 1 << 20) % (room + 1)
    sizes = sizes.at[giver].add(-moved).at[taker].add(moved)
    labels = jnp.searchsorted(jnp.cumsum(sizes), jnp.arange(rows * top), side="right").astype(jnp.int32)
    grid = labels.reshape(top, rows).T
    grid = grid[jax.random.permutation(jax.random.fold_in(own, 1), rows)]
    turn = jax.random.randint(jax.random.fold_in(own, 2), (rows, 1), 0, top)
    return jnp.take_along_axis(grid, (jnp.arange(top)[None, :] + turn) % top, axis=1)


def portions_of(count, total, bound, lean, full):
    weights = [(1 << 20) // math.isqrt(standing ** lean) + 1 for standing in range(1, count + 1)]
    largest = bound if full else min(bound, max(-(-total // count), total * weights[0] // sum(weights)))
    least = 1 if total - largest >= count - 1 else 0
    holding, spare = [largest] + [least] * (count - 1), total - largest - least * (count - 1)
    while spare > 0:
        candidates = [i for i in range(1, count) if holding[i] < largest] or [i for i in range(1, count) if holding[i] < bound]
        mass, remaining = sum([weights[i] for i in candidates]), spare
        for i in candidates:
            more = min(bound - holding[i], max(1, remaining * weights[i] // mass), spare)
            holding[i] = holding[i] + more
            spare = spare - more
    return np.array(holding)


def noise(stream_key, extent, scale, reach, shards=(), kind=jnp.bfloat16):
    result = jax.random.normal(stream_key, extent, jnp.float32) * scale
    if len(shards) > 0:
        result = block_levels(stream_key, extent, shards, -0.22, 0.18) * result
    return jnp.clip(result, min=-reach, max=reach).astype(kind)


def setup_inputs(seed: int = 0) -> dict:
    seeds = jax.random.split(jax.random.key(seed), 17)
    tokens = draw_tokens(jax.random.fold_in(seeds[16], 71), 0)
    norm1_gain = jnp.clip(1.0 + 0.18 * jax.random.normal(seeds[1], (D,), jnp.float32), 0.1, 1.9)
    w_query = noise(seeds[2], (D, QW), D ** -0.5, 0.125, ((0, 2),))
    w_key = noise(seeds[3], (D, KV_W), D ** -0.5, 0.125, ((0, 2),))
    w_value = noise(seeds[4], (D, KV_W), D ** -0.5, 0.125, ((0, 2),))
    head_bias = jnp.clip(-7.0 + 5.5 * jax.random.uniform(seeds[5], (Q_HEADS,), jnp.float32) ** block_levels(seeds[5], (Q_HEADS,), ((0, 2),), -0.2, 0.2), -7.0, -1.5)
    key_cache = noise(seeds[6], (TOKENS, MAXLEN, KV_W), 1.0, 6.0, ((0, 16), (2, 2)))
    value_cache = noise(seeds[7], (TOKENS, MAXLEN, KV_W), 1.0, 6.0, ((0, 16), (2, 2)))
    seq_lengths = draw_seq_lengths(jax.random.fold_in(seeds[16], 71), 0)
    w_out = noise(seeds[9], (QW, D), (QW // 4) ** -0.5, 0.375, ((0, 2),))
    norm2_gain = jnp.clip(jnp.exp(math.log(8.0) - 2.7725887 * jax.random.uniform(seeds[10], (D,), jnp.float32) ** block_levels(seeds[10], (D,), ((0, 2),), -0.2, 0.2)), 0.5, 8.0)
    route_ids_keys = jax.random.split(jax.random.fold_in(seeds[11], 1), TOKENS // SEQ_DEV)
    route_ids_turns = jax.random.permutation(jax.random.fold_in(seeds[11], 3), TOKENS // SEQ_DEV)
    route_ids = jax.vmap(lambda own, number: deal_out(jax.random.fold_in(seeds[11], 2), own, number, SEQ_DEV, EXPERTS, TOPK, CAP, 2))(route_ids_keys, route_ids_turns).reshape((TOKENS, TOPK))
    route_logits = noise(seeds[12], (TOKENS, TOPK), 1.0, 6.0, ((0, 16),), jnp.float32)
    expert_gate = noise(seeds[13], (EXPERTS, D, FF), D ** -0.5, 0.125, ((0, 16), (2, 2)))
    expert_up = noise(seeds[14], (EXPERTS, D, FF), D ** -0.5, 0.125, ((0, 16), (2, 2)))
    expert_down = noise(seeds[15], (EXPERTS, FF, D), FF ** -0.5, 0.125, ((0, 16), (1, 2)))
    return {"tokens": tokens, "norm1_gain": norm1_gain, "w_query": w_query, "w_key": w_key, "w_value": w_value, "head_bias": head_bias, "key_cache": key_cache, "value_cache": value_cache, "seq_lengths": seq_lengths, "w_out": w_out, "norm2_gain": norm2_gain, "route_ids": route_ids, "route_logits": route_logits, "expert_gate": expert_gate, "expert_up": expert_up, "expert_down": expert_down}


LN_EPS = 1e-05
SWIGLU_ALPHA = 1.702
SWIGLU_LIMIT = 7.0

def layer_norm(values, norm_gain):
    widened = values.astype(jnp.float32)
    columns = values.shape[-1]
    average = lax.optimization_barrier(jnp.sum(widened, axis=-1, keepdims=True)) / columns
    spread = lax.optimization_barrier(jnp.sum(widened * widened, axis=-1, keepdims=True)) / columns - average * average
    return (widened - average) * lax.rsqrt(spread + LN_EPS) * norm_gain

def stick_read(query_block, key_block, value_block, length_block, head_bias):
    sequences = query_block.shape[0]
    positions = key_block.shape[1]
    kv_heads = key_block.shape[2]
    head_size = key_block.shape[3]
    grouped = query_block.reshape(sequences, kv_heads, -1, head_size)
    scores = jnp.einsum('bkgd,blkd->bkgl', grouped.astype(jnp.float32), key_block.astype(jnp.float32)) * head_size ** (-0.5)
    scores = scores + head_bias.reshape(kv_heads, -1)[None, :, :, None]
    live_mask = (lax.broadcasted_iota(jnp.int32, (sequences, positions), 1) < length_block[:, None])[:, None, None, :]
    spent_log = jnp.where(live_mask, jax.nn.softplus(scores), 0.0)
    tail_sum = lax.cumsum(spent_log, axis=3, reverse=True) - spent_log
    weights = jnp.where(live_mask, jnp.exp(jax.nn.log_sigmoid(scores) - tail_sum), 0.0).astype(jnp.bfloat16)
    mixture = jnp.einsum('bkgl,blkd->bkgd', weights.astype(jnp.float32), value_block.astype(jnp.float32))
    return mixture.astype(jnp.bfloat16).reshape(sequences, -1)

def expert_rows(rows_in, gate_weight, up_weight, down_weight):
    gate_pre = jnp.dot(rows_in, gate_weight, preferred_element_type=jnp.float32)
    up_pre = jnp.dot(rows_in, up_weight, preferred_element_type=jnp.float32)
    clipped = jnp.minimum(gate_pre, SWIGLU_LIMIT)
    linear = jnp.clip(up_pre, -SWIGLU_LIMIT, SWIGLU_LIMIT)
    activated = (clipped * jax.nn.sigmoid(SWIGLU_ALPHA * clipped) * (linear + 1.0)).astype(jnp.bfloat16)
    hidden_cols = FF // N_TP
    running = jnp.zeros((rows_in.shape[0], D), jnp.float32)
    for portion in range(N_TP):
        partial_value = jnp.dot(activated[:, portion * hidden_cols:(portion + 1) * hidden_cols], down_weight[portion * hidden_cols:(portion + 1) * hidden_cols], preferred_element_type=jnp.float32)
        running = running + lax.optimization_barrier(partial_value.astype(jnp.bfloat16)).astype(jnp.float32)
    return running.astype(jnp.bfloat16)

def slots_of(ids_block):
    flat_ids = ids_block.reshape(-1)
    expert_hot = (flat_ids[:, None] == jnp.arange(EXPERTS, dtype=jnp.int32)[None, :]).astype(jnp.int32)
    earlier = jnp.cumsum(expert_hot, axis=0, dtype=jnp.int32) - expert_hot
    return flat_ids * CAP + lax.optimization_barrier(jnp.sum(earlier * expert_hot, axis=1, dtype=jnp.int32))

def reference(tokens, norm1_gain, w_query, w_key, w_value, head_bias, key_cache, value_cache, seq_lengths, w_out, norm2_gain, route_ids, route_logits, expert_gate, expert_up, expert_down):
    normed = layer_norm(tokens, norm1_gain).astype(jnp.bfloat16)
    query_rows = jnp.dot(normed, w_query, preferred_element_type=jnp.float32).astype(jnp.bfloat16)
    new_key = jnp.dot(normed, w_key, preferred_element_type=jnp.float32).astype(jnp.bfloat16)
    new_value = jnp.dot(normed, w_value, preferred_element_type=jnp.float32).astype(jnp.bfloat16)

    def read_block(items):
        return stick_read(items[0], items[1], items[2], items[3], head_bias)
    attended = lax.map(read_block, (query_rows.reshape(N_EP, SEQ_DEV, QW), key_cache.reshape(N_EP, SEQ_DEV, MAXLEN, KV_HEADS, HEAD), value_cache.reshape(N_EP, SEQ_DEV, MAXLEN, KV_HEADS, HEAD), seq_lengths.reshape(N_EP, SEQ_DEV)))
    attended = attended.reshape(TOKENS, QW)
    head_cols = QW // N_TP
    branch = jnp.zeros((TOKENS, D), jnp.float32)
    for portion in range(N_TP):
        partial_value = jnp.dot(attended[:, portion * head_cols:(portion + 1) * head_cols], w_out[portion * head_cols:(portion + 1) * head_cols], preferred_element_type=jnp.float32)
        branch = branch + lax.optimization_barrier(partial_value.astype(jnp.bfloat16)).astype(jnp.float32)
    residual = (tokens.astype(jnp.float32) + branch).astype(jnp.bfloat16)
    normed_two = layer_norm(residual, norm2_gain).astype(jnp.bfloat16)
    targets = jax.vmap(slots_of)(route_ids.reshape(N_EP, SEQ_DEV, TOPK))
    sources = jnp.repeat(normed_two.reshape(N_EP, SEQ_DEV, D), TOPK, axis=1)
    device_ids = jnp.arange(N_EP, dtype=jnp.int32)[:, None]
    dispatch = jnp.zeros((N_EP, EXPERTS * CAP, D), jnp.bfloat16).at[device_ids, targets].set(sources)
    by_expert = dispatch.reshape(N_EP, EXPERTS, CAP, D).transpose(1, 0, 2, 3).reshape(EXPERTS, N_EP * CAP, D)

    def run_one(items):
        return expert_rows(items[0], items[1], items[2], items[3])
    results = lax.map(run_one, (by_expert, expert_gate, expert_up, expert_down))
    by_source = results.reshape(EXPERTS, N_EP, CAP, D).transpose(1, 0, 2, 3).reshape(N_EP, EXPERTS * CAP, D)
    picked = by_source[device_ids, targets].reshape(TOKENS, TOPK, D).astype(jnp.float32)
    exp_logits = jnp.exp(route_logits)
    route_probs = exp_logits / lax.optimization_barrier(jnp.sum(exp_logits, axis=1, keepdims=True))
    moe_out = lax.optimization_barrier(jnp.sum(route_probs[:, :, None] * picked, axis=1))
    mixed_out = (residual.astype(jnp.float32) + moe_out).astype(jnp.bfloat16)
    return (mixed_out, new_key, new_value)
```

```python
import functools

import jax
import jax.numpy as jnp
from jax import lax
from jax.experimental import pallas as pl
from jax.experimental.pallas import tpu as pltpu
from jax.sharding import PartitionSpec as P

HEAD = 64
LN_EPS = 1e-05
SWIGLU_ALPHA = 1.702
SWIGLU_LIMIT = 7.0
MESH = pl.DeviceIdType.MESH
F32 = jnp.float32
BF16 = jnp.bfloat16
DEAD = -1e30
POS_BLOCK = 256
COL_BLOCK = 256
GATE_BLOCK = 512
PAD = 16
VMEM_BYTES = 63 * 1024 * 1024
LANES = 128


def dot(a, b):
    return jnp.dot(a, b, preferred_element_type=F32)


def kernel(
    n,
    cap,
    tok_hbm,
    g1_hbm,
    wq_hbm,
    wk_hbm,
    wv_hbm,
    bias_ref,
    kc_hbm,
    vc_hbm,
    lens_ref,
    wo_hbm,
    g2_hbm,
    ids_hbm,
    logits_hbm,
    gate_hbm,
    up_hbm,
    down_hbm,
    out_ref,
    nk_ref,
    nv_ref,
    x_own,
    x_peer,
    g1,
    wq,
    wk,
    wv,
    kc,
    vc,
    wo,
    g2,
    ids,
    logits,
    gate,
    up,
    down,
    proj_send,
    proj_recv,
    q_rows,
    z_ref,
    att_ref,
    part_send,
    part_recv,
    res_ref,
    tables_send,
    tables_recv,
    rows_ref,
    rows_recv,
    disp,
    recv_own,
    recv_peer,
    gate_acc,
    up_acc,
    act_ref,
    down_send,
    down_recv,
    down_own,
    back_send,
    back_recv,
    sum_send,
    sum_recv,
    load_sem,
    one_send,
    one_recv,
    table_send_sem,
    table_recv_sem,
    rows_send_sem,
    rows_recv_sem,
    sum_send_sem,
    sum_recv_sem,
    disp_send_sem,
    disp_recv_sem,
    fwd_send_sem,
    fwd_recv_sem,
    down_send_sem,
    down_recv_sem,
    back_send_sem,
    back_recv_sem,
    local_sem,
):
    ep = lax.axis_index("ep")
    tp = lax.axis_index("tp")
    other = 1 - tp
    seqs, half = x_own.shape
    width = 2 * half
    slots = n * cap

    loads = []
    pairs = (
        (tok_hbm, x_own),
        (g1_hbm, g1),
        (wq_hbm, wq),
        (wk_hbm, wk),
        (wv_hbm, wv),
        (kc_hbm, kc),
        (vc_hbm, vc),
        (wo_hbm, wo),
        (g2_hbm, g2),
        (ids_hbm, ids),
        (logits_hbm, logits),
        (gate_hbm, gate),
        (up_hbm, up),
        (down_hbm, down),
    )
    for i, (src, dst) in enumerate(pairs):
        copy = pltpu.make_async_copy(src, dst, load_sem.at[i])
        loads.append(copy)
    for i in (0, 2, 3, 4, 1, 9, 10, 8):
        loads[i].start()

    def peer_copy(src, dst, i):
        return pltpu.make_async_remote_copy(
            src_ref=src,
            dst_ref=dst,
            send_sem=one_send.at[i],
            recv_sem=one_recv.at[i],
            device_id=(ep, other),
            device_id_type=MESH,
        )

    barrier = pltpu.get_barrier_semaphore()
    pl.semaphore_signal(barrier, inc=1, device_id=(ep, other), device_id_type=MESH)

    planes = tables_send.shape[0]
    plane = n // planes
    level = ep // plane
    spot = ep % plane

    def column(i):
        return lax.rem(level + i, planes) * plane + spot

    def beside(i):
        return level * plane + lax.rem(spot + i, plane)

    if planes == 4:
        inner = lax.rem((level + 1) // 2, 2)
        over = lax.rem(level + 2, 4)
        across = 3 - level
        partners = (
            level,
            level + 1 - 2 * lax.rem(level, 2),
            inner * across + (1 - inner) * over,
            inner * over + (1 - inner) * across,
        )
    else:
        partners = (level,)

    def greet_column(i, carry):
        pl.semaphore_signal(barrier, inc=1, device_id=(column(i), tp), device_id_type=MESH)
        return carry

    def greet_beside(i, carry):
        pl.semaphore_signal(barrier, inc=1, device_id=(beside(i), tp), device_id_type=MESH)
        return carry

    lax.fori_loop(1, planes, greet_column, 0)
    lax.fori_loop(1, plane, greet_beside, 0)
    for i in (0, 1, 2, 3, 4):
        loads[i].wait()
    for i in (5, 6, 7):
        loads[i].start()
    mine = x_own[...].astype(F32)
    mean_own = jnp.sum(mine, axis=1, keepdims=True) / half
    centred = mine - mean_own
    square_own = jnp.sum(centred * centred, axis=1, keepdims=True)
    gain = g1[...]
    gain_hi = gain.astype(BF16)
    gain_lo = (gain - gain_hi.astype(F32)).astype(BF16)
    pad_row = lax.broadcasted_iota(jnp.int32, (PAD, half), 0)
    gains = jnp.where(
        pad_row == 0, gain_hi.astype(F32), jnp.where(pad_row == 1, gain_lo.astype(F32), 0.0)
    )
    stacked = jnp.concatenate([centred * gain, gains], axis=0).astype(BF16)
    pq = dot(stacked, wq[...])
    pk = dot(stacked, wk[...])
    pv = dot(stacked, wv[...])
    qc = pq.shape[1] // 2
    kcols = pk.shape[1] // 2
    first = tp == 0
    used = qc + 2 * kcols
    proj_send[:, :qc] = jnp.where(first, pq[:, qc:], pq[:, :qc])
    proj_send[:, qc : qc + kcols] = jnp.where(first, pk[:, kcols:], pk[:, :kcols])
    proj_send[:, qc + kcols : used] = jnp.where(first, pv[:, kcols:], pv[:, :kcols])
    proj_send[:seqs, used : used + LANES] = jnp.broadcast_to(mean_own, (seqs, LANES))
    proj_send[:seqs, used + LANES :] = jnp.broadcast_to(square_own, (seqs, LANES))
    pl.semaphore_wait(barrier, planes + plane - 1)

    proj_copy = peer_copy(proj_send, proj_recv, 1)
    proj_copy.start()
    tok_copy = peer_copy(x_own, x_peer, 0)
    tok_copy.start()

    def stats(a, b):
        total = jnp.sum(a, axis=1, keepdims=True) + jnp.sum(b, axis=1, keepdims=True)
        square = jnp.sum(a * a, axis=1, keepdims=True) + jnp.sum(b * b, axis=1, keepdims=True)
        mean = total / width
        return mean, lax.rsqrt(square / width - mean * mean + LN_EPS)

    for i in (11, 12, 13):
        loads[i].start()
    loads[9].wait()
    loads[10].wait()
    top = ids.shape[0]
    slot_row = lax.broadcasted_iota(jnp.int32, (slots, seqs), 0)
    slot_expert = slot_row // cap
    slot_rank = slot_row - slot_expert * cap
    id_rows = ids[...]
    raw = jnp.exp(logits[...])
    probs = raw / jnp.sum(raw, axis=0, keepdims=True)
    hot = jnp.zeros((slots, seqs), F32)
    prob_hot = jnp.zeros((slots, seqs), F32)
    for k in range(top):
        match = id_rows[k : k + 1, :] == slot_expert
        hot = hot + jnp.where(match, 1.0, 0.0)
        prob_hot = prob_hot + jnp.where(match, probs[k : k + 1, :], 0.0)
    earlier = (
        lax.broadcasted_iota(jnp.int32, (seqs, seqs), 0)
        < lax.broadcasted_iota(jnp.int32, (seqs, seqs), 1)
    )
    rank = dot(hot.astype(BF16), jnp.where(earlier, 1.0, 0.0).astype(BF16))
    chosen = (hot > 0.5) & (jnp.abs(rank - slot_rank.astype(F32)) < 0.5)
    placing = jnp.where(chosen, 1.0, 0.0).astype(BF16)
    weight = jnp.where(chosen, prob_hot, 0.0)
    weight_hi = weight.astype(BF16)
    weight_lo = (weight - weight_hi.astype(F32)).astype(BF16)
    group = plane * cap
    for q in range(planes):
        at = slice(q * group, (q + 1) * group)
        tables_send[q, 0] = placing[at]
        tables_send[q, 1] = weight_hi[at]
        tables_send[q, 2] = weight_lo[at]

    groups = qc // HEAD
    bias = jnp.zeros((groups, 1), F32)
    head_row = lax.broadcasted_iota(jnp.int32, (groups, 1), 0)
    for h in range(groups):
        bias = bias + jnp.where(head_row == h, bias_ref[h], 0.0)

    own_q = jnp.where(first, pq[:, :qc], pq[:, qc:])
    own_k = jnp.where(first, pk[:, :kcols], pk[:, kcols:])
    own_v = jnp.where(first, pv[:, :kcols], pv[:, kcols:])
    proj_copy.wait()
    mean_peer = proj_recv[:seqs, used : used + 1]
    square_peer = proj_recv[:seqs, used + LANES : used + LANES + 1]
    apart = (mean_own - mean_peer) * 0.5
    scale = lax.rsqrt((square_own + square_peer) / width + apart * apart + LN_EPS)

    def joined(own, lo, hi):
        tilt = (own[seqs : seqs + 1] + own[seqs + 1 : seqs + 2]) - (
            proj_recv[seqs : seqs + 1, lo:hi] + proj_recv[seqs + 1 : seqs + 2, lo:hi]
        )
        return (scale * (own[:seqs] + proj_recv[:seqs, lo:hi] + apart * tilt)).astype(BF16)

    query = joined(own_q, 0, qc).astype(F32)
    nk_ref[...] = joined(own_k, qc, qc + kcols)
    nv_ref[...] = joined(own_v, qc + kcols, used)
    for h in range(groups):
        q_rows[:, h, :] = query[:, h * HEAD : (h + 1) * HEAD]

    def to_level(src, dst, sends, recvs, i):
        to = partners[i]
        return pltpu.make_async_remote_copy(
            src_ref=src.at[to],
            dst_ref=dst.at[level],
            send_sem=sends.at[to],
            recv_sem=recvs.at[level],
            device_id=(to * plane + spot, tp),
            device_id_type=MESH,
        )

    def from_level(src, dst, sends, recvs, i):
        source = partners[i]
        return pltpu.make_async_remote_copy(
            src_ref=src.at[source],
            dst_ref=dst.at[source],
            send_sem=sends.at[source],
            recv_sem=recvs.at[source],
            device_id=(source * plane + spot, tp),
            device_id_type=MESH,
        )

    table_args = (tables_send, tables_recv, table_send_sem, table_recv_sem)
    for i in range(1, planes):
        to_level(*table_args, i).start()
    tables_recv[level] = tables_send[level]

    positions = kc.shape[2]
    loads[5].wait()
    place = lax.broadcasted_iota(jnp.int32, (groups, positions), 1)

    def score_step(i, carry):
        for j in range(4):
            b = i * 4 + j
            s = dot(q_rows[b].astype(BF16), kc[b]) * HEAD ** (-0.5) + bias
            z_ref[pl.ds(pl.multiple_of(b * groups, groups), groups), :] = jnp.where(
                place < lens_ref[b], s, DEAD
            )
        return carry

    lax.fori_loop(0, seqs // 4, score_step, 0)

    after = (
        lax.broadcasted_iota(jnp.int32, (POS_BLOCK, POS_BLOCK), 0)
        > lax.broadcasted_iota(jnp.int32, (POS_BLOCK, POS_BLOCK), 1)
    )
    after = jnp.where(after, 1.0, 0.0).astype(BF16)
    row_block = 64

    def break_step(i, carry):
        rows = pl.ds(pl.multiple_of(i * row_block, row_block), row_block)
        beyond = jnp.zeros((row_block, 1), F32)
        for c in reversed(range(positions // POS_BLOCK)):
            cols = slice(c * POS_BLOCK, (c + 1) * POS_BLOCK)
            z = z_ref[rows, cols]
            tail = jnp.log1p(jnp.exp(-jnp.abs(z)))
            spent = jnp.maximum(z, 0.0) + tail
            hi = spent.astype(BF16)
            lo = (spent - hi.astype(F32)).astype(BF16)
            sums = dot(jnp.concatenate([hi, lo], axis=0), after)
            inside = sums[:row_block] + sums[row_block:]
            z_ref[rows, cols] = jnp.exp(jnp.minimum(z, 0.0) - tail - (inside + beyond))
            beyond = beyond + inside[:, :1] + spent[:, :1]
        return carry

    lax.fori_loop(0, seqs * groups // row_block, break_step, 0)

    loads[6].wait()

    def read_step(i, carry):
        rows = pl.ds(pl.multiple_of(i * 4 * groups, 4 * groups), 4 * groups)
        weights = z_ref[rows, :].astype(BF16)
        values = vc[pl.ds(i * 4, 4)].reshape(4 * HEAD, positions)
        mixed = lax.dot_general(
            weights, values, (((1,), (1,)), ((), ())), preferred_element_type=F32
        )
        for j in range(4):
            att_ref[i * 4 + j] = mixed[
                j * groups : (j + 1) * groups, j * HEAD : (j + 1) * HEAD
            ]
        return carry

    lax.fori_loop(0, seqs // 4, read_step, 0)
    attended = jnp.concatenate([att_ref[:, h, :] for h in range(groups)], axis=1).astype(BF16)

    loads[7].wait()
    part = dot(attended, wo[...]).astype(BF16)
    part_send[0] = part[:, :half]
    part_send[1] = part[:, half:]
    part_copy = peer_copy(part_send, part_recv, 2)
    part_copy.start()
    loads[8].wait()
    tok_copy.wait()
    part_copy.wait()
    mine = x_own[...].astype(F32)
    theirs = x_peer[...].astype(F32)
    res_own = (mine + (part_send[tp].astype(F32) + part_recv[tp].astype(F32))).astype(BF16)
    res_other = (
        theirs + (part_send[other].astype(F32) + part_recv[other].astype(F32))
    ).astype(BF16)
    res_ref[...] = res_own
    mine = res_own.astype(F32)
    mean, scale = stats(mine, res_other.astype(F32))
    normed_two = ((mine - mean) * scale * g2[...]).astype(BF16)
    rows_ref[...] = normed_two

    def rows_copy(i):
        to = partners[i]
        return pltpu.make_async_remote_copy(
            src_ref=rows_ref,
            dst_ref=rows_recv.at[level],
            send_sem=rows_send_sem.at[to],
            recv_sem=rows_recv_sem.at[level],
            device_id=(to * plane + spot, tp),
            device_id_type=MESH,
        )

    def rows_arrival(i):
        source = partners[i]
        return pltpu.make_async_remote_copy(
            src_ref=rows_ref,
            dst_ref=rows_recv.at[source],
            send_sem=rows_send_sem.at[source],
            recv_sem=rows_recv_sem.at[source],
            device_id=(source * plane + spot, tp),
            device_id_type=MESH,
        )

    def beside_copy(src, dst, sends, recvs, i, j):
        source = partners[i]
        to = lax.rem(spot + j, plane)
        return pltpu.make_async_remote_copy(
            src_ref=src.at[source, to],
            dst_ref=dst.at[source, spot],
            send_sem=sends.at[i, j],
            recv_sem=recvs.at[i, j],
            device_id=(level * plane + to, tp),
            device_id_type=MESH,
        )

    def beside_arrival(src, dst, sends, recvs, i, j):
        source = partners[i]
        giver = lax.rem(spot + plane - j, plane)
        return pltpu.make_async_remote_copy(
            src_ref=src.at[source, giver],
            dst_ref=dst.at[source, giver],
            send_sem=sends.at[i, j],
            recv_sem=recvs.at[i, j],
            device_id=(level * plane + giver, tp),
            device_id_type=MESH,
        )

    def fwd_copy(i):
        source = partners[i]
        return pltpu.make_async_remote_copy(
            src_ref=recv_own.at[source],
            dst_ref=recv_peer.at[source],
            send_sem=fwd_send_sem.at[i],
            recv_sem=fwd_recv_sem.at[i],
            device_id=(ep, other),
            device_id_type=MESH,
        )

    disp_args = (disp, recv_own, disp_send_sem, disp_recv_sem)
    for i in range(1, planes):
        rows_copy(i).start()
    for i in range(1, planes):
        from_level(*table_args, i).wait_recv()
    keeps = []

    def place_rows(i, rows):
        source = partners[i]
        placed = dot(tables_recv[source, 0], rows).astype(BF16)
        disp[source] = placed.reshape(plane, cap, half)
        for j in range(1, plane):
            beside_copy(*disp_args, i, j).start()
        keep = pltpu.make_async_copy(
            disp.at[source, spot], recv_own.at[source, spot], local_sem.at[i]
        )
        keep.start()
        keeps.append(keep)

    place_rows(0, normed_two)
    for i in range(1, planes):
        rows_arrival(i).wait_recv()
        place_rows(i, rows_recv[partners[i]])
    for i in range(planes):
        keeps[i].wait()
        for j in range(1, plane):
            beside_arrival(*disp_args, i, j).wait_recv()
        fwd_copy(i).start()

    loads[11].wait()
    loads[12].wait()
    rows_block = min(slots, 256)
    row_blocks = slots // rows_block
    per_block = rows_block // group
    hidden = gate.shape[1]

    def first_half(i, carry):
        cols = pl.ds(pl.multiple_of(i * GATE_BLOCK, GATE_BLOCK), GATE_BLOCK)
        depth = pl.ds(pl.multiple_of(tp * half, half), half)
        for r in range(row_blocks):
            rows = recv_own[r * per_block : (r + 1) * per_block].reshape(rows_block, half)
            at = slice(r * rows_block, (r + 1) * rows_block)
            gate_acc[at, cols] = dot(rows, gate[depth, cols])
            up_acc[at, cols] = dot(rows, up[depth, cols])
        return carry

    lax.fori_loop(0, hidden // GATE_BLOCK, first_half, 0)

    for i in range(planes):
        fwd_copy(i).wait()

    def second_half(i, carry):
        cols = pl.ds(pl.multiple_of(i * GATE_BLOCK, GATE_BLOCK), GATE_BLOCK)
        depth = pl.ds(pl.multiple_of(other * half, half), half)
        for r in range(row_blocks):
            rows = recv_peer[r * per_block : (r + 1) * per_block].reshape(rows_block, half)
            at = slice(r * rows_block, (r + 1) * rows_block)
            g = gate_acc[at, cols] + dot(rows, gate[depth, cols])
            u = up_acc[at, cols] + dot(rows, up[depth, cols])
            c = jnp.minimum(g, SWIGLU_LIMIT)
            linear = jnp.clip(u, -SWIGLU_LIMIT, SWIGLU_LIMIT)
            act_ref[at, cols] = (
                c * jax.nn.sigmoid(SWIGLU_ALPHA * c) * (linear + 1.0)
            ).astype(BF16)
        return carry

    lax.fori_loop(0, hidden // GATE_BLOCK, second_half, 0)

    loads[13].wait()
    tiles = half // COL_BLOCK

    def down_copy(i):
        return pltpu.make_async_remote_copy(
            src_ref=down_send.at[i],
            dst_ref=down_recv.at[i],
            send_sem=down_send_sem.at[i],
            recv_sem=down_recv_sem.at[i],
            device_id=(ep, other),
            device_id_type=MESH,
        )

    def down_tile(ref, side, i):
        cols = pl.ds(pl.multiple_of(side * half + i * COL_BLOCK, COL_BLOCK), COL_BLOCK)
        for r in range(row_blocks):
            at = slice(r * rows_block, (r + 1) * rows_block)
            ref[i, at, :] = dot(act_ref[at, :], down[:, cols]).astype(BF16)

    def down_other(i, carry):
        down_tile(down_send, other, i)
        down_copy(i).start()
        return carry

    lax.fori_loop(0, tiles, down_other, 0)

    def down_mine(i, carry):
        down_tile(down_own, tp, i)
        return carry

    lax.fori_loop(0, tiles, down_mine, 0)
    for i in range(tiles):
        down_copy(i).wait()
        total = (down_own[i].astype(F32) + down_recv[i].astype(F32)).astype(BF16)
        back_send[:, :, :, i * COL_BLOCK : (i + 1) * COL_BLOCK] = total.reshape(
            planes, plane, cap, COL_BLOCK
        )

    back_args = (back_send, back_recv, back_send_sem, back_recv_sem)
    order = tuple(reversed(range(planes)))
    back_keeps = {}
    for i in order:
        for j in range(1, plane):
            beside_copy(*back_args, i, j).start()
        source = partners[i]
        back_keeps[i] = pltpu.make_async_copy(
            back_send.at[source, spot], back_recv.at[source, spot], local_sem.at[planes + i]
        )
        back_keeps[i].start()

    sum_args = (sum_send, sum_recv, sum_send_sem, sum_recv_sem)
    over_slots = (((0,), (0,)), ((), ()))
    total = res_ref[...].astype(F32)
    for i in order:
        source = partners[i]
        back_keeps[i].wait()
        for j in range(1, plane):
            beside_arrival(*back_args, i, j).wait_recv()
        back = back_recv[source].reshape(group, half)
        mixed = lax.dot_general(
            tables_recv[source, 1], back, over_slots, preferred_element_type=F32
        ) + lax.dot_general(tables_recv[source, 2], back, over_slots, preferred_element_type=F32)
        if i == 0:
            total = total + mixed
        else:
            sum_send[source] = mixed.astype(BF16)
            to_level(*sum_args, i).start()
    for i in range(1, planes):
        from_level(*sum_args, i).wait_recv()
        total = total + sum_recv[partners[i]].astype(F32)
    out_ref[...] = total.astype(BF16)

    for i in range(1, planes):
        to_level(*table_args, i).wait_send()
        rows_copy(i).wait_send()
        to_level(*sum_args, i).wait_send()
    for i in range(planes):
        for j in range(1, plane):
            beside_copy(*disp_args, i, j).wait_send()
            beside_copy(*back_args, i, j).wait_send()


def publish(*refs):
    sems = refs[-1]
    count = len(refs) // 2
    copies = []
    for i in range(count):
        copy = pltpu.make_async_copy(refs[i], refs[count + i], sems.at[i])
        copy.start()
        copies.append(copy)
    for copy in copies:
        copy.wait()


def local(
    tokens,
    norm1_gain,
    w_query,
    w_key,
    w_value,
    head_bias,
    key_cache,
    value_cache,
    seq_lengths,
    w_out,
    norm2_gain,
    route_ids,
    route_logits,
    expert_gate,
    expert_up,
    expert_down,
):
    n = lax.axis_size("ep")
    seqs, half = tokens.shape
    top = route_ids.shape[1]
    experts = n * expert_gate.shape[0]
    capacity = max(2, 2 * seqs * top // experts)
    cap = -(-capacity // 16) * 16
    slots = n * cap
    planes = 4 if n % 4 == 0 else 1
    plane = n // planes
    qc = w_query.shape[1] // 2
    kcols = w_key.shape[1] // 2
    groups = qc // HEAD
    positions = key_cache.shape[1]
    hidden = expert_gate.shape[2]
    tiles = half // COL_BLOCK
    keys = jnp.swapaxes(key_cache, 1, 2)
    values = jnp.swapaxes(value_cache, 1, 2)
    operands = (
        tokens,
        norm1_gain.reshape(1, -1),
        w_query,
        w_key,
        w_value,
        head_bias,
        keys,
        values,
        seq_lengths,
        w_out,
        norm2_gain.reshape(1, -1),
        route_ids.T,
        route_logits.T,
        expert_gate.reshape(expert_gate.shape[1:]),
        expert_up.reshape(expert_up.shape[1:]),
        expert_down.reshape(expert_down.shape[1:]),
    )
    in_smem = (5, 8)
    in_specs = [
        pl.BlockSpec(memory_space=pltpu.SMEM if i in in_smem else pl.ANY)
        for i in range(len(operands))
    ]
    vmem = pl.BlockSpec(memory_space=pltpu.VMEM)
    loaded = [
        pltpu.VMEM(a.shape, a.dtype) for i, a in enumerate(operands) if i not in in_smem
    ]
    dma = pltpu.SemaphoreType.DMA
    scratch = (
        [loaded[0], loaded[0]]
        + loaded[1:]
        + [
            pltpu.VMEM((seqs + PAD, qc + 2 * kcols + 2 * LANES), F32),
            pltpu.VMEM((seqs + PAD, qc + 2 * kcols + 2 * LANES), F32),
            pltpu.VMEM((seqs, groups, HEAD), F32),
            pltpu.VMEM((seqs * groups, positions), F32),
            pltpu.VMEM((seqs, groups, HEAD), F32),
            pltpu.VMEM((2, seqs, half), BF16),
            pltpu.VMEM((2, seqs, half), BF16),
            pltpu.VMEM((seqs, half), BF16),
            pltpu.VMEM((planes, 3, plane * cap, seqs), BF16),
            pltpu.VMEM((planes, 3, plane * cap, seqs), BF16),
            pltpu.VMEM((seqs, half), BF16),
            pltpu.VMEM((planes, seqs, half), BF16),
            pltpu.VMEM((planes, plane, cap, half), BF16),
            pltpu.VMEM((planes, plane, cap, half), BF16),
            pltpu.VMEM((planes, plane, cap, half), BF16),
            pltpu.VMEM((slots, hidden), F32),
            pltpu.VMEM((slots, hidden), F32),
            pltpu.VMEM((slots, hidden), BF16),
            pltpu.VMEM((tiles, slots, COL_BLOCK), BF16),
            pltpu.VMEM((tiles, slots, COL_BLOCK), BF16),
            pltpu.VMEM((tiles, slots, COL_BLOCK), BF16),
            pltpu.VMEM((planes, plane, cap, half), BF16),
            pltpu.VMEM((planes, plane, cap, half), BF16),
            pltpu.VMEM((planes, seqs, half), BF16),
            pltpu.VMEM((planes, seqs, half), BF16),
            dma((len(loaded),)),
            dma((3,)),
            dma((3,)),
            dma((planes,)),
            dma((planes,)),
            dma((planes,)),
            dma((planes,)),
            dma((planes,)),
            dma((planes,)),
            dma((planes, plane)),
            dma((planes, plane)),
            dma((planes,)),
            dma((planes,)),
            dma((tiles,)),
            dma((tiles,)),
            dma((planes, plane)),
            dma((planes, plane)),
            dma((2 * planes,)),
        ]
    )
    shapes = ((seqs, half), (seqs, kcols), (seqs, kcols))
    results = pl.pallas_call(
        functools.partial(kernel, n, cap),
        out_shape=tuple(pltpu.VMEM(shape, BF16) for shape in shapes),
        in_specs=in_specs,
        out_specs=(vmem, vmem, vmem),
        scratch_shapes=scratch,
        compiler_params=pltpu.CompilerParams(
            collective_id=0, has_side_effects=True, vmem_limit_bytes=VMEM_BYTES
        ),
    )(*operands)
    return pl.pallas_call(
        publish,
        out_shape=tuple(jax.ShapeDtypeStruct(shape, BF16) for shape in shapes),
        in_specs=[vmem] * len(shapes),
        out_specs=tuple([pl.BlockSpec(memory_space=pl.ANY)] * len(shapes)),
        scratch_shapes=[dma((len(shapes),))],
    )(*(pltpu.with_memory_space_constraint(r, pltpu.VMEM) for r in results))


def solution(mesh):
    in_specs = (
        P("ep", "tp"),
        P("tp"),
        P("tp", None),
        P("tp", None),
        P("tp", None),
        P("tp"),
        P("ep", None, "tp"),
        P("ep", None, "tp"),
        P("ep"),
        P("tp", None),
        P("tp"),
        P("ep", None),
        P("ep", None),
        P("ep", None, "tp"),
        P("ep", None, "tp"),
        P("ep", "tp", None),
    )
    out_specs = (P("ep", "tp"), P("ep", "tp"), P("ep", "tp"))
    return jax.shard_map(local, mesh=mesh, in_specs=in_specs, out_specs=out_specs, check_vma=False)
```

```python
import functools

import jax
import jax.numpy as jnp
from jax import lax
from jax.experimental import pallas as pl
from jax.experimental.pallas import tpu as pltpu
from jax.sharding import PartitionSpec as P

HEAD = 64
LN_EPS = 1e-05
SWIGLU_ALPHA = 1.702
SWIGLU_LIMIT = 7.0
MESH = pl.DeviceIdType.MESH
F32 = jnp.float32
BF16 = jnp.bfloat16
DEAD = -1e30
POS_BLOCK = 256
COL_BLOCK = 512
GATE_BLOCK = 512
PAD = 16
BATCH = 4
CHUNKS = 2
VMEM_BYTES = 63 * 1024 * 1024
LANES = 128


def dot(a, b):
    return jnp.dot(a, b, preferred_element_type=F32)


def kernel(
    n,
    cap,
    tok_hbm,
    g1_hbm,
    wq_hbm,
    wk_hbm,
    wv_hbm,
    bias_ref,
    kc_hbm,
    vc_hbm,
    lens_ref,
    wo_hbm,
    g2_hbm,
    ids_hbm,
    logits_hbm,
    gate_hbm,
    up_hbm,
    down_hbm,
    out_ref,
    nk_ref,
    nv_ref,
    x_own,
    x_peer,
    g1,
    wq,
    wk,
    wv,
    kc,
    vc,
    wo,
    g2,
    ids,
    logits,
    gate,
    up,
    down,
    proj_send,
    proj_recv,
    q_rows,
    q_wide,
    z_ref,
    w_ref,
    att_ref,
    part_send,
    part_recv,
    res_ref,
    route_send,
    route_recv,
    tables,
    rows_ref,
    rows_recv,
    disp,
    recv_own,
    recv_peer,
    gate_acc,
    up_acc,
    act_ref,
    down_send,
    down_recv,
    down_own,
    back_send,
    back_recv,
    sum_send,
    sum_recv,
    total_ref,
    load_sem,
    one_send,
    one_recv,
    route_send_sem,
    route_recv_sem,
    rows_send_sem,
    rows_recv_sem,
    sum_send_sem,
    sum_recv_sem,
    disp_send_sem,
    disp_recv_sem,
    fwd_send_sem,
    fwd_recv_sem,
    down_send_sem,
    down_recv_sem,
    back_send_sem,
    back_recv_sem,
    local_sem,
    back_local_sem,
):
    ep = lax.axis_index("ep")
    tp = lax.axis_index("tp")
    other = 1 - tp
    seqs, half = x_own.shape
    width = 2 * half

    loads = []
    pairs = (
        (tok_hbm, x_own),
        (g1_hbm, g1),
        (wq_hbm, wq),
        (wk_hbm, wk),
        (wv_hbm, wv),
        (kc_hbm, kc),
        (vc_hbm, vc),
        (wo_hbm, wo),
        (g2_hbm, g2),
        (ids_hbm, ids),
        (logits_hbm, logits),
        (gate_hbm, gate),
        (up_hbm, up),
        (down_hbm, down),
    )
    for i, (src, dst) in enumerate(pairs):
        copy = pltpu.make_async_copy(src, dst, load_sem.at[i])
        loads.append(copy)
    for i in (0, 2, 3, 4, 1, 9, 10, 8):
        loads[i].start()

    def peer_copy(src, dst, i):
        return pltpu.make_async_remote_copy(
            src_ref=src,
            dst_ref=dst,
            send_sem=one_send.at[i],
            recv_sem=one_recv.at[i],
            device_id=(ep, other),
            device_id_type=MESH,
        )

    barrier = pltpu.get_barrier_semaphore()
    pl.semaphore_signal(barrier, inc=1, device_id=(ep, other), device_id_type=MESH)

    planes = tables.shape[0]
    plane = n // planes
    level = ep // plane
    spot = ep % plane

    def column(i):
        return lax.rem(level + i, planes) * plane + spot

    def beside(i):
        return level * plane + lax.rem(spot + i, plane)

    if planes == 4:
        inner = lax.rem((level + 1) // 2, 2)
        over = lax.rem(level + 2, 4)
        across = 3 - level
        partners = (
            level,
            inner * across + (1 - inner) * over,
            level + 1 - 2 * lax.rem(level, 2),
            inner * over + (1 - inner) * across,
        )
        pairs = ((0, 1), (2, 3))
        eager = (1, 3, 2)
    else:
        partners = (level,)
        pairs = ((0,),)
        eager = ()

    def greet_column(i, carry):
        pl.semaphore_signal(barrier, inc=1, device_id=(column(i), tp), device_id_type=MESH)
        return carry

    def greet_beside(i, carry):
        pl.semaphore_signal(barrier, inc=1, device_id=(beside(i), tp), device_id_type=MESH)
        return carry

    lax.fori_loop(1, planes, greet_column, 0)
    lax.fori_loop(1, plane, greet_beside, 0)
    for i in (0, 1, 2, 3, 4):
        loads[i].wait()
    for i in (5, 6, 7):
        loads[i].start()
    mine = x_own[...].astype(F32)
    mean_own = jnp.sum(mine, axis=1, keepdims=True) / half
    centred = mine - mean_own
    square_own = jnp.sum(centred * centred, axis=1, keepdims=True)
    gain = g1[...]
    gain_hi = gain.astype(BF16)
    gain_lo = (gain - gain_hi.astype(F32)).astype(BF16)
    pad_row = lax.broadcasted_iota(jnp.int32, (PAD, half), 0)
    gains = jnp.where(
        pad_row == 0, gain_hi.astype(F32), jnp.where(pad_row == 1, gain_lo.astype(F32), 0.0)
    )
    stacked = jnp.concatenate([centred * gain, gains], axis=0).astype(BF16)
    pq = dot(stacked, wq[...])
    pk = dot(stacked, wk[...])
    pv = dot(stacked, wv[...])
    qc = pq.shape[1] // 2
    kcols = pk.shape[1] // 2
    first = tp == 0
    used = qc + 2 * kcols
    proj_send[:, :qc] = jnp.where(first, pq[:, qc:], pq[:, :qc])
    proj_send[:, qc : qc + kcols] = jnp.where(first, pk[:, kcols:], pk[:, :kcols])
    proj_send[:, qc + kcols : used] = jnp.where(first, pv[:, kcols:], pv[:, :kcols])
    proj_send[:seqs, used : used + LANES] = jnp.broadcast_to(mean_own, (seqs, LANES))
    proj_send[:seqs, used + LANES :] = jnp.broadcast_to(square_own, (seqs, LANES))
    pl.semaphore_wait(barrier, planes + plane - 1)

    proj_copy = peer_copy(proj_send, proj_recv, 1)
    proj_copy.start()
    loads[9].wait()
    loads[10].wait()
    top = ids.shape[0]
    route_send[:top] = ids[...].astype(F32)
    route_send[top:] = logits[...]

    def route_copy(i, mine):
        to = partners[i]
        return pltpu.make_async_remote_copy(
            src_ref=route_send,
            dst_ref=route_recv.at[level if mine else to],
            send_sem=route_send_sem.at[to],
            recv_sem=route_recv_sem.at[level if mine else to],
            device_id=(to * plane + spot, tp),
            device_id_type=MESH,
        )

    for i in eager:
        route_copy(i, True).start()
    tok_copy = peer_copy(x_own, x_peer, 0)
    tok_copy.start()

    def stats(a, b):
        total = jnp.sum(a, axis=1, keepdims=True) + jnp.sum(b, axis=1, keepdims=True)
        square = jnp.sum(a * a, axis=1, keepdims=True) + jnp.sum(b * b, axis=1, keepdims=True)
        mean = total / width
        return mean, lax.rsqrt(square / width - mean * mean + LN_EPS)

    group = plane * cap
    slot_row = lax.broadcasted_iota(jnp.int32, (group, seqs), 0)
    slot_expert = slot_row // cap
    slot_rank = (slot_row - slot_expert * cap).astype(F32)
    slot_expert = (slot_expert + level * plane).astype(F32)
    earlier = (
        lax.broadcasted_iota(jnp.int32, (seqs, seqs), 0)
        < lax.broadcasted_iota(jnp.int32, (seqs, seqs), 1)
    )
    earlier = jnp.where(earlier, 1.0, 0.0).astype(BF16)

    def make_tables(k):
        route = route_send[...] if k == 0 else route_recv[partners[k]]
        raw = jnp.exp(route[top:])
        probs = raw / jnp.sum(raw, axis=0, keepdims=True)
        hot = jnp.zeros((group, seqs), F32)
        prob_hot = jnp.zeros((group, seqs), F32)
        for i in range(top):
            match = jnp.abs(route[i : i + 1] - slot_expert) < 0.5
            hot = hot + jnp.where(match, 1.0, 0.0)
            prob_hot = prob_hot + jnp.where(match, probs[i : i + 1, :], 0.0)
        rank = dot(hot.astype(BF16), earlier)
        chosen = (hot > 0.5) & (jnp.abs(rank - slot_rank) < 0.5)
        weight = jnp.where(chosen, prob_hot, 0.0)
        weight_hi = weight.astype(BF16)
        tables[k, 0] = jnp.where(chosen, 1.0, 0.0).astype(BF16)
        tables[k, 1] = weight_hi
        tables[k, 2] = (weight - weight_hi.astype(F32)).astype(BF16)

    groups = qc // HEAD
    bias = jnp.zeros((groups, 1), F32)
    head_row = lax.broadcasted_iota(jnp.int32, (groups, 1), 0)
    for h in range(groups):
        bias = bias + jnp.where(head_row == h, bias_ref[h], 0.0)

    own_q = jnp.where(first, pq[:, :qc], pq[:, qc:])
    own_k = jnp.where(first, pk[:, :kcols], pk[:, kcols:])
    own_v = jnp.where(first, pv[:, :kcols], pv[:, kcols:])
    proj_copy.wait()
    mean_peer = proj_recv[:seqs, used : used + 1]
    square_peer = proj_recv[:seqs, used + LANES : used + LANES + 1]
    apart = (mean_own - mean_peer) * 0.5
    scale = lax.rsqrt((square_own + square_peer) / width + apart * apart + LN_EPS)

    def joined(own, lo, hi):
        tilt = (own[seqs : seqs + 1] + own[seqs + 1 : seqs + 2]) - (
            proj_recv[seqs : seqs + 1, lo:hi] + proj_recv[seqs + 1 : seqs + 2, lo:hi]
        )
        return (scale * (own[:seqs] + proj_recv[:seqs, lo:hi] + apart * tilt)).astype(BF16)

    query = joined(own_q, 0, qc).astype(F32)
    nk_ref[...] = joined(own_k, qc, qc + kcols)
    nv_ref[...] = joined(own_v, qc + kcols, used)
    for h in range(groups):
        q_rows[:, h, :] = query[:, h * HEAD : (h + 1) * HEAD]
    flat = q_rows[...].reshape(seqs * groups, HEAD).astype(BF16)
    wide_row = lax.broadcasted_iota(jnp.int32, (seqs * groups, BATCH * HEAD), 0)
    wide_col = lax.broadcasted_iota(jnp.int32, (seqs * groups, BATCH * HEAD), 1)
    q_wide[...] = jnp.where(
        lax.rem(wide_row // groups, BATCH) == wide_col // HEAD,
        jnp.concatenate([flat] * BATCH, axis=1),
        jnp.zeros((), BF16),
    )

    positions = kc.shape[2]
    after = (
        lax.broadcasted_iota(jnp.int32, (POS_BLOCK, POS_BLOCK), 0)
        > lax.broadcasted_iota(jnp.int32, (POS_BLOCK, POS_BLOCK), 1)
    )
    after = jnp.where(after, 1.0, 0.0).astype(BF16)
    chunk = seqs // CHUNKS
    step_rows = BATCH * groups
    place = lax.broadcasted_iota(jnp.int32, (step_rows, positions), 1)
    step_seq = lax.broadcasted_iota(jnp.int32, (step_rows, 1), 0) // groups
    step_bias = jnp.concatenate([bias] * BATCH, axis=0)

    def score(c):
        for i in range(c * chunk // BATCH, (c + 1) * chunk // BATCH):
            rows = slice(i * step_rows, (i + 1) * step_rows)
            keys = kc[i * BATCH : (i + 1) * BATCH].reshape(BATCH * HEAD, positions)
            length = jnp.zeros((step_rows, 1), jnp.int32)
            for j in range(BATCH):
                length = jnp.where(step_seq == j, lens_ref[i * BATCH + j], length)
            s = dot(q_wide[rows, :], keys) * HEAD ** (-0.5) + step_bias
            z_ref[rows, :] = jnp.where(place < length, s, DEAD)

    def spend(c):
        count = chunk * groups
        rows = slice(c * count, (c + 1) * count)
        beyond = jnp.zeros((count, 1), F32)
        for b in reversed(range(positions // POS_BLOCK)):
            cols = slice(b * POS_BLOCK, (b + 1) * POS_BLOCK)
            z = z_ref[rows, cols]
            tail = jnp.log(1.0 + jnp.exp(-jnp.abs(z)))
            spent = jnp.maximum(z, 0.0) + tail
            hi = spent.astype(BF16)
            lo = (spent - hi.astype(F32)).astype(BF16)
            sums = dot(jnp.concatenate([hi, lo], axis=0), after)
            inside = sums[:count] + sums[count:]
            w_ref[rows, cols] = jnp.exp(
                jnp.minimum(z, 0.0) - tail - (inside + beyond)
            ).astype(BF16)
            beyond = beyond + inside[:, :1] + spent[:, :1]

    def read(c):
        for i in range(c * chunk // BATCH, (c + 1) * chunk // BATCH):
            weights = w_ref[i * step_rows : (i + 1) * step_rows, :]
            values = vc[i * BATCH : (i + 1) * BATCH].reshape(BATCH * HEAD, positions)
            mixed = lax.dot_general(
                weights, values, (((1,), (1,)), ((), ())), preferred_element_type=F32
            )
            for j in range(BATCH):
                att_ref[i * BATCH + j] = mixed[
                    j * groups : (j + 1) * groups, j * HEAD : (j + 1) * HEAD
                ]

    def part_copy(c):
        return peer_copy(part_send.at[c], part_recv.at[c], 2 + c)

    def project(c):
        mine = slice(c * chunk, (c + 1) * chunk)
        attended = jnp.concatenate([att_ref[mine, h, :] for h in range(groups)], axis=1)
        part = dot(attended.astype(BF16), wo[...]).astype(BF16)
        part_send[c, 0] = part[:, :half]
        part_send[c, 1] = part[:, half:]
        part_copy(c).start()

    def rows_copy(i, c):
        to = partners[i]
        return pltpu.make_async_remote_copy(
            src_ref=rows_ref.at[c],
            dst_ref=rows_recv.at[level, c],
            send_sem=rows_send_sem.at[to, c],
            recv_sem=rows_recv_sem.at[level, c],
            device_id=(to * plane + spot, tp),
            device_id_type=MESH,
        )

    def rows_arrival(i, c):
        source = partners[i]
        return pltpu.make_async_remote_copy(
            src_ref=rows_ref.at[c],
            dst_ref=rows_recv.at[source, c],
            send_sem=rows_send_sem.at[source, c],
            recv_sem=rows_recv_sem.at[source, c],
            device_id=(source * plane + spot, tp),
            device_id_type=MESH,
        )

    def settle(c):
        at = slice(c * chunk, (c + 1) * chunk)
        part_copy(c).wait()
        res_own = (
            x_own[at, :].astype(F32)
            + (part_send[c, tp].astype(F32) + part_recv[c, tp].astype(F32))
        ).astype(BF16)
        res_other = (
            x_peer[at, :].astype(F32)
            + (part_send[c, other].astype(F32) + part_recv[c, other].astype(F32))
        ).astype(BF16)
        res_ref[at, :] = res_own
        mine = res_own.astype(F32)
        mean, scale = stats(mine, res_other.astype(F32))
        rows_ref[c] = ((mine - mean) * scale * g2[...]).astype(BF16)
        for i in eager:
            rows_copy(i, c).start()

    loads[5].wait()
    for c in range(CHUNKS):
        score(c)
        spend(c)
        if c == 0:
            loads[6].wait()
            for i in (11, 12, 13):
                loads[i].start()
            loads[7].wait()
            loads[8].wait()
            tok_copy.wait()
        else:
            settle(c - 1)
        read(c)
        project(c)
    for k in range(planes):
        if k > 0:
            route_copy(k, False).wait_recv()
        make_tables(k)
    settle(CHUNKS - 1)

    def beside_copy(src, dst, send_sem, recv_sem, j):
        to = lax.rem(spot + j, plane)
        return pltpu.make_async_remote_copy(
            src_ref=src(to),
            dst_ref=dst(spot),
            send_sem=send_sem,
            recv_sem=recv_sem,
            device_id=(level * plane + to, tp),
            device_id_type=MESH,
        )

    def disp_copy(k, j):
        return beside_copy(
            lambda to: disp.at[k, to],
            lambda giver: recv_own.at[k, giver],
            disp_send_sem.at[k],
            disp_recv_sem.at[k],
            j,
        )

    def disp_all(k):
        return pltpu.make_async_remote_copy(
            src_ref=disp.at[k, pl.ds(0, plane - 1)],
            dst_ref=recv_own.at[k, pl.ds(0, plane - 1)],
            send_sem=disp_send_sem.at[k],
            recv_sem=disp_recv_sem.at[k],
            device_id=(ep, other),
            device_id_type=MESH,
        )

    def disp_keep(k):
        return pltpu.make_async_copy(disp.at[k, spot], recv_own.at[k, spot], local_sem.at[k])

    def fwd_copy(k):
        return pltpu.make_async_remote_copy(
            src_ref=recv_own.at[k],
            dst_ref=recv_peer.at[k],
            send_sem=fwd_send_sem.at[k],
            recv_sem=fwd_recv_sem.at[k],
            device_id=(ep, other),
            device_id_type=MESH,
        )

    for k in range(planes):
        if k > 0:
            for c in range(CHUNKS):
                rows_arrival(k, c).wait_recv()
            rows = rows_recv[partners[k]].reshape(seqs, half)
        else:
            rows = rows_ref[...].reshape(seqs, half)
        placed = dot(tables[k, 0], rows).astype(BF16)
        disp[k] = placed.reshape(plane, cap, half)
        for j in range(1, plane):
            disp_copy(k, j).start()
        disp_keep(k).start()

    def gather(k):
        disp_keep(k).wait()
        disp_all(k).wait_recv()
        fwd_copy(k).start()

    hidden = gate.shape[1]
    own_depth = pl.ds(pl.multiple_of(tp * half, half), half)
    peer_depth = pl.ds(pl.multiple_of(other * half, half), half)
    held = len(pairs[0])
    rows_block = min(held * group, 256)
    row_blocks = held * group // rows_block
    per_block = rows_block // cap

    def rows_of(ref, pair, r):
        rows = ref[pair[0] : pair[0] + held].reshape(held * plane, cap, half)
        return rows[r * per_block : (r + 1) * per_block].reshape(rows_block, half)

    def swiglu(g, u):
        c = jnp.minimum(g, SWIGLU_LIMIT)
        linear = jnp.clip(u, -SWIGLU_LIMIT, SWIGLU_LIMIT)
        return (c * jax.nn.sigmoid(SWIGLU_ALPHA * c) * (linear + 1.0)).astype(BF16)

    def first_half(pair):
        def body(i, carry):
            cols = pl.ds(pl.multiple_of(i * GATE_BLOCK, GATE_BLOCK), GATE_BLOCK)
            for r in range(row_blocks):
                rows = rows_of(recv_own, pair, r)
                at = slice(r * rows_block, (r + 1) * rows_block)
                gate_acc[at, cols] = dot(rows, gate[own_depth, cols])
                up_acc[at, cols] = dot(rows, up[own_depth, cols])
            return carry

        lax.fori_loop(0, hidden // GATE_BLOCK, body, 0)

    def second_half(p, pair):
        def body(i, carry):
            cols = pl.ds(pl.multiple_of(i * GATE_BLOCK, GATE_BLOCK), GATE_BLOCK)
            for r in range(row_blocks):
                rows = rows_of(recv_peer, pair, r)
                at = slice(r * rows_block, (r + 1) * rows_block)
                g = gate_acc[at, cols] + dot(rows, gate[peer_depth, cols])
                u = up_acc[at, cols] + dot(rows, up[peer_depth, cols])
                act_ref[p, at, cols] = swiglu(g, u)
            return carry

        lax.fori_loop(0, hidden // GATE_BLOCK, body, 0)

    def whole_depth(p, pair):
        def body(i, carry):
            cols = pl.ds(pl.multiple_of(i * GATE_BLOCK, GATE_BLOCK), GATE_BLOCK)
            for r in range(row_blocks):
                mine = rows_of(recv_own, pair, r)
                theirs = rows_of(recv_peer, pair, r)
                at = slice(r * rows_block, (r + 1) * rows_block)
                g = dot(mine, gate[own_depth, cols]) + dot(theirs, gate[peer_depth, cols])
                u = dot(mine, up[own_depth, cols]) + dot(theirs, up[peer_depth, cols])
                act_ref[p, at, cols] = swiglu(g, u)
            return carry

        lax.fori_loop(0, hidden // GATE_BLOCK, body, 0)

    tiles = half // COL_BLOCK
    all_tiles = pl.ds(0, tiles)
    one_tile = [pl.ds(t, 1) for t in range(tiles)]

    def down_copy(p, t):
        return pltpu.make_async_remote_copy(
            src_ref=down_send.at[p, t],
            dst_ref=down_recv.at[p, t],
            send_sem=down_send_sem.at[p, t],
            recv_sem=down_recv_sem.at[p, t],
            device_id=(ep, other),
            device_id_type=MESH,
        )

    def down_tile(p, side, t, r):
        cols = pl.ds(pl.multiple_of(side * half + t * COL_BLOCK, COL_BLOCK), COL_BLOCK)
        at = slice(r * rows_block, (r + 1) * rows_block)
        return dot(act_ref[p, at, :], down[:, cols]).astype(BF16)

    def down_all(p):
        return pltpu.make_async_remote_copy(
            src_ref=down_send.at[p],
            dst_ref=down_recv.at[p],
            send_sem=down_send_sem.at[p, 0],
            recv_sem=down_recv_sem.at[p, 0],
            device_id=(ep, other),
            device_id_type=MESH,
        )

    def down_other(p, together):
        for t in range(tiles):
            for r in range(row_blocks):
                at = slice(r * rows_block, (r + 1) * rows_block)
                down_send[p, t, at, :] = down_tile(p, other, t, r)
            if not together:
                down_copy(p, t).start()
        if together:
            down_all(p).start()

    def back_copy(k, at, j):
        return beside_copy(
            lambda to: back_send.at[k, to, at],
            lambda giver: back_recv.at[k, giver, at],
            back_send_sem.at[k],
            back_recv_sem.at[k, at.start // at.size],
            j,
        )

    def back_all(k, at):
        return pltpu.make_async_remote_copy(
            src_ref=back_send.at[k, pl.ds(0, plane - 1), at],
            dst_ref=back_recv.at[k, pl.ds(0, plane - 1), at],
            send_sem=back_send_sem.at[k],
            recv_sem=back_recv_sem.at[k, at.start // at.size],
            device_id=(ep, other),
            device_id_type=MESH,
        )

    def back_keep(k, at):
        return pltpu.make_async_copy(
            back_send.at[k, spot, at],
            back_recv.at[k, spot, at],
            back_local_sem.at[k, at.start // at.size],
        )

    def send_back(k, at):
        for j in range(1, plane):
            back_copy(k, at, j).start()
        back_keep(k, at).start()

    def down_join(p, pair, t):
        total = (down_own[t].astype(F32) + down_recv[p, t].astype(F32)).astype(BF16)
        total = total.reshape(held, plane, cap, COL_BLOCK)
        for i, k in enumerate(pair):
            back_send[k, :, t] = total[i]

    def down_mine(p, pair, together):
        for t in range(tiles):
            for r in range(row_blocks):
                at = slice(r * rows_block, (r + 1) * rows_block)
                down_own[t, at, :] = down_tile(p, tp, t, r)
            if not together:
                down_copy(p, t).wait()
                down_join(p, pair, t)
                send_back(pair[-1], one_tile[t])
        if together:
            down_all(p).wait()
            for t in range(tiles):
                down_join(p, pair, t)
            for k in reversed(pair):
                send_back(k, all_tiles)
        else:
            for k in reversed(pair[:-1]):
                for t in range(tiles):
                    send_back(k, one_tile[t])

    def sum_copy(k, t):
        to = partners[k]
        return pltpu.make_async_remote_copy(
            src_ref=sum_send.at[to, t],
            dst_ref=sum_recv.at[level, t],
            send_sem=sum_send_sem.at[to, t],
            recv_sem=sum_recv_sem.at[level, t],
            device_id=(to * plane + spot, tp),
            device_id_type=MESH,
        )

    def sum_arrival(k, t):
        source = partners[k]
        return pltpu.make_async_remote_copy(
            src_ref=sum_send.at[source, t],
            dst_ref=sum_recv.at[source, t],
            send_sem=sum_send_sem.at[source, t],
            recv_sem=sum_recv_sem.at[source, t],
            device_id=(source * plane + spot, tp),
            device_id_type=MESH,
        )

    over_slots = (((0,), (0,)), ((), ()))

    def combine(k, at):
        back_keep(k, at).wait()
        back_all(k, at).wait_recv()
        to = partners[k]
        mixes = []
        for t in range(at.start, at.start + at.size):
            back = back_recv[k, :, t].reshape(group, COL_BLOCK)
            mixes.append(
                lax.dot_general(tables[k, 1], back, over_slots, preferred_element_type=F32)
                + lax.dot_general(tables[k, 2], back, over_slots, preferred_element_type=F32)
            )
        for t, mixed in zip(range(at.start, at.start + at.size), mixes):
            cols = slice(t * COL_BLOCK, (t + 1) * COL_BLOCK)
            if k == 0:
                total_ref[:, cols] = res_ref[:, cols].astype(F32) + mixed
            else:
                sum_send[to, t] = mixed.astype(BF16)
        if k > 0:
            for t in range(at.start, at.start + at.size):
                sum_copy(k, t).start()

    for k in pairs[0]:
        gather(k)
    loads[11].wait()
    loads[12].wait()
    first_half(pairs[0])
    for k in pairs[0]:
        fwd_copy(k).wait()
    second_half(0, pairs[0])
    loads[13].wait()
    down_other(0, True)
    if len(pairs) > 1:
        for k in pairs[1]:
            gather(k)
    down_mine(0, pairs[0], True)
    if len(pairs) > 1:
        for k in pairs[1]:
            fwd_copy(k).wait()
        whole_depth(1, pairs[1])
        down_other(1, False)
        down_mine(1, pairs[1], False)
    for i in range(1, planes):
        route_copy(i, True).wait_send()
        for c in range(CHUNKS):
            rows_copy(i, c).wait_send()
    for k in range(planes):
        disp_all(k).wait_send()
    for k in reversed(pairs[0]):
        combine(k, all_tiles)
        back_all(k, all_tiles).wait_send()
    if len(pairs) > 1:
        for k in reversed(pairs[1]):
            for t in range(tiles):
                combine(k, one_tile[t])
        for k in pairs[1]:
            back_all(k, all_tiles).wait_send()
    for k in eager:
        for t in range(tiles):
            sum_arrival(k, t).wait_recv()
    for t in range(tiles):
        cols = slice(t * COL_BLOCK, (t + 1) * COL_BLOCK)
        total = total_ref[:, cols]
        for k in range(1, planes):
            total = total + sum_recv[partners[k], t].astype(F32)
        out_ref[:, cols] = total.astype(BF16)

    for i in range(1, planes):
        for t in range(tiles):
            sum_copy(i, t).wait_send()


def publish(*refs):
    sems = refs[-1]
    count = len(refs) // 2
    copies = []
    for i in range(count):
        copy = pltpu.make_async_copy(refs[i], refs[count + i], sems.at[i])
        copy.start()
        copies.append(copy)
    for copy in copies:
        copy.wait()


def local(
    tokens,
    norm1_gain,
    w_query,
    w_key,
    w_value,
    head_bias,
    key_cache,
    value_cache,
    seq_lengths,
    w_out,
    norm2_gain,
    route_ids,
    route_logits,
    expert_gate,
    expert_up,
    expert_down,
):
    n = lax.axis_size("ep")
    seqs, half = tokens.shape
    top = route_ids.shape[1]
    experts = n * expert_gate.shape[0]
    capacity = max(2, 2 * seqs * top // experts)
    cap = -(-capacity // 16) * 16
    slots = n * cap
    planes = 4 if n % 4 == 0 else 1
    plane = n // planes
    qc = w_query.shape[1] // 2
    kcols = w_key.shape[1] // 2
    groups = qc // HEAD
    positions = key_cache.shape[1]
    hidden = expert_gate.shape[2]
    tiles = half // COL_BLOCK
    pair_count = 2 if planes == 4 else 1
    keys = jnp.swapaxes(key_cache, 1, 2)
    values = jnp.swapaxes(value_cache, 1, 2)
    operands = (
        tokens,
        norm1_gain.reshape(1, -1),
        w_query,
        w_key,
        w_value,
        head_bias,
        keys,
        values,
        seq_lengths,
        w_out,
        norm2_gain.reshape(1, -1),
        route_ids.T,
        route_logits.T,
        expert_gate.reshape(expert_gate.shape[1:]),
        expert_up.reshape(expert_up.shape[1:]),
        expert_down.reshape(expert_down.shape[1:]),
    )
    in_smem = (5, 8)
    in_specs = [
        pl.BlockSpec(memory_space=pltpu.SMEM if i in in_smem else pl.ANY)
        for i in range(len(operands))
    ]
    vmem = pl.BlockSpec(memory_space=pltpu.VMEM)
    loaded = [
        pltpu.VMEM(a.shape, a.dtype) for i, a in enumerate(operands) if i not in in_smem
    ]
    dma = pltpu.SemaphoreType.DMA
    scratch = (
        [loaded[0], loaded[0]]
        + loaded[1:]
        + [
            pltpu.VMEM((seqs + PAD, qc + 2 * kcols + 2 * LANES), F32),
            pltpu.VMEM((seqs + PAD, qc + 2 * kcols + 2 * LANES), F32),
            pltpu.VMEM((seqs, groups, HEAD), F32),
            pltpu.VMEM((seqs * groups, BATCH * HEAD), BF16),
            pltpu.VMEM((seqs * groups, positions), F32),
            pltpu.VMEM((seqs * groups, positions), BF16),
            pltpu.VMEM((seqs, groups, HEAD), F32),
            pltpu.VMEM((CHUNKS, 2, seqs // CHUNKS, half), BF16),
            pltpu.VMEM((CHUNKS, 2, seqs // CHUNKS, half), BF16),
            pltpu.VMEM((seqs, half), BF16),
            pltpu.VMEM((2 * top, seqs), F32),
            pltpu.VMEM((planes, 2 * top, seqs), F32),
            pltpu.VMEM((planes, 3, plane * cap, seqs), BF16),
            pltpu.VMEM((CHUNKS, seqs // CHUNKS, half), BF16),
            pltpu.VMEM((planes, CHUNKS, seqs // CHUNKS, half), BF16),
            pltpu.VMEM((planes, plane, cap, half), BF16),
            pltpu.VMEM((planes, plane, cap, half), BF16),
            pltpu.VMEM((planes, plane, cap, half), BF16),
            pltpu.VMEM((slots // pair_count, hidden), F32),
            pltpu.VMEM((slots // pair_count, hidden), F32),
            pltpu.VMEM((pair_count, slots // pair_count, hidden), BF16),
            pltpu.VMEM((pair_count, tiles, slots // pair_count, COL_BLOCK), BF16),
            pltpu.VMEM((pair_count, tiles, slots // pair_count, COL_BLOCK), BF16),
            pltpu.VMEM((tiles, slots // pair_count, COL_BLOCK), BF16),
            pltpu.VMEM((planes, plane, tiles, cap, COL_BLOCK), BF16),
            pltpu.VMEM((planes, plane, tiles, cap, COL_BLOCK), BF16),
            pltpu.VMEM((planes, tiles, seqs, COL_BLOCK), BF16),
            pltpu.VMEM((planes, tiles, seqs, COL_BLOCK), BF16),
            pltpu.VMEM((seqs, half), F32),
            dma((len(loaded),)),
            dma((2 + CHUNKS,)),
            dma((2 + CHUNKS,)),
            dma((planes,)),
            dma((planes,)),
            dma((planes, CHUNKS)),
            dma((planes, CHUNKS)),
            dma((planes, tiles)),
            dma((planes, tiles)),
            dma((planes,)),
            dma((planes,)),
            dma((planes,)),
            dma((planes,)),
            dma((pair_count, tiles)),
            dma((pair_count, tiles)),
            dma((planes,)),
            dma((planes, tiles)),
            dma((planes,)),
            dma((planes, tiles)),
        ]
    )
    shapes = ((seqs, half), (seqs, kcols), (seqs, kcols))
    results = pl.pallas_call(
        functools.partial(kernel, n, cap),
        out_shape=tuple(pltpu.VMEM(shape, BF16) for shape in shapes),
        in_specs=in_specs,
        out_specs=(vmem, vmem, vmem),
        scratch_shapes=scratch,
        compiler_params=pltpu.CompilerParams(
            collective_id=0, has_side_effects=True, vmem_limit_bytes=VMEM_BYTES
        ),
    )(*operands)
    return pl.pallas_call(
        publish,
        out_shape=tuple(jax.ShapeDtypeStruct(shape, BF16) for shape in shapes),
        in_specs=[vmem] * len(shapes),
        out_specs=tuple([pl.BlockSpec(memory_space=pl.ANY)] * len(shapes)),
        scratch_shapes=[dma((len(shapes),))],
    )(*(pltpu.with_memory_space_constraint(r, pltpu.VMEM) for r in results))


def solution(mesh):
    in_specs = (
        P("ep", "tp"),
        P("tp"),
        P("tp", None),
        P("tp", None),
        P("tp", None),
        P("tp"),
        P("ep", None, "tp"),
        P("ep", None, "tp"),
        P("ep"),
        P("tp", None),
        P("tp"),
        P("ep", None),
        P("ep", None),
        P("ep", None, "tp"),
        P("ep", None, "tp"),
        P("ep", "tp", None),
    )
    out_specs = (P("ep", "tp"), P("ep", "tp"), P("ep", "tp"))
    return jax.shard_map(local, mesh=mesh, in_specs=in_specs, out_specs=out_specs, check_vma=False)
```

```python
import functools

import jax
import jax.numpy as jnp
from jax import lax
from jax.experimental import pallas as pl
from jax.experimental.pallas import tpu as pltpu
from jax.sharding import PartitionSpec as P

HEAD = 64
LN_EPS = 1e-05
SWIGLU_ALPHA = 1.702
SWIGLU_LIMIT = 7.0
MESH = pl.DeviceIdType.MESH
F32 = jnp.float32
BF16 = jnp.bfloat16
DEAD = -1e30
POS_BLOCK = 256
COL_BLOCK = 512
GATE_BLOCK = 512
PAD = 16
BATCH = 4
CHUNKS = 2
VMEM_BYTES = 63 * 1024 * 1024
LANES = 128


def dot(a, b):
    return jnp.dot(a, b, preferred_element_type=F32)


def kernel(
    n,
    cap,
    tok_hbm,
    g1_hbm,
    wq_hbm,
    wk_hbm,
    wv_hbm,
    bias_hbm,
    kc_hbm,
    vc_hbm,
    lens_hbm,
    wo_hbm,
    g2_hbm,
    ids_hbm,
    logits_hbm,
    gate_hbm,
    up_hbm,
    down_hbm,
    out_ref,
    nk_ref,
    nv_ref,
    bias_ref,
    lens_ref,
    x_own,
    x_peer,
    g1,
    wq,
    wk,
    wv,
    kc,
    vc,
    wo,
    g2,
    ids,
    logits,
    gate,
    up,
    down,
    proj_send,
    proj_recv,
    q_rows,
    q_wide,
    z_ref,
    w_ref,
    att_ref,
    part_send,
    part_recv,
    res_ref,
    route_send,
    route_recv,
    tables,
    rows_ref,
    rows_recv,
    disp,
    recv_own,
    recv_peer,
    gate_acc,
    up_acc,
    act_ref,
    down_send,
    down_recv,
    down_own,
    back_send,
    back_recv,
    sum_send,
    sum_recv,
    total_ref,
    load_sem,
    one_send,
    one_recv,
    route_send_sem,
    route_recv_sem,
    rows_send_sem,
    rows_recv_sem,
    relay_sem,
    sum_send_sem,
    sum_recv_sem,
    disp_send_sem,
    disp_recv_sem,
    fwd_send_sem,
    fwd_recv_sem,
    down_send_sem,
    down_recv_sem,
    back_send_sem,
    back_recv_sem,
    local_sem,
    back_local_sem,
):
    ep = lax.axis_index("ep")
    tp = lax.axis_index("tp")
    other = 1 - tp
    seqs, half = x_own.shape
    width = 2 * half

    loads = []
    pairs = (
        (tok_hbm, x_own),
        (g1_hbm, g1),
        (wq_hbm, wq),
        (wk_hbm, wk),
        (wv_hbm, wv),
        (kc_hbm, kc),
        (vc_hbm, vc),
        (wo_hbm, wo),
        (g2_hbm, g2),
        (ids_hbm, ids),
        (logits_hbm, logits),
        (gate_hbm, gate),
        (up_hbm, up),
        (down_hbm, down),
        (bias_hbm, bias_ref),
        (lens_hbm, lens_ref),
    )
    for i, (src, dst) in enumerate(pairs):
        copy = pltpu.make_async_copy(src, dst, load_sem.at[i])
        loads.append(copy)
    for i in (0, 1, 2, 3, 4, 14, 15, 9, 10, 8, 5, 6, 7):
        loads[i].start()

    def peer_copy(src, dst, i):
        return pltpu.make_async_remote_copy(
            src_ref=src,
            dst_ref=dst,
            send_sem=one_send.at[i],
            recv_sem=one_recv.at[i],
            device_id=(ep, other),
            device_id_type=MESH,
        )

    barrier = pltpu.get_barrier_semaphore()
    pl.semaphore_signal(barrier, inc=1, device_id=(ep, other), device_id_type=MESH)

    planes = tables.shape[0]
    plane = n // planes
    level = ep // plane
    spot = ep % plane

    def column(i):
        return lax.rem(level + i, planes) * plane + spot

    def beside(i):
        return level * plane + lax.rem(spot + i, plane)

    if planes == 4:
        inner = lax.rem((level + 1) // 2, 2)
        partners = (
            level,
            lax.rem(level + 2, 4),
            level + 1 - 2 * lax.rem(level, 2),
            3 - level,
        )
        teams = ((0,), (1,), (2, 3))
        eager = (1, 3, 2)
    else:
        partners = (level,)
        inner = 0
        teams = ((0,),)
        eager = ()

    def greet_column(i, carry):
        pl.semaphore_signal(barrier, inc=1, device_id=(column(i), tp), device_id_type=MESH)
        return carry

    def greet_beside(i, carry):
        pl.semaphore_signal(barrier, inc=1, device_id=(beside(i), tp), device_id_type=MESH)
        return carry

    lax.fori_loop(1, planes, greet_column, 0)
    lax.fori_loop(1, plane, greet_beside, 0)
    loads[0].wait()
    loads[1].wait()
    mine = x_own[...].astype(F32)
    mean_own = jnp.sum(mine, axis=1, keepdims=True) / half
    centred = mine - mean_own
    square_own = jnp.sum(centred * centred, axis=1, keepdims=True)
    gain = g1[...]
    gain_hi = gain.astype(BF16)
    gain_lo = (gain - gain_hi.astype(F32)).astype(BF16)
    pad_row = lax.broadcasted_iota(jnp.int32, (PAD, half), 0)
    gains = jnp.where(
        pad_row == 0, gain_hi.astype(F32), jnp.where(pad_row == 1, gain_lo.astype(F32), 0.0)
    )
    stacked = jnp.concatenate([centred * gain, gains], axis=0).astype(BF16)
    for i in (2, 3, 4):
        loads[i].wait()
    pq = dot(stacked, wq[...])
    pk = dot(stacked, wk[...])
    pv = dot(stacked, wv[...])
    qc = pq.shape[1] // 2
    kcols = pk.shape[1] // 2
    first = tp == 0
    used = qc + 2 * kcols
    proj_send[:, :qc] = jnp.where(first, pq[:, qc:], pq[:, :qc])
    proj_send[:, qc : qc + kcols] = jnp.where(first, pk[:, kcols:], pk[:, :kcols])
    proj_send[:, qc + kcols : used] = jnp.where(first, pv[:, kcols:], pv[:, :kcols])
    proj_send[:seqs, used : used + LANES] = jnp.broadcast_to(mean_own, (seqs, LANES))
    proj_send[:seqs, used + LANES :] = jnp.broadcast_to(square_own, (seqs, LANES))
    pl.semaphore_wait(barrier, planes + plane - 1)

    proj_copy = peer_copy(proj_send, proj_recv, 1)
    proj_copy.start()
    loads[9].wait()
    loads[10].wait()
    top = ids.shape[0]
    route_send[:top] = ids[...].astype(F32)
    route_send[top:] = logits[...]

    def route_copy(i, mine):
        to = partners[i]
        return pltpu.make_async_remote_copy(
            src_ref=route_send,
            dst_ref=route_recv.at[level if mine else to],
            send_sem=route_send_sem.at[to],
            recv_sem=route_recv_sem.at[level if mine else to],
            device_id=(to * plane + spot, tp),
            device_id_type=MESH,
        )

    for i in eager:
        route_copy(i, True).start()
    tok_copy = peer_copy(x_own, x_peer, 0)
    tok_copy.start()

    def stats(a, b):
        total = jnp.sum(a, axis=1, keepdims=True) + jnp.sum(b, axis=1, keepdims=True)
        square = jnp.sum(a * a, axis=1, keepdims=True) + jnp.sum(b * b, axis=1, keepdims=True)
        mean = total / width
        return mean, lax.rsqrt(square / width - mean * mean + LN_EPS)

    group = plane * cap
    slot_row = lax.broadcasted_iota(jnp.int32, (group, seqs), 0)
    slot_expert = slot_row // cap
    slot_rank = (slot_row - slot_expert * cap).astype(F32)
    slot_expert = (slot_expert + level * plane).astype(F32)
    earlier = (
        lax.broadcasted_iota(jnp.int32, (seqs, seqs), 0)
        < lax.broadcasted_iota(jnp.int32, (seqs, seqs), 1)
    )
    earlier = jnp.where(earlier, 1.0, 0.0).astype(BF16)

    def make_tables(k):
        route = route_send[...] if k == 0 else route_recv[partners[k]]
        raw = jnp.exp(route[top:])
        probs = raw / jnp.sum(raw, axis=0, keepdims=True)
        hot = jnp.zeros((group, seqs), F32)
        prob_hot = jnp.zeros((group, seqs), F32)
        for i in range(top):
            match = jnp.abs(route[i : i + 1] - slot_expert) < 0.5
            hot = hot + jnp.where(match, 1.0, 0.0)
            prob_hot = prob_hot + jnp.where(match, probs[i : i + 1, :], 0.0)
        rank = dot(hot.astype(BF16), earlier)
        chosen = (hot > 0.5) & (jnp.abs(rank - slot_rank) < 0.5)
        weight = jnp.where(chosen, prob_hot, 0.0)
        weight_hi = weight.astype(BF16)
        tables[k, 0] = jnp.where(chosen, 1.0, 0.0).astype(BF16)
        tables[k, 1] = weight_hi
        tables[k, 2] = (weight - weight_hi.astype(F32)).astype(BF16)

    groups = qc // HEAD
    loads[14].wait()
    loads[15].wait()
    bias = jnp.zeros((groups, 1), F32)
    head_row = lax.broadcasted_iota(jnp.int32, (groups, 1), 0)
    for h in range(groups):
        bias = bias + jnp.where(head_row == h, bias_ref[h], 0.0)

    own_q = jnp.where(first, pq[:, :qc], pq[:, qc:])
    own_k = jnp.where(first, pk[:, :kcols], pk[:, kcols:])
    own_v = jnp.where(first, pv[:, :kcols], pv[:, kcols:])
    proj_copy.wait()
    mean_peer = proj_recv[:seqs, used : used + 1]
    square_peer = proj_recv[:seqs, used + LANES : used + LANES + 1]
    apart = (mean_own - mean_peer) * 0.5
    scale = lax.rsqrt((square_own + square_peer) / width + apart * apart + LN_EPS)

    def joined(own, lo, hi):
        tilt = (own[seqs : seqs + 1] + own[seqs + 1 : seqs + 2]) - (
            proj_recv[seqs : seqs + 1, lo:hi] + proj_recv[seqs + 1 : seqs + 2, lo:hi]
        )
        return (scale * (own[:seqs] + proj_recv[:seqs, lo:hi] + apart * tilt)).astype(BF16)

    query = joined(own_q, 0, qc).astype(F32)
    nk_ref[...] = joined(own_k, qc, qc + kcols)
    nv_ref[...] = joined(own_v, qc + kcols, used)
    for h in range(groups):
        q_rows[:, h, :] = query[:, h * HEAD : (h + 1) * HEAD]
    flat = q_rows[...].reshape(seqs * groups, HEAD).astype(BF16)
    wide_row = lax.broadcasted_iota(jnp.int32, (seqs * groups, BATCH * HEAD), 0)
    wide_col = lax.broadcasted_iota(jnp.int32, (seqs * groups, BATCH * HEAD), 1)
    q_wide[...] = jnp.where(
        lax.rem(wide_row // groups, BATCH) == wide_col // HEAD,
        jnp.concatenate([flat] * BATCH, axis=1),
        jnp.zeros((), BF16),
    )

    positions = kc.shape[2]
    after = (
        lax.broadcasted_iota(jnp.int32, (POS_BLOCK, POS_BLOCK), 0)
        > lax.broadcasted_iota(jnp.int32, (POS_BLOCK, POS_BLOCK), 1)
    )
    after = jnp.where(after, 1.0, 0.0).astype(BF16)
    chunk = seqs // CHUNKS
    step_rows = BATCH * groups
    place = lax.broadcasted_iota(jnp.int32, (step_rows, positions), 1)
    step_seq = lax.broadcasted_iota(jnp.int32, (step_rows, 1), 0) // groups
    step_bias = jnp.concatenate([bias] * BATCH, axis=0)

    def score(c):
        for i in range(c * chunk // BATCH, (c + 1) * chunk // BATCH):
            rows = slice(i * step_rows, (i + 1) * step_rows)
            keys = kc[i * BATCH : (i + 1) * BATCH].reshape(BATCH * HEAD, positions)
            length = jnp.zeros((step_rows, 1), jnp.int32)
            for j in range(BATCH):
                length = jnp.where(step_seq == j, lens_ref[i * BATCH + j], length)
            s = dot(q_wide[rows, :], keys) * HEAD ** (-0.5) + step_bias
            z_ref[rows, :] = jnp.where(place < length, s, DEAD)

    def spend(c):
        count = chunk * groups
        rows = slice(c * count, (c + 1) * count)
        beyond = jnp.zeros((count, 1), F32)
        for b in reversed(range(positions // POS_BLOCK)):
            cols = slice(b * POS_BLOCK, (b + 1) * POS_BLOCK)
            z = z_ref[rows, cols]
            tail = jnp.log(1.0 + jnp.exp(-jnp.abs(z)))
            spent = jnp.maximum(z, 0.0) + tail
            hi = spent.astype(BF16)
            lo = (spent - hi.astype(F32)).astype(BF16)
            sums = dot(jnp.concatenate([hi, lo], axis=0), after)
            inside = sums[:count] + sums[count:]
            w_ref[rows, cols] = jnp.exp(
                jnp.minimum(z, 0.0) - tail - (inside + beyond)
            ).astype(BF16)
            beyond = beyond + inside[:, :1] + spent[:, :1]

    def read(c):
        for i in range(c * chunk // BATCH, (c + 1) * chunk // BATCH):
            weights = w_ref[i * step_rows : (i + 1) * step_rows, :]
            values = vc[i * BATCH : (i + 1) * BATCH].reshape(BATCH * HEAD, positions)
            mixed = lax.dot_general(
                weights, values, (((1,), (1,)), ((), ())), preferred_element_type=F32
            )
            for j in range(BATCH):
                att_ref[i * BATCH + j] = mixed[
                    j * groups : (j + 1) * groups, j * HEAD : (j + 1) * HEAD
                ]

    def part_copy(c):
        return peer_copy(part_send.at[c], part_recv.at[c], 2 + c)

    def project(c):
        mine = slice(c * chunk, (c + 1) * chunk)
        attended = jnp.concatenate([att_ref[mine, h, :] for h in range(groups)], axis=1)
        part = dot(attended.astype(BF16), wo[...]).astype(BF16)
        part_send[c, 0] = part[:, :half]
        part_send[c, 1] = part[:, half:]
        part_copy(c).start()

    def rows_copy(to, c):
        return pltpu.make_async_remote_copy(
            src_ref=rows_ref.at[c],
            dst_ref=rows_recv.at[level, c],
            send_sem=rows_send_sem.at[to, c],
            recv_sem=rows_recv_sem.at[level, c],
            device_id=(to * plane + spot, tp),
            device_id_type=MESH,
        )

    def relay_copy(c):
        far = partners[1]
        return pltpu.make_async_remote_copy(
            src_ref=rows_recv.at[far, c],
            dst_ref=rows_recv.at[far, c],
            send_sem=relay_sem.at[c],
            recv_sem=rows_recv_sem.at[far, c],
            device_id=(partners[2] * plane + spot, tp),
            device_id_type=MESH,
        )

    def rows_arrival(i, c):
        source = partners[i]
        return pltpu.make_async_remote_copy(
            src_ref=rows_ref.at[c],
            dst_ref=rows_recv.at[source, c],
            send_sem=rows_send_sem.at[source, c],
            recv_sem=rows_recv_sem.at[source, c],
            device_id=(source * plane + spot, tp),
            device_id_type=MESH,
        )

    def settle(c):
        at = slice(c * chunk, (c + 1) * chunk)
        part_copy(c).wait()
        res_own = (
            x_own[at, :].astype(F32)
            + (part_send[c, tp].astype(F32) + part_recv[c, tp].astype(F32))
        ).astype(BF16)
        res_other = (
            x_peer[at, :].astype(F32)
            + (part_send[c, other].astype(F32) + part_recv[c, other].astype(F32))
        ).astype(BF16)
        res_ref[at, :] = res_own
        mine = res_own.astype(F32)
        mean, scale = stats(mine, res_other.astype(F32))
        rows_ref[c] = ((mine - mean) * scale * g2[...]).astype(BF16)
        if planes > 1:
            rows_copy(partners[1], c).start()

            @pl.when(inner == 1)
            def _():
                rows_copy(partners[3], c).start()

            rows_copy(partners[2], c).start()

    loads[5].wait()
    for c in range(CHUNKS):
        score(c)
        spend(c)
        if c == 0:
            loads[6].wait()
            for i in (11, 12, 13):
                loads[i].start()
            loads[7].wait()
            loads[8].wait()
            tok_copy.wait()
        else:
            settle(c - 1)
        read(c)
        project(c)
    for k in range(planes):
        if k > 0:
            route_copy(k, False).wait_recv()
        make_tables(k)
    settle(CHUNKS - 1)

    def beside_copy(src, dst, send_sem, recv_sem, j):
        to = lax.rem(spot + j, plane)
        return pltpu.make_async_remote_copy(
            src_ref=src(to),
            dst_ref=dst(spot),
            send_sem=send_sem,
            recv_sem=recv_sem,
            device_id=(level * plane + to, tp),
            device_id_type=MESH,
        )

    def disp_copy(k, j):
        return beside_copy(
            lambda to: disp.at[k, to],
            lambda giver: recv_own.at[k, giver],
            disp_send_sem.at[k],
            disp_recv_sem.at[k],
            j,
        )

    def disp_all(k):
        return pltpu.make_async_remote_copy(
            src_ref=disp.at[k, pl.ds(0, plane - 1)],
            dst_ref=recv_own.at[k, pl.ds(0, plane - 1)],
            send_sem=disp_send_sem.at[k],
            recv_sem=disp_recv_sem.at[k],
            device_id=(ep, other),
            device_id_type=MESH,
        )

    def disp_keep(k):
        return pltpu.make_async_copy(disp.at[k, spot], recv_own.at[k, spot], local_sem.at[k])

    def fwd_copy(k):
        return pltpu.make_async_remote_copy(
            src_ref=recv_own.at[k],
            dst_ref=recv_peer.at[k],
            send_sem=fwd_send_sem.at[k],
            recv_sem=fwd_recv_sem.at[k],
            device_id=(ep, other),
            device_id_type=MESH,
        )

    def place_rows(k):
        if k > 0:
            rows = rows_recv[partners[k]].reshape(seqs, half)
        else:
            rows = rows_ref[...].reshape(seqs, half)
        placed = dot(tables[k, 0], rows).astype(BF16)
        disp[k] = placed.reshape(plane, cap, half)
        for j in range(1, plane):
            disp_copy(k, j).start()
        disp_keep(k).start()

    def receive_rows(k):
        for c in range(CHUNKS):
            rows_arrival(k, c).wait_recv()

    def gather(k):
        disp_keep(k).wait()
        disp_all(k).wait_recv()
        fwd_copy(k).start()

    hidden = gate.shape[1]
    own_depth = pl.ds(pl.multiple_of(tp * half, half), half)
    peer_depth = pl.ds(pl.multiple_of(other * half, half), half)
    def blocks_of(team):
        count = len(team) * group
        size = min(count, 256)
        return [slice(i * size, (i + 1) * size) for i in range(count // size)]

    def rows_of(ref, team, at):
        rows = ref[team[0] : team[-1] + 1].reshape(len(team) * plane, cap, half)
        return rows[at.start // cap : at.stop // cap].reshape(at.stop - at.start, half)

    def swiglu(g, u):
        c = jnp.minimum(g, SWIGLU_LIMIT)
        linear = jnp.clip(u, -SWIGLU_LIMIT, SWIGLU_LIMIT)
        return (c * jax.nn.sigmoid(SWIGLU_ALPHA * c) * (linear + 1.0)).astype(BF16)

    def first_half(team):
        def body(i, carry):
            cols = pl.ds(pl.multiple_of(i * GATE_BLOCK, GATE_BLOCK), GATE_BLOCK)
            for at in blocks_of(team):
                rows = rows_of(recv_own, team, at)
                gate_acc[at, cols] = dot(rows, gate[own_depth, cols])
                up_acc[at, cols] = dot(rows, up[own_depth, cols])
            return carry

        lax.fori_loop(0, hidden // GATE_BLOCK, body, 0)

    def second_half(team):
        def body(i, carry):
            cols = pl.ds(pl.multiple_of(i * GATE_BLOCK, GATE_BLOCK), GATE_BLOCK)
            for at in blocks_of(team):
                rows = rows_of(recv_peer, team, at)
                g = gate_acc[at, cols] + dot(rows, gate[peer_depth, cols])
                u = up_acc[at, cols] + dot(rows, up[peer_depth, cols])
                act_ref[at, cols] = swiglu(g, u)
            return carry

        lax.fori_loop(0, hidden // GATE_BLOCK, body, 0)

    def whole_depth(team):
        def body(i, carry):
            cols = pl.ds(pl.multiple_of(i * GATE_BLOCK, GATE_BLOCK), GATE_BLOCK)
            for at in blocks_of(team):
                mine = rows_of(recv_own, team, at)
                theirs = rows_of(recv_peer, team, at)
                g = dot(mine, gate[own_depth, cols]) + dot(theirs, gate[peer_depth, cols])
                u = dot(mine, up[own_depth, cols]) + dot(theirs, up[peer_depth, cols])
                act_ref[at, cols] = swiglu(g, u)
            return carry

        lax.fori_loop(0, hidden // GATE_BLOCK, body, 0)

    tiles = half // COL_BLOCK
    all_tiles = pl.ds(0, tiles)
    one_tile = [pl.ds(t, 1) for t in range(tiles)]

    def down_copy(p, at):
        team = teams[p]
        ks = pl.ds(team[0], len(team))
        return pltpu.make_async_remote_copy(
            src_ref=down_send.at[at, ks],
            dst_ref=down_recv.at[at, ks],
            send_sem=down_send_sem.at[p, at.start // at.size],
            recv_sem=down_recv_sem.at[p, at.start // at.size],
            device_id=(ep, other),
            device_id_type=MESH,
        )

    def down_tile(ref, p, side, t):
        team = teams[p]
        cols = pl.ds(pl.multiple_of(side * half + t * COL_BLOCK, COL_BLOCK), COL_BLOCK)
        for at in blocks_of(team):
            value = dot(act_ref[at, :], down[:, cols]).astype(BF16)
            size = at.stop - at.start
            if size <= group:
                k, begin = team[0] + at.start // group, at.start % group
                ref[t, k, begin : begin + size, :] = value
            else:
                k = team[0] + at.start // group
                ref[t, k : k + size // group] = value.reshape(size // group, group, COL_BLOCK)

    def down_other(p, parts):
        for at in parts:
            for t in range(at.start, at.start + at.size):
                down_tile(down_send, p, other, t)
            down_copy(p, at).start()

    def back_copy(k, at, j):
        return beside_copy(
            lambda to: back_send.at[k, to, at],
            lambda giver: back_recv.at[k, giver, at],
            back_send_sem.at[k],
            back_recv_sem.at[k, at.start // at.size],
            j,
        )

    def back_all(k, at):
        return pltpu.make_async_remote_copy(
            src_ref=back_send.at[k, pl.ds(0, plane - 1), at],
            dst_ref=back_recv.at[k, pl.ds(0, plane - 1), at],
            send_sem=back_send_sem.at[k],
            recv_sem=back_recv_sem.at[k, at.start // at.size],
            device_id=(ep, other),
            device_id_type=MESH,
        )

    def back_keep(k, at):
        return pltpu.make_async_copy(
            back_send.at[k, spot, at],
            back_recv.at[k, spot, at],
            back_local_sem.at[k, at.start // at.size],
        )

    def send_back(k, at):
        for j in range(1, plane):
            back_copy(k, at, j).start()
        back_keep(k, at).start()

    def down_join(p, t):
        for k in teams[p]:
            total = (down_own[t, k].astype(F32) + down_recv[t, k].astype(F32)).astype(BF16)
            back_send[k, :, t] = total.reshape(plane, cap, COL_BLOCK)

    def down_mine(p):
        for t in range(tiles):
            down_tile(down_own, p, tp, t)

    def join_whole(p):
        down_copy(p, all_tiles).wait()
        for t in range(tiles):
            down_join(p, t)
        for k in teams[p]:
            send_back(k, all_tiles)

    def join_tiles(p):
        for t in range(tiles):
            down_tile(down_own, p, tp, t)
            down_copy(p, one_tile[t]).wait()
            down_join(p, t)
            send_back(teams[p][-1], one_tile[t])
        for k in reversed(teams[p][:-1]):
            for t in range(tiles):
                send_back(k, one_tile[t])

    def sum_copy(k, t):
        to = partners[k]
        return pltpu.make_async_remote_copy(
            src_ref=sum_send.at[to, t],
            dst_ref=sum_recv.at[level, t],
            send_sem=sum_send_sem.at[to, t],
            recv_sem=sum_recv_sem.at[level, t],
            device_id=(to * plane + spot, tp),
            device_id_type=MESH,
        )

    def sum_arrival(k, t):
        source = partners[k]
        return pltpu.make_async_remote_copy(
            src_ref=sum_send.at[source, t],
            dst_ref=sum_recv.at[source, t],
            send_sem=sum_send_sem.at[source, t],
            recv_sem=sum_recv_sem.at[source, t],
            device_id=(source * plane + spot, tp),
            device_id_type=MESH,
        )

    over_slots = (((0,), (0,)), ((), ()))

    def combine(k, at):
        back_keep(k, at).wait()
        back_all(k, at).wait_recv()
        to = partners[k]
        mixes = []
        for t in range(at.start, at.start + at.size):
            back = back_recv[k, :, t].reshape(group, COL_BLOCK)
            mixes.append(
                lax.dot_general(tables[k, 1], back, over_slots, preferred_element_type=F32)
                + lax.dot_general(tables[k, 2], back, over_slots, preferred_element_type=F32)
            )
        for t, mixed in zip(range(at.start, at.start + at.size), mixes):
            cols = slice(t * COL_BLOCK, (t + 1) * COL_BLOCK)
            if k == 0:
                total_ref[:, cols] = res_ref[:, cols].astype(F32) + mixed
            else:
                sum_send[to, t] = mixed.astype(BF16)
        if k > 0:
            for t in range(at.start, at.start + at.size):
                sum_copy(k, t).start()

    def run_far():
        whole_depth(teams[2])
        down_other(2, one_tile)
        join_tiles(2)

    place_rows(0)
    if planes > 1:
        receive_rows(1)

        @pl.when(inner == 1)
        def _():
            for c in range(CHUNKS):
                relay_copy(c).start()

        place_rows(1)
    gather(0)
    if planes > 1:
        receive_rows(2)
        place_rows(2)
    for i in (11, 12, 13):
        loads[i].wait()
    fwd_copy(0).wait()
    whole_depth(teams[0])
    down_other(0, [all_tiles])
    if planes > 1:
        receive_rows(3)
        place_rows(3)
    down_mine(0)
    join_whole(0)
    if planes > 1:
        gather(1)
        first_half(teams[1])
        fwd_copy(1).wait()
        second_half(teams[1])
        down_other(1, [all_tiles])
        gather(2)
        gather(3)
        down_mine(1)
        join_whole(1)
        fwd_copy(2).wait()
        fwd_copy(3).wait()
        run_far()
        for i in range(1, planes):
            route_copy(i, True).wait_send()
        for c in range(CHUNKS):
            rows_copy(partners[1], c).wait_send()
            rows_copy(partners[2], c).wait_send()

        @pl.when(inner == 1)
        def _():
            for c in range(CHUNKS):
                rows_copy(partners[3], c).wait_send()
                relay_copy(c).wait_send()

    for k in range(planes):
        disp_all(k).wait_send()
    for k in (1, 0) if planes > 1 else (0,):
        combine(k, all_tiles)
        back_all(k, all_tiles).wait_send()
    if planes > 1:
        for k in (3, 2):
            for t in range(tiles):
                combine(k, one_tile[t])
        for k in (3, 2):
            back_all(k, all_tiles).wait_send()
    for k in eager:
        for t in range(tiles):
            sum_arrival(k, t).wait_recv()
    for t in range(tiles):
        cols = slice(t * COL_BLOCK, (t + 1) * COL_BLOCK)
        total = total_ref[:, cols]
        for k in range(1, planes):
            total = total + sum_recv[partners[k], t].astype(F32)
        out_ref[:, cols] = total.astype(BF16)

    for i in range(1, planes):
        for t in range(tiles):
            sum_copy(i, t).wait_send()


def publish(*refs):
    sems = refs[-1]
    count = len(refs) // 2
    copies = []
    for i in range(count):
        copy = pltpu.make_async_copy(refs[i], refs[count + i], sems.at[i])
        copy.start()
        copies.append(copy)
    for copy in copies:
        copy.wait()


def local(
    tokens,
    norm1_gain,
    w_query,
    w_key,
    w_value,
    head_bias,
    key_cache,
    value_cache,
    seq_lengths,
    w_out,
    norm2_gain,
    route_ids,
    route_logits,
    expert_gate,
    expert_up,
    expert_down,
):
    n = lax.axis_size("ep")
    seqs, half = tokens.shape
    top = route_ids.shape[1]
    experts = n * expert_gate.shape[0]
    capacity = max(2, 2 * seqs * top // experts)
    cap = -(-capacity // 16) * 16
    planes = 4 if n % 4 == 0 else 1
    plane = n // planes
    qc = w_query.shape[1] // 2
    kcols = w_key.shape[1] // 2
    groups = qc // HEAD
    positions = key_cache.shape[1]
    hidden = expert_gate.shape[2]
    tiles = half // COL_BLOCK
    team_count = 3 if planes == 4 else 1
    most = plane * cap * (2 if planes == 4 else 1)
    keys = jnp.swapaxes(key_cache, 1, 2)
    values = jnp.swapaxes(value_cache, 1, 2)
    operands = (
        tokens,
        norm1_gain.reshape(1, -1),
        w_query,
        w_key,
        w_value,
        head_bias,
        keys,
        values,
        seq_lengths,
        w_out,
        norm2_gain.reshape(1, -1),
        route_ids.T,
        route_logits.T,
        expert_gate.reshape(expert_gate.shape[1:]),
        expert_up.reshape(expert_up.shape[1:]),
        expert_down.reshape(expert_down.shape[1:]),
    )
    in_smem = (5, 8)
    in_specs = [
        pl.BlockSpec(memory_space=pl.ANY) for i in range(len(operands))
    ]
    vmem = pl.BlockSpec(memory_space=pltpu.VMEM)
    loaded = [
        pltpu.VMEM(a.shape, a.dtype) for i, a in enumerate(operands) if i not in in_smem
    ]
    dma = pltpu.SemaphoreType.DMA
    scratch = (
        [pltpu.SMEM(operands[i].shape, operands[i].dtype) for i in in_smem]
        + [loaded[0], loaded[0]]
        + loaded[1:]
        + [
            pltpu.VMEM((seqs + PAD, qc + 2 * kcols + 2 * LANES), F32),
            pltpu.VMEM((seqs + PAD, qc + 2 * kcols + 2 * LANES), F32),
            pltpu.VMEM((seqs, groups, HEAD), F32),
            pltpu.VMEM((seqs * groups, BATCH * HEAD), BF16),
            pltpu.VMEM((seqs * groups, positions), F32),
            pltpu.VMEM((seqs * groups, positions), BF16),
            pltpu.VMEM((seqs, groups, HEAD), F32),
            pltpu.VMEM((CHUNKS, 2, seqs // CHUNKS, half), BF16),
            pltpu.VMEM((CHUNKS, 2, seqs // CHUNKS, half), BF16),
            pltpu.VMEM((seqs, half), BF16),
            pltpu.VMEM((2 * top, seqs), F32),
            pltpu.VMEM((planes, 2 * top, seqs), F32),
            pltpu.VMEM((planes, 3, plane * cap, seqs), BF16),
            pltpu.VMEM((CHUNKS, seqs // CHUNKS, half), BF16),
            pltpu.VMEM((planes, CHUNKS, seqs // CHUNKS, half), BF16),
            pltpu.VMEM((planes, plane, cap, half), BF16),
            pltpu.VMEM((planes, plane, cap, half), BF16),
            pltpu.VMEM((planes, plane, cap, half), BF16),
            pltpu.VMEM((most, hidden), F32),
            pltpu.VMEM((most, hidden), F32),
            pltpu.VMEM((most, hidden), BF16),
            pltpu.VMEM((tiles, planes, plane * cap, COL_BLOCK), BF16),
            pltpu.VMEM((tiles, planes, plane * cap, COL_BLOCK), BF16),
            pltpu.VMEM((tiles, planes, plane * cap, COL_BLOCK), BF16),
            pltpu.VMEM((planes, plane, tiles, cap, COL_BLOCK), BF16),
            pltpu.VMEM((planes, plane, tiles, cap, COL_BLOCK), BF16),
            pltpu.VMEM((planes, tiles, seqs, COL_BLOCK), BF16),
            pltpu.VMEM((planes, tiles, seqs, COL_BLOCK), BF16),
            pltpu.VMEM((seqs, half), F32),
            dma((len(operands),)),
            dma((2 + CHUNKS,)),
            dma((2 + CHUNKS,)),
            dma((planes,)),
            dma((planes,)),
            dma((planes, CHUNKS)),
            dma((planes, CHUNKS)),
            dma((CHUNKS,)),
            dma((planes, tiles)),
            dma((planes, tiles)),
            dma((planes,)),
            dma((planes,)),
            dma((planes,)),
            dma((planes,)),
            dma((team_count, tiles)),
            dma((team_count, tiles)),
            dma((planes,)),
            dma((planes, tiles)),
            dma((planes,)),
            dma((planes, tiles)),
        ]
    )
    shapes = ((seqs, half), (seqs, kcols), (seqs, kcols))
    results = pl.pallas_call(
        functools.partial(kernel, n, cap),
        out_shape=tuple(pltpu.VMEM(shape, BF16) for shape in shapes),
        in_specs=in_specs,
        out_specs=(vmem, vmem, vmem),
        scratch_shapes=scratch,
        compiler_params=pltpu.CompilerParams(
            collective_id=0, has_side_effects=True, vmem_limit_bytes=VMEM_BYTES
        ),
    )(*operands)
    return pl.pallas_call(
        publish,
        out_shape=tuple(jax.ShapeDtypeStruct(shape, BF16) for shape in shapes),
        in_specs=[vmem] * len(shapes),
        out_specs=tuple([pl.BlockSpec(memory_space=pl.ANY)] * len(shapes)),
        scratch_shapes=[dma((len(shapes),))],
    )(*(pltpu.with_memory_space_constraint(r, pltpu.VMEM) for r in results))


def solution(mesh):
    in_specs = (
        P("ep", "tp"),
        P("tp"),
        P("tp", None),
        P("tp", None),
        P("tp", None),
        P("tp"),
        P("ep", None, "tp"),
        P("ep", None, "tp"),
        P("ep"),
        P("tp", None),
        P("tp"),
        P("ep", None),
        P("ep", None),
        P("ep", None, "tp"),
        P("ep", None, "tp"),
        P("ep", "tp", None),
    )
    out_specs = (P("ep", "tp"), P("ep", "tp"), P("ep", "tp"))
    return jax.shard_map(local, mesh=mesh, in_specs=in_specs, out_specs=out_specs, check_vma=False)
```

```python
import functools

import jax
import jax.numpy as jnp
from jax import lax
from jax.experimental import pallas as pl
from jax.experimental.pallas import tpu as pltpu
from jax.sharding import PartitionSpec as P

HEAD = 64
LN_EPS = 1e-05
SWIGLU_ALPHA = 1.702
SWIGLU_LIMIT = 7.0
MESH = pl.DeviceIdType.MESH
F32 = jnp.float32
BF16 = jnp.bfloat16
DEAD = -1e30
POS_BLOCK = 256
COL_BLOCK = 512
GATE_BLOCK = 512
PAD = 16
BATCH = 4
CHUNKS = 2
VMEM_BYTES = 63 * 1024 * 1024
LANES = 128


def dot(a, b):
    return jnp.dot(a, b, preferred_element_type=F32)


def kernel(
    n,
    cap,
    tok_hbm,
    g1_hbm,
    wq_hbm,
    wk_hbm,
    wv_hbm,
    bias_hbm,
    kc_hbm,
    vc_hbm,
    lens_hbm,
    wo_hbm,
    g2_hbm,
    ids_hbm,
    logits_hbm,
    gate_hbm,
    up_hbm,
    down_hbm,
    out_ref,
    nk_ref,
    nv_ref,
    bias_ref,
    lens_ref,
    x_own,
    x_peer,
    g1,
    wq,
    wk,
    wv,
    kc,
    vc,
    wo,
    g2,
    ids,
    logits,
    gate,
    up,
    down,
    proj_send,
    proj_recv,
    q_rows,
    q_wide,
    z_ref,
    w_ref,
    att_ref,
    part_send,
    part_recv,
    res_ref,
    route_send,
    route_recv,
    tables,
    rows_ref,
    rows_recv,
    disp,
    recv_own,
    recv_peer,
    gate_acc,
    up_acc,
    act_ref,
    down_send,
    down_recv,
    down_own,
    back_send,
    back_recv,
    sum_send,
    sum_recv,
    total_ref,
    load_sem,
    one_send,
    one_recv,
    route_send_sem,
    route_recv_sem,
    rows_send_sem,
    rows_recv_sem,
    sum_send_sem,
    sum_recv_sem,
    disp_send_sem,
    disp_recv_sem,
    fwd_send_sem,
    fwd_recv_sem,
    down_send_sem,
    down_recv_sem,
    back_send_sem,
    back_recv_sem,
):
    ep = lax.axis_index("ep")
    tp = lax.axis_index("tp")
    other = 1 - tp
    seqs, half = x_own.shape
    width = 2 * half

    loads = []
    pairs = (
        (tok_hbm, x_own),
        (g1_hbm, g1),
        (wq_hbm, wq),
        (wk_hbm, wk),
        (wv_hbm, wv),
        (kc_hbm, kc),
        (vc_hbm, vc),
        (wo_hbm, wo),
        (g2_hbm, g2),
        (ids_hbm, ids),
        (logits_hbm, logits),
        (gate_hbm, gate),
        (up_hbm, up),
        (down_hbm, down),
        (bias_hbm, bias_ref),
        (lens_hbm, lens_ref),
    )
    for i, (src, dst) in enumerate(pairs):
        slot = (10, 11, 12, 11, 12)[i - 11] if i > 10 else i
        loads.append(pltpu.make_async_copy(src, dst, load_sem.at[slot]))
    for i in (0, 1, 2, 3, 4, 14, 15, 9, 10, 8, 5, 6, 7):
        loads[i].start()

    def tally(ref, sem):
        return pltpu.make_async_remote_copy(
            src_ref=ref,
            dst_ref=ref,
            send_sem=sem,
            recv_sem=sem,
            device_id=(ep, other),
            device_id_type=MESH,
        )

    def peer_copy(src, dst, i):
        return pltpu.make_async_remote_copy(
            src_ref=src,
            dst_ref=dst,
            send_sem=one_send.at[min(i, 1)],
            recv_sem=one_recv.at[i],
            device_id=(ep, other),
            device_id_type=MESH,
        )

    barrier = pltpu.get_barrier_semaphore()
    pl.semaphore_signal(barrier, inc=1, device_id=(ep, other), device_id_type=MESH)

    planes = tables.shape[0]
    plane = n // planes
    level = ep // plane
    spot = ep % plane

    def column(i):
        return lax.rem(level + i, planes) * plane + spot

    def beside(i):
        return level * plane + lax.rem(spot + i, plane)

    if planes == 4:
        inner = lax.rem((level + 1) // 2, 2)
        partners = (
            level,
            lax.rem(level + 2, 4),
            level + 1 - 2 * lax.rem(level, 2),
            3 - level,
        )
        teams = ((0,), (1,), (2, 3))
        eager = (1, 3, 2)
    else:
        partners = (level,)
        inner = 0
        teams = ((0,),)
        eager = ()

    def greet_column(i, carry):
        pl.semaphore_signal(barrier, inc=1, device_id=(column(i), tp), device_id_type=MESH)
        return carry

    def greet_beside(i, carry):
        pl.semaphore_signal(barrier, inc=1, device_id=(beside(i), tp), device_id_type=MESH)
        return carry

    lax.fori_loop(1, planes, greet_column, 0)
    lax.fori_loop(1, plane, greet_beside, 0)
    loads[0].wait()
    loads[1].wait()
    mine = x_own[...].astype(F32)
    mean_own = jnp.sum(mine, axis=1, keepdims=True) / half
    centred = mine - mean_own
    square_own = jnp.sum(centred * centred, axis=1, keepdims=True)
    gain = g1[...]
    gain_hi = gain.astype(BF16)
    gain_lo = (gain - gain_hi.astype(F32)).astype(BF16)
    pad_row = lax.broadcasted_iota(jnp.int32, (PAD, half), 0)
    gains = jnp.where(
        pad_row == 0, gain_hi.astype(F32), jnp.where(pad_row == 1, gain_lo.astype(F32), 0.0)
    )
    stacked = jnp.concatenate([centred * gain, gains], axis=0).astype(BF16)
    for i in (2, 3, 4):
        loads[i].wait()
    pq = dot(stacked, wq[...])
    pk = dot(stacked, wk[...])
    pv = dot(stacked, wv[...])
    qc = pq.shape[1] // 2
    kcols = pk.shape[1] // 2
    first = tp == 0
    used = qc + 2 * kcols
    proj_send[:, :qc] = jnp.where(first, pq[:, qc:], pq[:, :qc])
    proj_send[:, qc : qc + kcols] = jnp.where(first, pk[:, kcols:], pk[:, :kcols])
    proj_send[:, qc + kcols : used] = jnp.where(first, pv[:, kcols:], pv[:, :kcols])
    proj_send[:seqs, used : used + LANES] = jnp.broadcast_to(mean_own, (seqs, LANES))
    proj_send[:seqs, used + LANES :] = jnp.broadcast_to(square_own, (seqs, LANES))
    pl.semaphore_wait(barrier, planes + plane - 1)

    proj_copy = peer_copy(proj_send, proj_recv, 1)
    proj_copy.start()
    loads[9].wait()
    loads[10].wait()
    top = ids.shape[0]
    route_send[:top] = ids[...].astype(F32)
    route_send[top:] = logits[...]

    def route_copy(i):
        to = partners[i]
        return pltpu.make_async_remote_copy(
            src_ref=route_send,
            dst_ref=route_recv.at[level],
            send_sem=route_send_sem.at[0],
            recv_sem=route_recv_sem.at[0],
            device_id=(to * plane + spot, tp),
            device_id_type=MESH,
        )

    for i in eager:
        route_copy(i).start()
    tok_copy = peer_copy(x_own, x_peer, 0)
    tok_copy.start()

    def stats(a, b):
        total = jnp.sum(a, axis=1, keepdims=True) + jnp.sum(b, axis=1, keepdims=True)
        square = jnp.sum(a * a, axis=1, keepdims=True) + jnp.sum(b * b, axis=1, keepdims=True)
        mean = total / width
        return mean, lax.rsqrt(square / width - mean * mean + LN_EPS)

    group = plane * cap
    slot_row = lax.broadcasted_iota(jnp.int32, (group, seqs), 0)
    slot_expert = slot_row // cap
    slot_rank = (slot_row - slot_expert * cap).astype(F32)
    slot_expert = (slot_expert + level * plane).astype(F32)
    earlier = (
        lax.broadcasted_iota(jnp.int32, (seqs, seqs), 0)
        < lax.broadcasted_iota(jnp.int32, (seqs, seqs), 1)
    )
    earlier = jnp.where(earlier, 1.0, 0.0).astype(BF16)

    def make_tables(k):
        route = route_send[...] if k == 0 else route_recv[partners[k]]
        raw = jnp.exp(route[top:])
        probs = raw / jnp.sum(raw, axis=0, keepdims=True)
        hot = jnp.zeros((group, seqs), F32)
        prob_hot = jnp.zeros((group, seqs), F32)
        for i in range(top):
            match = jnp.abs(route[i : i + 1] - slot_expert) < 0.5
            hot = hot + jnp.where(match, 1.0, 0.0)
            prob_hot = prob_hot + jnp.where(match, probs[i : i + 1, :], 0.0)
        rank = dot(hot.astype(BF16), earlier)
        chosen = (hot > 0.5) & (jnp.abs(rank - slot_rank) < 0.5)
        weight = jnp.where(chosen, prob_hot, 0.0)
        weight_hi = weight.astype(BF16)
        tables[k, 0] = jnp.where(chosen, 1.0, 0.0).astype(BF16)
        tables[k, 1] = weight_hi
        tables[k, 2] = (weight - weight_hi.astype(F32)).astype(BF16)

    groups = qc // HEAD
    loads[14].wait()
    loads[15].wait()
    bias = jnp.zeros((groups, 1), F32)
    head_row = lax.broadcasted_iota(jnp.int32, (groups, 1), 0)
    for h in range(groups):
        bias = bias + jnp.where(head_row == h, bias_ref[h], 0.0)

    own_q = jnp.where(first, pq[:, :qc], pq[:, qc:])
    own_k = jnp.where(first, pk[:, :kcols], pk[:, kcols:])
    own_v = jnp.where(first, pv[:, :kcols], pv[:, kcols:])
    proj_copy.wait()
    mean_peer = proj_recv[:seqs, used : used + 1]
    square_peer = proj_recv[:seqs, used + LANES : used + LANES + 1]
    apart = (mean_own - mean_peer) * 0.5
    scale = lax.rsqrt((square_own + square_peer) / width + apart * apart + LN_EPS)

    def joined(own, lo, hi):
        tilt = (own[seqs : seqs + 1] + own[seqs + 1 : seqs + 2]) - (
            proj_recv[seqs : seqs + 1, lo:hi] + proj_recv[seqs + 1 : seqs + 2, lo:hi]
        )
        return (scale * (own[:seqs] + proj_recv[:seqs, lo:hi] + apart * tilt)).astype(BF16)

    query = joined(own_q, 0, qc).astype(F32)
    nk_ref[...] = joined(own_k, qc, qc + kcols)
    nv_ref[...] = joined(own_v, qc + kcols, used)
    for h in range(groups):
        q_rows[:, h, :] = query[:, h * HEAD : (h + 1) * HEAD]
    flat = q_rows[...].reshape(seqs * groups, HEAD).astype(BF16)
    wide_row = lax.broadcasted_iota(jnp.int32, (seqs * groups, BATCH * HEAD), 0)
    wide_col = lax.broadcasted_iota(jnp.int32, (seqs * groups, BATCH * HEAD), 1)
    q_wide[...] = jnp.where(
        lax.rem(wide_row // groups, BATCH) == wide_col // HEAD,
        jnp.concatenate([flat] * BATCH, axis=1),
        jnp.zeros((), BF16),
    )

    positions = kc.shape[2]
    after = (
        lax.broadcasted_iota(jnp.int32, (POS_BLOCK, POS_BLOCK), 0)
        > lax.broadcasted_iota(jnp.int32, (POS_BLOCK, POS_BLOCK), 1)
    )
    after = jnp.where(after, 1.0, 0.0).astype(BF16)
    chunk = seqs // CHUNKS
    step_rows = BATCH * groups
    place = lax.broadcasted_iota(jnp.int32, (step_rows, positions), 1)
    step_seq = lax.broadcasted_iota(jnp.int32, (step_rows, 1), 0) // groups
    step_bias = jnp.concatenate([bias] * BATCH, axis=0)

    def score(c):
        for i in range(c * chunk // BATCH, (c + 1) * chunk // BATCH):
            rows = slice(i * step_rows, (i + 1) * step_rows)
            keys = kc[i * BATCH : (i + 1) * BATCH].reshape(BATCH * HEAD, positions)
            length = jnp.zeros((step_rows, 1), jnp.int32)
            for j in range(BATCH):
                length = jnp.where(step_seq == j, lens_ref[i * BATCH + j], length)
            s = dot(q_wide[rows, :], keys) * HEAD ** (-0.5) + step_bias
            z_ref[rows, :] = jnp.where(place < length, s, DEAD)

    def spend(c):
        count = chunk * groups
        rows = slice(c * count, (c + 1) * count)
        beyond = jnp.zeros((count, 1), F32)
        for b in reversed(range(positions // POS_BLOCK)):
            cols = slice(b * POS_BLOCK, (b + 1) * POS_BLOCK)
            z = z_ref[rows, cols]
            tail = jnp.log(1.0 + jnp.exp(-jnp.abs(z)))
            spent = jnp.maximum(z, 0.0) + tail
            hi = spent.astype(BF16)
            lo = (spent - hi.astype(F32)).astype(BF16)
            sums = dot(jnp.concatenate([hi, lo], axis=0), after)
            inside = sums[:count] + sums[count:]
            w_ref[rows, cols] = jnp.exp(
                jnp.minimum(z, 0.0) - tail - (inside + beyond)
            ).astype(BF16)
            beyond = beyond + inside[:, :1] + spent[:, :1]

    def read(c):
        for i in range(c * chunk // BATCH, (c + 1) * chunk // BATCH):
            weights = w_ref[i * step_rows : (i + 1) * step_rows, :]
            values = vc[i * BATCH : (i + 1) * BATCH].reshape(BATCH * HEAD, positions)
            mixed = lax.dot_general(
                weights, values, (((1,), (1,)), ((), ())), preferred_element_type=F32
            )
            for j in range(BATCH):
                att_ref[i * BATCH + j] = mixed[
                    j * groups : (j + 1) * groups, j * HEAD : (j + 1) * HEAD
                ]

    def part_copy(c):
        return peer_copy(part_send.at[c], part_recv.at[c], 2 + c)

    def project(c):
        mine = slice(c * chunk, (c + 1) * chunk)
        attended = jnp.concatenate([att_ref[mine, h, :] for h in range(groups)], axis=1)
        part = dot(attended.astype(BF16), wo[...]).astype(BF16)
        part_send[c, 0] = part[:, :half]
        part_send[c, 1] = part[:, half:]
        part_copy(c).start()

    def rows_copy(to, c):
        return pltpu.make_async_remote_copy(
            src_ref=rows_ref.at[c],
            dst_ref=rows_recv.at[level, c],
            send_sem=rows_send_sem.at[0],
            recv_sem=rows_recv_sem.at[level],
            device_id=(to * plane + spot, tp),
            device_id_type=MESH,
        )

    def relay_copy(c):
        far = partners[1]
        return pltpu.make_async_remote_copy(
            src_ref=rows_recv.at[far, c],
            dst_ref=rows_recv.at[far, c],
            send_sem=rows_send_sem.at[0],
            recv_sem=rows_recv_sem.at[far],
            device_id=(partners[2] * plane + spot, tp),
            device_id_type=MESH,
        )

    def settle(c):
        at = slice(c * chunk, (c + 1) * chunk)
        part_copy(c).wait()
        res_own = (
            x_own[at, :].astype(F32)
            + (part_send[c, tp].astype(F32) + part_recv[c, tp].astype(F32))
        ).astype(BF16)
        res_other = (
            x_peer[at, :].astype(F32)
            + (part_send[c, other].astype(F32) + part_recv[c, other].astype(F32))
        ).astype(BF16)
        res_ref[at, :] = res_own
        mine = res_own.astype(F32)
        mean, scale = stats(mine, res_other.astype(F32))
        rows_ref[c] = ((mine - mean) * scale * g2[...]).astype(BF16)
        if planes > 1:
            rows_copy(partners[1], c).start()

            @pl.when(inner == 1)
            def _():
                rows_copy(partners[3], c).start()

            rows_copy(partners[2], c).start()

    loads[5].wait()
    for c in range(CHUNKS):
        score(c)
        spend(c)
        if c == 0:
            loads[6].wait()
            for i in (11, 12, 13):
                loads[i].start()
            loads[7].wait()
            loads[8].wait()
            tok_copy.wait()
        else:
            settle(c - 1)
        read(c)
        project(c)
    for k in range(planes):
        if k == 1:
            tally(route_recv.at[pl.ds(0, planes - 1)], route_recv_sem.at[0]).wait_recv()
        make_tables(k)
    settle(CHUNKS - 1)

    def beside_copy(src, dst, send_sem, recv_sem, j):
        to = lax.rem(spot + j, plane)
        return pltpu.make_async_remote_copy(
            src_ref=src(to),
            dst_ref=dst(spot),
            send_sem=send_sem,
            recv_sem=recv_sem,
            device_id=(level * plane + to, tp),
            device_id_type=MESH,
        )

    def disp_copy(k, j):
        return beside_copy(
            lambda to: disp.at[k, to],
            lambda giver: recv_own.at[k, giver],
            disp_send_sem.at[0],
            disp_recv_sem.at[k],
            j,
        )

    def disp_keep(k):
        return pltpu.make_async_copy(disp.at[k, spot], recv_own.at[k, spot], load_sem.at[k])

    def fwd_copy(k):
        return pltpu.make_async_remote_copy(
            src_ref=recv_own.at[k],
            dst_ref=recv_peer.at[k],
            send_sem=fwd_send_sem.at[0],
            recv_sem=fwd_recv_sem.at[k],
            device_id=(ep, other),
            device_id_type=MESH,
        )

    def place_rows(k):
        if k > 0:
            rows = rows_recv[partners[k]].reshape(seqs, half)
        else:
            rows = rows_ref[...].reshape(seqs, half)
        placed = dot(tables[k, 0], rows).astype(BF16)
        disp[k] = placed.reshape(plane, cap, half)
        for j in range(1, plane):
            disp_copy(k, j).start()
        disp_keep(k).start()

    def receive_rows(k):
        source = partners[k]
        tally(rows_recv.at[source], rows_recv_sem.at[source]).wait_recv()

    def gather(k):
        disp_keep(k).wait()
        tally(recv_own.at[k, pl.ds(0, plane - 1)], disp_recv_sem.at[k]).wait_recv()
        fwd_copy(k).start()

    hidden = gate.shape[1]
    own_depth = pl.ds(pl.multiple_of(tp * half, half), half)
    peer_depth = pl.ds(pl.multiple_of(other * half, half), half)
    def blocks_of(team):
        count = len(team) * group
        size = min(count, 256)
        return [slice(i * size, (i + 1) * size) for i in range(count // size)]

    def rows_of(ref, team, at):
        rows = ref[team[0] : team[-1] + 1].reshape(len(team) * plane, cap, half)
        return rows[at.start // cap : at.stop // cap].reshape(at.stop - at.start, half)

    def swiglu(g, u):
        c = jnp.minimum(g, SWIGLU_LIMIT)
        linear = jnp.clip(u, -SWIGLU_LIMIT, SWIGLU_LIMIT)
        return (c * jax.nn.sigmoid(SWIGLU_ALPHA * c) * (linear + 1.0)).astype(BF16)

    def first_half(team):
        def body(i, carry):
            cols = pl.ds(pl.multiple_of(i * GATE_BLOCK, GATE_BLOCK), GATE_BLOCK)
            for at in blocks_of(team):
                rows = rows_of(recv_own, team, at)
                gate_acc[at, cols] = dot(rows, gate[own_depth, cols])
                up_acc[at, cols] = dot(rows, up[own_depth, cols])
            return carry

        lax.fori_loop(0, hidden // GATE_BLOCK, body, 0)

    def second_half(team):
        def body(i, carry):
            cols = pl.ds(pl.multiple_of(i * GATE_BLOCK, GATE_BLOCK), GATE_BLOCK)
            for at in blocks_of(team):
                rows = rows_of(recv_peer, team, at)
                g = gate_acc[at, cols] + dot(rows, gate[peer_depth, cols])
                u = up_acc[at, cols] + dot(rows, up[peer_depth, cols])
                act_ref[at, cols] = swiglu(g, u)
            return carry

        lax.fori_loop(0, hidden // GATE_BLOCK, body, 0)

    def whole_depth(team):
        def body(i, carry):
            cols = pl.ds(pl.multiple_of(i * GATE_BLOCK, GATE_BLOCK), GATE_BLOCK)
            for at in blocks_of(team):
                mine = rows_of(recv_own, team, at)
                theirs = rows_of(recv_peer, team, at)
                g = dot(mine, gate[own_depth, cols]) + dot(theirs, gate[peer_depth, cols])
                u = dot(mine, up[own_depth, cols]) + dot(theirs, up[peer_depth, cols])
                act_ref[at, cols] = swiglu(g, u)
            return carry

        lax.fori_loop(0, hidden // GATE_BLOCK, body, 0)

    tiles = half // COL_BLOCK
    all_tiles = pl.ds(0, tiles)
    one_tile = [pl.ds(t, 1) for t in range(tiles)]

    def down_copy(p, at):
        team = teams[p]
        ks = pl.ds(team[0], len(team))
        slot = p + at.start // at.size
        return pltpu.make_async_remote_copy(
            src_ref=down_send.at[at, ks],
            dst_ref=down_recv.at[at, ks],
            send_sem=down_send_sem.at[0],
            recv_sem=down_recv_sem.at[slot],
            device_id=(ep, other),
            device_id_type=MESH,
        )

    def down_tile(ref, p, side, t):
        team = teams[p]
        cols = pl.ds(pl.multiple_of(side * half + t * COL_BLOCK, COL_BLOCK), COL_BLOCK)
        for at in blocks_of(team):
            value = dot(act_ref[at, :], down[:, cols]).astype(BF16)
            size = at.stop - at.start
            if size <= group:
                k, begin = team[0] + at.start // group, at.start % group
                ref[t, k, begin : begin + size, :] = value
            else:
                k = team[0] + at.start // group
                ref[t, k : k + size // group] = value.reshape(size // group, group, COL_BLOCK)

    def down_other(p, parts):
        for at in parts:
            for t in range(at.start, at.start + at.size):
                down_tile(down_send, p, other, t)
            down_copy(p, at).start()

    def back_slot(k, at):
        return k + at.start // at.size + (tiles - 1 if k == 3 else 0)

    def back_copy(k, at, j):
        return beside_copy(
            lambda to: back_send.at[k, to, at],
            lambda giver: back_recv.at[k, giver, at],
            back_send_sem.at[0],
            back_recv_sem.at[back_slot(k, at)],
            j,
        )

    def back_keep(k, at):
        return pltpu.make_async_copy(
            back_send.at[k, spot, at],
            back_recv.at[k, spot, at],
            load_sem.at[planes + back_slot(k, at)],
        )

    def send_back(k, at):
        for j in range(1, plane):
            back_copy(k, at, j).start()
        back_keep(k, at).start()

    def down_join(p, t):
        for k in teams[p]:
            total = (down_own[t, k].astype(F32) + down_recv[t, k].astype(F32)).astype(BF16)
            back_send[k, :, t] = total.reshape(plane, cap, COL_BLOCK)

    def down_mine(p):
        for t in range(tiles):
            down_tile(down_own, p, tp, t)

    def join_whole(p):
        down_copy(p, all_tiles).wait_recv()
        for t in range(tiles):
            down_join(p, t)
        for k in teams[p]:
            send_back(k, all_tiles)

    def join_tiles(p):
        for t in range(tiles):
            down_tile(down_own, p, tp, t)
            down_copy(p, one_tile[t]).wait_recv()
            down_join(p, t)
            send_back(teams[p][-1], one_tile[t])
        for k in reversed(teams[p][:-1]):
            for t in range(tiles):
                send_back(k, one_tile[t])

    def sum_copy(k, t):
        to = partners[k]
        return pltpu.make_async_remote_copy(
            src_ref=sum_send.at[to, t],
            dst_ref=sum_recv.at[level, t],
            send_sem=sum_send_sem.at[0],
            recv_sem=sum_recv_sem.at[0],
            device_id=(to * plane + spot, tp),
            device_id_type=MESH,
        )

    over_slots = (((0,), (0,)), ((), ()))

    def combine(k, at):
        back_keep(k, at).wait()
        arrived = back_recv.at[k, pl.ds(0, plane - 1), at]
        tally(arrived, back_recv_sem.at[back_slot(k, at)]).wait_recv()
        to = partners[k]
        mixes = []
        for t in range(at.start, at.start + at.size):
            back = back_recv[k, :, t].reshape(group, COL_BLOCK)
            mixes.append(
                lax.dot_general(tables[k, 1], back, over_slots, preferred_element_type=F32)
                + lax.dot_general(tables[k, 2], back, over_slots, preferred_element_type=F32)
            )
        for t, mixed in zip(range(at.start, at.start + at.size), mixes):
            cols = slice(t * COL_BLOCK, (t + 1) * COL_BLOCK)
            if k == 0:
                total_ref[:, cols] = res_ref[:, cols].astype(F32) + mixed
            else:
                sum_send[to, t] = mixed.astype(BF16)
        if k > 0:
            for t in range(at.start, at.start + at.size):
                sum_copy(k, t).start()

    def run_far():
        whole_depth(teams[2])
        down_other(2, one_tile)
        join_tiles(2)

    place_rows(0)
    if planes > 1:
        receive_rows(1)

        @pl.when(inner == 1)
        def _():
            for c in range(CHUNKS):
                relay_copy(c).start()

        place_rows(1)
    gather(0)
    if planes > 1:
        receive_rows(2)
        place_rows(2)
    for i in (11, 12, 13):
        loads[i].wait()
    fwd_copy(0).wait_recv()
    whole_depth(teams[0])
    down_other(0, [all_tiles])
    if planes > 1:
        receive_rows(3)
        place_rows(3)
    down_mine(0)
    join_whole(0)
    if planes > 1:
        gather(1)
        first_half(teams[1])
        fwd_copy(1).wait_recv()
        second_half(teams[1])
        down_other(1, [all_tiles])
        gather(2)
        gather(3)
        down_mine(1)
        join_whole(1)
        fwd_copy(2).wait_recv()
        fwd_copy(3).wait_recv()
        run_far()
        tally(route_recv.at[pl.ds(0, planes - 1)], route_send_sem.at[0]).wait_send()

        @pl.when(inner == 1)
        def _():
            tally(rows_recv, rows_send_sem.at[0]).wait_send()

        @pl.when(inner == 0)
        def _():
            tally(rows_recv.at[pl.ds(0, 2)], rows_send_sem.at[0]).wait_send()

    tally(disp.at[:, pl.ds(0, plane - 1)], disp_send_sem.at[0]).wait_send()
    tally(recv_own, fwd_send_sem.at[0]).wait_send()
    tally(down_send, down_send_sem.at[0]).wait_send()
    for k in (1, 0) if planes > 1 else (0,):
        combine(k, all_tiles)
    if planes > 1:
        for k in (3, 2):
            for t in range(tiles):
                combine(k, one_tile[t])
    tally(back_send.at[:, pl.ds(0, plane - 1)], back_send_sem.at[0]).wait_send()
    if planes > 1:
        tally(sum_recv.at[pl.ds(0, planes - 1)], sum_recv_sem.at[0]).wait_recv()
    for t in range(tiles):
        cols = slice(t * COL_BLOCK, (t + 1) * COL_BLOCK)
        total = total_ref[:, cols]
        for k in range(1, planes):
            total = total + sum_recv[partners[k], t].astype(F32)
        out_ref[:, cols] = total.astype(BF16)

    if planes > 1:
        tally(sum_send.at[pl.ds(0, planes - 1)], sum_send_sem.at[0]).wait_send()


def publish(*refs):
    sems = refs[-1]
    count = len(refs) // 2
    copies = []
    for i in range(count):
        copy = pltpu.make_async_copy(refs[i], refs[count + i], sems.at[i])
        copy.start()
        copies.append(copy)
    for copy in copies:
        copy.wait()


def local(
    tokens,
    norm1_gain,
    w_query,
    w_key,
    w_value,
    head_bias,
    key_cache,
    value_cache,
    seq_lengths,
    w_out,
    norm2_gain,
    route_ids,
    route_logits,
    expert_gate,
    expert_up,
    expert_down,
):
    n = lax.axis_size("ep")
    seqs, half = tokens.shape
    top = route_ids.shape[1]
    experts = n * expert_gate.shape[0]
    capacity = max(2, 2 * seqs * top // experts)
    cap = -(-capacity // 16) * 16
    planes = 4 if n % 4 == 0 else 1
    plane = n // planes
    qc = w_query.shape[1] // 2
    kcols = w_key.shape[1] // 2
    groups = qc // HEAD
    positions = key_cache.shape[1]
    hidden = expert_gate.shape[2]
    tiles = half // COL_BLOCK
    team_count = 3 if planes == 4 else 1
    most = plane * cap * (2 if planes == 4 else 1)
    keys = jnp.swapaxes(key_cache, 1, 2)
    values = jnp.swapaxes(value_cache, 1, 2)
    operands = (
        tokens,
        norm1_gain.reshape(1, -1),
        w_query,
        w_key,
        w_value,
        head_bias,
        keys,
        values,
        seq_lengths,
        w_out,
        norm2_gain.reshape(1, -1),
        route_ids.T,
        route_logits.T,
        expert_gate.reshape(expert_gate.shape[1:]),
        expert_up.reshape(expert_up.shape[1:]),
        expert_down.reshape(expert_down.shape[1:]),
    )
    in_smem = (5, 8)
    in_specs = [
        pl.BlockSpec(memory_space=pl.ANY) for i in range(len(operands))
    ]
    vmem = pl.BlockSpec(memory_space=pltpu.VMEM)
    loaded = [
        pltpu.VMEM(a.shape, a.dtype) for i, a in enumerate(operands) if i not in in_smem
    ]
    dma = pltpu.SemaphoreType.DMA
    scratch = (
        [pltpu.SMEM(operands[i].shape, operands[i].dtype) for i in in_smem]
        + [loaded[0], loaded[0]]
        + loaded[1:]
        + [
            pltpu.VMEM((seqs + PAD, qc + 2 * kcols + 2 * LANES), F32),
            pltpu.VMEM((seqs + PAD, qc + 2 * kcols + 2 * LANES), F32),
            pltpu.VMEM((seqs, groups, HEAD), F32),
            pltpu.VMEM((seqs * groups, BATCH * HEAD), BF16),
            pltpu.VMEM((seqs * groups, positions), F32),
            pltpu.VMEM((seqs * groups, positions), BF16),
            pltpu.VMEM((seqs, groups, HEAD), F32),
            pltpu.VMEM((CHUNKS, 2, seqs // CHUNKS, half), BF16),
            pltpu.VMEM((CHUNKS, 2, seqs // CHUNKS, half), BF16),
            pltpu.VMEM((seqs, half), BF16),
            pltpu.VMEM((2 * top, seqs), F32),
            pltpu.VMEM((planes, 2 * top, seqs), F32),
            pltpu.VMEM((planes, 3, plane * cap, seqs), BF16),
            pltpu.VMEM((CHUNKS, seqs // CHUNKS, half), BF16),
            pltpu.VMEM((planes, CHUNKS, seqs // CHUNKS, half), BF16),
            pltpu.VMEM((planes, plane, cap, half), BF16),
            pltpu.VMEM((planes, plane, cap, half), BF16),
            pltpu.VMEM((planes, plane, cap, half), BF16),
            pltpu.VMEM((most, hidden), F32),
            pltpu.VMEM((most, hidden), F32),
            pltpu.VMEM((most, hidden), BF16),
            pltpu.VMEM((tiles, planes, plane * cap, COL_BLOCK), BF16),
            pltpu.VMEM((tiles, planes, plane * cap, COL_BLOCK), BF16),
            pltpu.VMEM((tiles, planes, plane * cap, COL_BLOCK), BF16),
            pltpu.VMEM((planes, plane, tiles, cap, COL_BLOCK), BF16),
            pltpu.VMEM((planes, plane, tiles, cap, COL_BLOCK), BF16),
            pltpu.VMEM((planes, tiles, seqs, COL_BLOCK), BF16),
            pltpu.VMEM((planes, tiles, seqs, COL_BLOCK), BF16),
            pltpu.VMEM((seqs, half), F32),
            dma((13,)),
            dma((2,)),
            dma((2 + CHUNKS,)),
            dma((1,)),
            dma((1,)),
            dma((1,)),
            dma((planes,)),
            dma((1,)),
            dma((1,)),
            dma((1,)),
            dma((planes,)),
            dma((1,)),
            dma((planes,)),
            dma((1,)),
            dma((2 + tiles,)),
            dma((1,)),
            dma((2 + 2 * tiles,)),
        ]
    )
    shapes = ((seqs, half), (seqs, kcols), (seqs, kcols))
    results = pl.pallas_call(
        functools.partial(kernel, n, cap),
        out_shape=tuple(pltpu.VMEM(shape, BF16) for shape in shapes),
        in_specs=in_specs,
        out_specs=(vmem, vmem, vmem),
        scratch_shapes=scratch,
        compiler_params=pltpu.CompilerParams(
            collective_id=0, has_side_effects=True, vmem_limit_bytes=VMEM_BYTES
        ),
    )(*operands)
    return pl.pallas_call(
        publish,
        out_shape=tuple(jax.ShapeDtypeStruct(shape, BF16) for shape in shapes),
        in_specs=[vmem] * len(shapes),
        out_specs=tuple([pl.BlockSpec(memory_space=pl.ANY)] * len(shapes)),
        scratch_shapes=[dma((len(shapes),))],
    )(*(pltpu.with_memory_space_constraint(r, pltpu.VMEM) for r in results))


def solution(mesh):
    in_specs = (
        P("ep", "tp"),
        P("tp"),
        P("tp", None),
        P("tp", None),
        P("tp", None),
        P("tp"),
        P("ep", None, "tp"),
        P("ep", None, "tp"),
        P("ep"),
        P("tp", None),
        P("tp"),
        P("ep", None),
        P("ep", None),
        P("ep", None, "tp"),
        P("ep", None, "tp"),
        P("ep", "tp", None),
    )
    out_specs = (P("ep", "tp"), P("ep", "tp"), P("ep", "tp"))
    return jax.shard_map(local, mesh=mesh, in_specs=in_specs, out_specs=out_specs, check_vma=False)
```

```python
import functools

import jax
import jax.numpy as jnp
from jax import lax
from jax.experimental import pallas as pl
from jax.experimental.pallas import tpu as pltpu
from jax.sharding import PartitionSpec as P

HEAD = 64
LN_EPS = 1e-05
SWIGLU_ALPHA = 1.702
SWIGLU_LIMIT = 7.0
MESH = pl.DeviceIdType.MESH
F32 = jnp.float32
BF16 = jnp.bfloat16
DEAD = -1e30
POS_BLOCK = 256
COL_BLOCK = 512
GATE_BLOCK = 1024
BACK_BLOCK = 256
PAD = 16
BATCH = 4
CHUNKS = 2
VMEM_BYTES = 63 * 1024 * 1024
LANES = 128


def dot(a, b):
    return jnp.dot(a, b, preferred_element_type=F32)


def kernel(
    n,
    cap,
    tok_hbm,
    g1_hbm,
    wq_hbm,
    wk_hbm,
    wv_hbm,
    bias_hbm,
    kc_hbm,
    vc_hbm,
    lens_hbm,
    wo_hbm,
    g2_hbm,
    ids_hbm,
    logits_hbm,
    gate_hbm,
    up_hbm,
    down_hbm,
    out_ref,
    nk_ref,
    nv_ref,
    bias_ref,
    lens_ref,
    x_own,
    x_peer,
    g1,
    wq,
    wk,
    wv,
    kc,
    vc,
    wo,
    g2,
    ids,
    logits,
    gate,
    up,
    down,
    proj_send,
    proj_recv,
    q_rows,
    q_wide,
    z_ref,
    w_ref,
    att_ref,
    part_send,
    part_recv,
    res_ref,
    route_send,
    route_recv,
    tables,
    mixing,
    rows_ref,
    rows_recv,
    disp,
    recv_own,
    recv_peer,
    gate_acc,
    up_acc,
    act_ref,
    down_send,
    down_recv,
    down_own,
    back_send,
    back_recv,
    sum_send,
    sum_recv,
    total_ref,
    load_sem,
    one_send,
    one_recv,
    route_send_sem,
    route_recv_sem,
    rows_send_sem,
    rows_recv_sem,
    sum_send_sem,
    sum_recv_sem,
    disp_send_sem,
    disp_recv_sem,
    fwd_send_sem,
    fwd_recv_sem,
    down_send_sem,
    down_recv_sem,
    back_send_sem,
    back_recv_sem,
):
    ep = lax.axis_index("ep")
    tp = lax.axis_index("tp")
    other = 1 - tp
    seqs, half = x_own.shape
    width = 2 * half

    loads = []
    pairs = (
        (tok_hbm, x_own),
        (g1_hbm, g1),
        (wq_hbm, wq),
        (wk_hbm, wk),
        (wv_hbm, wv),
        (kc_hbm, kc),
        (vc_hbm, vc),
        (wo_hbm, wo),
        (g2_hbm, g2),
        (ids_hbm, ids),
        (logits_hbm, logits),
        (gate_hbm, gate),
        (up_hbm, up),
        (down_hbm, down),
        (bias_hbm, bias_ref),
        (lens_hbm, lens_ref),
    )
    for i, (src, dst) in enumerate(pairs):
        slot = (10, 11, 12, 11, 12)[i - 11] if i > 10 else i
        loads.append(pltpu.make_async_copy(src, dst, load_sem.at[slot]))
    for i in (0, 1, 2, 3, 4, 14, 15, 9, 10, 8, 5, 6, 7):
        loads[i].start()

    def tally(ref, sem):
        return pltpu.make_async_remote_copy(
            src_ref=ref,
            dst_ref=ref,
            send_sem=sem,
            recv_sem=sem,
            device_id=(ep, other),
            device_id_type=MESH,
        )

    def peer_copy(src, dst, i):
        return pltpu.make_async_remote_copy(
            src_ref=src,
            dst_ref=dst,
            send_sem=one_send.at[min(i, 1)],
            recv_sem=one_recv.at[i],
            device_id=(ep, other),
            device_id_type=MESH,
        )

    barrier = pltpu.get_barrier_semaphore()
    pl.semaphore_signal(barrier, inc=1, device_id=(ep, other), device_id_type=MESH)

    planes = tables.shape[0]
    plane = n // planes
    level = ep // plane
    spot = ep % plane

    def column(i):
        return lax.rem(level + i, planes) * plane + spot

    def beside(i):
        return level * plane + lax.rem(spot + i, plane)

    if planes == 4:
        inner = lax.rem((level + 1) // 2, 2)
        partners = (
            level,
            lax.rem(level + 2, 4),
            level + 1 - 2 * lax.rem(level, 2),
            3 - level,
        )
        teams = ((0,), (1,), (2, 3))
        eager = (1, 3, 2)
    else:
        partners = (level,)
        inner = 0
        teams = ((0,),)
        eager = ()

    def greet_column(i, carry):
        pl.semaphore_signal(barrier, inc=1, device_id=(column(i), tp), device_id_type=MESH)
        return carry

    def greet_beside(i, carry):
        pl.semaphore_signal(barrier, inc=1, device_id=(beside(i), tp), device_id_type=MESH)
        return carry

    lax.fori_loop(1, planes, greet_column, 0)
    lax.fori_loop(1, plane, greet_beside, 0)
    loads[0].wait()
    loads[1].wait()
    mine = x_own[...].astype(F32)
    mean_own = jnp.sum(mine, axis=1, keepdims=True) / half
    centred = mine - mean_own
    square_own = jnp.sum(centred * centred, axis=1, keepdims=True)
    gain = g1[...]
    gain_hi = gain.astype(BF16)
    gain_lo = (gain - gain_hi.astype(F32)).astype(BF16)
    pad_row = lax.broadcasted_iota(jnp.int32, (PAD, half), 0)
    gains = jnp.where(
        pad_row == 0, gain_hi.astype(F32), jnp.where(pad_row == 1, gain_lo.astype(F32), 0.0)
    )
    stacked = jnp.concatenate([centred * gain, gains], axis=0).astype(BF16)
    for i in (2, 3, 4):
        loads[i].wait()
    pq = dot(stacked, wq[...])
    pk = dot(stacked, wk[...])
    pv = dot(stacked, wv[...])
    qc = pq.shape[1] // 2
    kcols = pk.shape[1] // 2
    first = tp == 0
    used = qc + 2 * kcols
    proj_send[:, :qc] = jnp.where(first, pq[:, qc:], pq[:, :qc])
    proj_send[:, qc : qc + kcols] = jnp.where(first, pk[:, kcols:], pk[:, :kcols])
    proj_send[:, qc + kcols : used] = jnp.where(first, pv[:, kcols:], pv[:, :kcols])
    proj_send[:seqs, used : used + LANES] = jnp.broadcast_to(mean_own, (seqs, LANES))
    proj_send[:seqs, used + LANES :] = jnp.broadcast_to(square_own, (seqs, LANES))
    pl.semaphore_wait(barrier, planes + plane - 1)

    proj_copy = peer_copy(proj_send, proj_recv, 1)
    proj_copy.start()
    loads[9].wait()
    loads[10].wait()
    top = ids.shape[0]
    route_send[:top] = ids[...].astype(F32)
    route_send[top:] = logits[...]

    def route_copy(i):
        to = partners[i]
        return pltpu.make_async_remote_copy(
            src_ref=route_send,
            dst_ref=route_recv.at[level],
            send_sem=route_send_sem.at[0],
            recv_sem=route_recv_sem.at[0],
            device_id=(to * plane + spot, tp),
            device_id_type=MESH,
        )

    for i in eager:
        route_copy(i).start()
    tok_copy = peer_copy(x_own, x_peer, 0)
    tok_copy.start()

    def stats(a, b):
        total = jnp.sum(a, axis=1, keepdims=True) + jnp.sum(b, axis=1, keepdims=True)
        square = jnp.sum(a * a, axis=1, keepdims=True) + jnp.sum(b * b, axis=1, keepdims=True)
        mean = total / width
        return mean, lax.rsqrt(square / width - mean * mean + LN_EPS)

    group = plane * cap
    slot_row = lax.broadcasted_iota(jnp.int32, (group, seqs), 0)
    slot_expert = slot_row // cap
    slot_rank = (slot_row - slot_expert * cap).astype(F32)
    slot_expert = (slot_expert + level * plane).astype(F32)
    earlier = (
        lax.broadcasted_iota(jnp.int32, (seqs, seqs), 0)
        < lax.broadcasted_iota(jnp.int32, (seqs, seqs), 1)
    )
    earlier = jnp.where(earlier, 1.0, 0.0).astype(BF16)

    def make_tables(k):
        route = route_send[...] if k == 0 else route_recv[partners[k]]
        raw = jnp.exp(route[top:])
        probs = raw / jnp.sum(raw, axis=0, keepdims=True)
        hot = jnp.zeros((group, seqs), F32)
        prob_hot = jnp.zeros((group, seqs), F32)
        for i in range(top):
            match = jnp.abs(route[i : i + 1] - slot_expert) < 0.5
            hot = hot + jnp.where(match, 1.0, 0.0)
            prob_hot = prob_hot + jnp.where(match, probs[i : i + 1, :], 0.0)
        rank = dot(hot.astype(BF16), earlier)
        chosen = (hot > 0.5) & (jnp.abs(rank - slot_rank) < 0.5)
        weight = jnp.where(chosen, prob_hot, 0.0)
        tables[k] = jnp.where(chosen, 1.0, 0.0).astype(BF16)
        weight = weight.T
        weight_hi = weight.astype(BF16)
        mixing[k, :, :group] = weight_hi.astype(F32)
        mixing[k, :, group:] = weight - weight_hi.astype(F32)

    groups = qc // HEAD
    loads[14].wait()
    loads[15].wait()
    bias = jnp.zeros((groups, 1), F32)
    head_row = lax.broadcasted_iota(jnp.int32, (groups, 1), 0)
    for h in range(groups):
        bias = bias + jnp.where(head_row == h, bias_ref[h], 0.0)

    own_q = jnp.where(first, pq[:, :qc], pq[:, qc:])
    own_k = jnp.where(first, pk[:, :kcols], pk[:, kcols:])
    own_v = jnp.where(first, pv[:, :kcols], pv[:, kcols:])
    proj_copy.wait()
    mean_peer = proj_recv[:seqs, used : used + 1]
    square_peer = proj_recv[:seqs, used + LANES : used + LANES + 1]
    apart = (mean_own - mean_peer) * 0.5
    scale = lax.rsqrt((square_own + square_peer) / width + apart * apart + LN_EPS)

    def joined(own, lo, hi):
        tilt = (own[seqs : seqs + 1] + own[seqs + 1 : seqs + 2]) - (
            proj_recv[seqs : seqs + 1, lo:hi] + proj_recv[seqs + 1 : seqs + 2, lo:hi]
        )
        return (scale * (own[:seqs] + proj_recv[:seqs, lo:hi] + apart * tilt)).astype(BF16)

    query = joined(own_q, 0, qc).astype(F32) * HEAD ** (-0.5)
    nk_ref[...] = joined(own_k, qc, qc + kcols)
    nv_ref[...] = joined(own_v, qc + kcols, used)
    for h in range(groups):
        q_rows[:, h, :] = query[:, h * HEAD : (h + 1) * HEAD]
    flat = q_rows[...].reshape(seqs * groups, HEAD).astype(BF16)
    wide_row = lax.broadcasted_iota(jnp.int32, (seqs * groups, BATCH * HEAD), 0)
    wide_col = lax.broadcasted_iota(jnp.int32, (seqs * groups, BATCH * HEAD), 1)
    q_wide[...] = jnp.where(
        lax.rem(wide_row // groups, BATCH) == wide_col // HEAD,
        jnp.concatenate([flat] * BATCH, axis=1),
        jnp.zeros((), BF16),
    )

    positions = kc.shape[2]
    after = (
        lax.broadcasted_iota(jnp.int32, (POS_BLOCK, POS_BLOCK), 0)
        > lax.broadcasted_iota(jnp.int32, (POS_BLOCK, POS_BLOCK), 1)
    )
    after = jnp.where(after, 1.0, 0.0).astype(BF16)
    chunk = seqs // CHUNKS
    step_rows = BATCH * groups
    place = lax.broadcasted_iota(jnp.int32, (step_rows, positions), 1)
    step_seq = lax.broadcasted_iota(jnp.int32, (step_rows, 1), 0) // groups
    step_bias = jnp.concatenate([bias] * BATCH, axis=0)

    def score(c):
        for i in range(c * chunk // BATCH, (c + 1) * chunk // BATCH):
            rows = slice(i * step_rows, (i + 1) * step_rows)
            keys = kc[i * BATCH : (i + 1) * BATCH].reshape(BATCH * HEAD, positions)
            length = jnp.zeros((step_rows, 1), jnp.int32)
            for j in range(BATCH):
                length = jnp.where(step_seq == j, lens_ref[i * BATCH + j], length)
            s = dot(q_wide[rows, :], keys) + step_bias
            z_ref[rows, :] = jnp.where(place < length, s, DEAD)

    def spend(c):
        count = chunk * groups
        rows = slice(c * count, (c + 1) * count)
        beyond = jnp.zeros((count, 1), F32)
        for b in reversed(range(positions // POS_BLOCK)):
            cols = slice(b * POS_BLOCK, (b + 1) * POS_BLOCK)
            z = z_ref[rows, cols]
            tail = jnp.log(1.0 + jnp.exp(-jnp.abs(z)))
            spent = jnp.maximum(z, 0.0) + tail
            hi = spent.astype(BF16)
            lo = (spent - hi.astype(F32)).astype(BF16)
            sums = dot(jnp.concatenate([hi, lo], axis=0), after)
            inside = sums[:count] + sums[count:]
            w_ref[rows, cols] = jnp.exp(
                jnp.minimum(z, 0.0) - tail - (inside + beyond)
            ).astype(BF16)
            beyond = beyond + inside[:, :1] + spent[:, :1]

    def read(c):
        for i in range(c * chunk // BATCH, (c + 1) * chunk // BATCH):
            weights = w_ref[i * step_rows : (i + 1) * step_rows, :]
            values = vc[i * BATCH : (i + 1) * BATCH].reshape(BATCH * HEAD, positions)
            mixed = lax.dot_general(
                weights, values, (((1,), (1,)), ((), ())), preferred_element_type=F32
            )
            for j in range(BATCH):
                att_ref[i * BATCH + j] = mixed[
                    j * groups : (j + 1) * groups, j * HEAD : (j + 1) * HEAD
                ]

    def part_copy(c):
        return peer_copy(part_send.at[c], part_recv.at[c], 2 + c)

    def project(c):
        mine = slice(c * chunk, (c + 1) * chunk)
        attended = jnp.concatenate([att_ref[mine, h, :] for h in range(groups)], axis=1)
        part = dot(attended.astype(BF16), wo[...]).astype(BF16)
        part_send[c, 0] = part[:, :half]
        part_send[c, 1] = part[:, half:]
        part_copy(c).start()

    def rows_copy(to, c):
        return pltpu.make_async_remote_copy(
            src_ref=rows_ref.at[c],
            dst_ref=rows_recv.at[level, c],
            send_sem=rows_send_sem.at[0],
            recv_sem=rows_recv_sem.at[level],
            device_id=(to * plane + spot, tp),
            device_id_type=MESH,
        )

    def relay_copy(c):
        far = partners[1]
        return pltpu.make_async_remote_copy(
            src_ref=rows_recv.at[far, c],
            dst_ref=rows_recv.at[far, c],
            send_sem=rows_send_sem.at[0],
            recv_sem=rows_recv_sem.at[far],
            device_id=(partners[2] * plane + spot, tp),
            device_id_type=MESH,
        )

    def settle(c):
        at = slice(c * chunk, (c + 1) * chunk)
        part_copy(c).wait()
        res_own = (
            x_own[at, :].astype(F32)
            + (part_send[c, tp].astype(F32) + part_recv[c, tp].astype(F32))
        ).astype(BF16)
        res_other = (
            x_peer[at, :].astype(F32)
            + (part_send[c, other].astype(F32) + part_recv[c, other].astype(F32))
        ).astype(BF16)
        res_ref[at, :] = res_own
        mine = res_own.astype(F32)
        mean, scale = stats(mine, res_other.astype(F32))
        rows_ref[c] = ((mine - mean) * scale * g2[...]).astype(BF16)
        if planes > 1:
            rows_copy(partners[1], c).start()

            @pl.when(inner == 1)
            def _():
                rows_copy(partners[3], c).start()

            rows_copy(partners[2], c).start()

    loads[5].wait()
    for c in range(CHUNKS):
        score(c)
        spend(c)
        if c == 0:
            loads[6].wait()
            for i in (11, 12, 13):
                loads[i].start()
            loads[7].wait()
            loads[8].wait()
            tok_copy.wait()
        else:
            settle(c - 1)
        read(c)
        project(c)
    for k in range(planes):
        if k == 1:
            tally(route_recv.at[pl.ds(0, planes - 1)], route_recv_sem.at[0]).wait_recv()
        make_tables(k)
    settle(CHUNKS - 1)

    def beside_copy(src, dst, send_sem, recv_sem, j):
        to = lax.rem(spot + j, plane)
        return pltpu.make_async_remote_copy(
            src_ref=src(to),
            dst_ref=dst(spot),
            send_sem=send_sem,
            recv_sem=recv_sem,
            device_id=(level * plane + to, tp),
            device_id_type=MESH,
        )

    def disp_copy(k, j):
        return beside_copy(
            lambda to: disp.at[k, to],
            lambda giver: recv_own.at[k, giver],
            disp_send_sem.at[0],
            disp_recv_sem.at[k],
            j,
        )

    def disp_keep(k):
        return pltpu.make_async_copy(disp.at[k, spot], recv_own.at[k, spot], load_sem.at[k])

    def fwd_copy(k):
        return pltpu.make_async_remote_copy(
            src_ref=recv_own.at[k],
            dst_ref=recv_peer.at[k],
            send_sem=fwd_send_sem.at[0],
            recv_sem=fwd_recv_sem.at[k],
            device_id=(ep, other),
            device_id_type=MESH,
        )

    def place_rows(k):
        if k > 0:
            rows = rows_recv[partners[k]].reshape(seqs, half)
        else:
            rows = rows_ref[...].reshape(seqs, half)
        placed = dot(tables[k], rows).astype(BF16)
        disp[k] = placed.reshape(plane, cap, half)
        for j in range(1, plane):
            disp_copy(k, j).start()
        disp_keep(k).start()

    def receive_rows(k):
        source = partners[k]
        tally(rows_recv.at[source], rows_recv_sem.at[source]).wait_recv()

    def gather(k):
        disp_keep(k).wait()
        tally(recv_own.at[k, pl.ds(0, plane - 1)], disp_recv_sem.at[k]).wait_recv()
        fwd_copy(k).start()

    hidden = gate.shape[1]
    own_depth = pl.ds(pl.multiple_of(tp * half, half), half)
    peer_depth = pl.ds(pl.multiple_of(other * half, half), half)
    def blocks_of(team):
        count = len(team) * group
        size = min(count, 256)
        return [slice(i * size, (i + 1) * size) for i in range(count // size)]

    def rows_of(ref, team, at):
        rows = ref[team[0] : team[-1] + 1].reshape(len(team) * plane, cap, half)
        return rows[at.start // cap : at.stop // cap].reshape(at.stop - at.start, half)

    def swiglu(g, u):
        c = jnp.minimum(g, SWIGLU_LIMIT)
        linear = jnp.clip(u, -SWIGLU_LIMIT, SWIGLU_LIMIT)
        return (c * jax.nn.sigmoid(SWIGLU_ALPHA * c) * (linear + 1.0)).astype(BF16)

    def first_half(team):
        def body(i, carry):
            cols = pl.ds(pl.multiple_of(i * GATE_BLOCK, GATE_BLOCK), GATE_BLOCK)
            for at in blocks_of(team):
                rows = rows_of(recv_own, team, at)
                gate_acc[at, cols] = dot(rows, gate[own_depth, cols])
                up_acc[at, cols] = dot(rows, up[own_depth, cols])
            return carry

        lax.fori_loop(0, hidden // GATE_BLOCK, body, 0)

    def second_half(team):
        def body(i, carry):
            cols = pl.ds(pl.multiple_of(i * GATE_BLOCK, GATE_BLOCK), GATE_BLOCK)
            for at in blocks_of(team):
                rows = rows_of(recv_peer, team, at)
                g = gate_acc[at, cols] + dot(rows, gate[peer_depth, cols])
                u = up_acc[at, cols] + dot(rows, up[peer_depth, cols])
                act_ref[at, cols] = swiglu(g, u)
            return carry

        lax.fori_loop(0, hidden // GATE_BLOCK, body, 0)

    def whole_depth(team):
        def body(i, carry):
            cols = pl.ds(pl.multiple_of(i * GATE_BLOCK, GATE_BLOCK), GATE_BLOCK)
            for at in blocks_of(team):
                mine = rows_of(recv_own, team, at)
                theirs = rows_of(recv_peer, team, at)
                g = dot(mine, gate[own_depth, cols]) + dot(theirs, gate[peer_depth, cols])
                u = dot(mine, up[own_depth, cols]) + dot(theirs, up[peer_depth, cols])
                act_ref[at, cols] = swiglu(g, u)
            return carry

        lax.fori_loop(0, hidden // GATE_BLOCK, body, 0)

    tiles = half // COL_BLOCK
    all_tiles = pl.ds(0, tiles)
    one_tile = [pl.ds(t, 1) for t in range(tiles)]
    backs = half // BACK_BLOCK
    all_backs = pl.ds(0, backs)
    one_back = [pl.ds(b, 1) for b in range(backs)]
    some_backs = [pl.ds(t * backs // tiles, backs // tiles) for t in range(tiles)]

    def down_copy(p, at):
        team = teams[p]
        ks = pl.ds(team[0], len(team))
        slot = p + at.start // at.size + (tiles - 1 if p == 2 else 0)
        return pltpu.make_async_remote_copy(
            src_ref=down_send.at[at, ks],
            dst_ref=down_recv.at[at, ks],
            send_sem=down_send_sem.at[0],
            recv_sem=down_recv_sem.at[slot],
            device_id=(ep, other),
            device_id_type=MESH,
        )

    def down_tile(ref, p, side, t):
        team = teams[p]
        cols = pl.ds(pl.multiple_of(side * half + t * COL_BLOCK, COL_BLOCK), COL_BLOCK)
        for at in blocks_of(team):
            value = dot(act_ref[at, :], down[:, cols]).astype(BF16)
            size = at.stop - at.start
            if size <= group:
                k, begin = team[0] + at.start // group, at.start % group
                ref[t, k, begin : begin + size, :] = value
            else:
                k = team[0] + at.start // group
                ref[t, k : k + size // group] = value.reshape(size // group, group, COL_BLOCK)

    def down_other(p, parts):
        for at in parts:
            for t in range(at.start, at.start + at.size):
                down_tile(down_send, p, other, t)
            down_copy(p, at).start()

    def back_slot(k, at):
        base = (0, 1, 1 + tiles, 1 + tiles + backs)[k]
        return base + at.start // at.size

    def back_copy(k, at, j):
        return beside_copy(
            lambda to: back_send.at[k, to, at],
            lambda giver: back_recv.at[k, giver, at],
            back_send_sem.at[0],
            back_recv_sem.at[back_slot(k, at)],
            j,
        )

    def back_keep(k, at):
        return pltpu.make_async_copy(
            back_send.at[k, spot, at],
            back_recv.at[k, spot, at],
            load_sem.at[planes + back_slot(k, at)],
        )

    def send_back(k, at):
        for j in range(1, plane):
            back_copy(k, at, j).start()
        back_keep(k, at).start()

    def down_join(p, t):
        for k in teams[p]:
            total = (down_own[t, k].astype(F32) + down_recv[t, k].astype(F32)).astype(BF16)
            for i in range(COL_BLOCK // BACK_BLOCK):
                piece = total[:, i * BACK_BLOCK : (i + 1) * BACK_BLOCK]
                at = t * (COL_BLOCK // BACK_BLOCK) + i
                back_send[k, :, at] = piece.reshape(plane, cap, BACK_BLOCK)

    def down_mine(p):
        for t in range(tiles):
            down_tile(down_own, p, tp, t)

    def join_whole(p):
        down_copy(p, all_tiles).wait_recv()
        for t in range(tiles):
            down_join(p, t)
        for k in teams[p]:
            send_back(k, all_backs)

    def join_tiles(p):
        for t in range(tiles):
            down_tile(down_own, p, tp, t)
            down_copy(p, one_tile[t]).wait_recv()
            down_join(p, t)
            for b in range(t * backs // tiles, (t + 1) * backs // tiles):
                send_back(teams[p][-1], one_back[b])
        for k in reversed(teams[p][:-1]):
            for b in range(backs):
                send_back(k, one_back[b])

    def sum_copy(k, t):
        to = partners[k]
        return pltpu.make_async_remote_copy(
            src_ref=sum_send.at[to, t],
            dst_ref=sum_recv.at[level, t],
            send_sem=sum_send_sem.at[0],
            recv_sem=sum_recv_sem.at[0],
            device_id=(to * plane + spot, tp),
            device_id_type=MESH,
        )

    def combine(k, at):
        back_keep(k, at).wait()
        arrived = back_recv.at[k, pl.ds(0, plane - 1), at]
        tally(arrived, back_recv_sem.at[back_slot(k, at)]).wait_recv()
        to = partners[k]
        mixes = []
        for t in range(at.start, at.start + at.size):
            back = back_recv[k, :, t].reshape(group, BACK_BLOCK)
            mixes.append(dot(mixing[k].astype(BF16), jnp.concatenate([back, back], axis=0)))
        for t, mixed in zip(range(at.start, at.start + at.size), mixes):
            cols = slice(t * BACK_BLOCK, (t + 1) * BACK_BLOCK)
            if k == 0:
                total_ref[:, cols] = res_ref[:, cols].astype(F32) + mixed
            else:
                sum_send[to, t] = mixed.astype(BF16)
        if k > 0:
            for t in range(at.start, at.start + at.size):
                sum_copy(k, t).start()

    def run_far():
        whole_depth(teams[2])
        down_other(2, one_tile)
        join_tiles(2)

    place_rows(0)
    if planes > 1:
        receive_rows(1)

        @pl.when(inner == 1)
        def _():
            for c in range(CHUNKS):
                relay_copy(c).start()

        place_rows(1)
    gather(0)
    if planes > 1:
        receive_rows(2)
        place_rows(2)
    for i in (11, 12, 13):
        loads[i].wait()
    first_half(teams[0])
    fwd_copy(0).wait_recv()
    second_half(teams[0])
    down_other(0, [all_tiles])
    if planes > 1:
        receive_rows(3)
        place_rows(3)
    down_mine(0)
    join_whole(0)
    if planes > 1:
        gather(1)
        first_half(teams[1])
        fwd_copy(1).wait_recv()
        second_half(teams[1])
        down_other(1, one_tile)
        gather(2)
        gather(3)
        down_mine(1)
        for t in range(tiles):
            down_copy(1, one_tile[t]).wait_recv()
            down_join(1, t)
            send_back(1, some_backs[t])
        fwd_copy(2).wait_recv()
        fwd_copy(3).wait_recv()
        run_far()
        tally(route_recv.at[pl.ds(0, planes - 1)], route_send_sem.at[0]).wait_send()

        @pl.when(inner == 1)
        def _():
            tally(rows_recv, rows_send_sem.at[0]).wait_send()

        @pl.when(inner == 0)
        def _():
            tally(rows_recv.at[pl.ds(0, 2)], rows_send_sem.at[0]).wait_send()

    tally(disp.at[:, pl.ds(0, plane - 1)], disp_send_sem.at[0]).wait_send()
    tally(recv_own, fwd_send_sem.at[0]).wait_send()
    tally(down_send, down_send_sem.at[0]).wait_send()
    if planes > 1:
        for at in some_backs:
            combine(1, at)
    combine(0, all_backs)
    if planes > 1:
        for k in (3, 2):
            for b in range(backs):
                combine(k, one_back[b])
    tally(back_send.at[:, pl.ds(0, plane - 1)], back_send_sem.at[0]).wait_send()
    if planes > 1:
        tally(sum_recv.at[pl.ds(0, planes - 1)], sum_recv_sem.at[0]).wait_recv()
    for t in range(backs):
        cols = slice(t * BACK_BLOCK, (t + 1) * BACK_BLOCK)
        total = total_ref[:, cols]
        for k in range(1, planes):
            total = total + sum_recv[partners[k], t].astype(F32)
        out_ref[:, cols] = total.astype(BF16)

    if planes > 1:
        tally(sum_send.at[pl.ds(0, planes - 1)], sum_send_sem.at[0]).wait_send()


def publish(*refs):
    sems = refs[-1]
    count = len(refs) // 2
    copies = []
    for i in range(count):
        copy = pltpu.make_async_copy(refs[i], refs[count + i], sems.at[i])
        copy.start()
        copies.append(copy)
    for copy in copies:
        copy.wait()


def local(
    tokens,
    norm1_gain,
    w_query,
    w_key,
    w_value,
    head_bias,
    key_cache,
    value_cache,
    seq_lengths,
    w_out,
    norm2_gain,
    route_ids,
    route_logits,
    expert_gate,
    expert_up,
    expert_down,
):
    n = lax.axis_size("ep")
    seqs, half = tokens.shape
    top = route_ids.shape[1]
    experts = n * expert_gate.shape[0]
    capacity = max(2, 2 * seqs * top // experts)
    cap = -(-capacity // 16) * 16
    planes = 4 if n % 4 == 0 else 1
    plane = n // planes
    qc = w_query.shape[1] // 2
    kcols = w_key.shape[1] // 2
    groups = qc // HEAD
    positions = key_cache.shape[1]
    hidden = expert_gate.shape[2]
    tiles = half // COL_BLOCK
    backs = half // BACK_BLOCK
    most = plane * cap * (2 if planes == 4 else 1)
    keys = jnp.swapaxes(key_cache, 1, 2)
    values = jnp.swapaxes(value_cache, 1, 2)
    operands = (
        tokens,
        norm1_gain.reshape(1, -1),
        w_query,
        w_key,
        w_value,
        head_bias,
        keys,
        values,
        seq_lengths,
        w_out,
        norm2_gain.reshape(1, -1),
        route_ids.T,
        route_logits.T,
        expert_gate.reshape(expert_gate.shape[1:]),
        expert_up.reshape(expert_up.shape[1:]),
        expert_down.reshape(expert_down.shape[1:]),
    )
    in_smem = (5, 8)
    in_specs = [
        pl.BlockSpec(memory_space=pl.ANY) for i in range(len(operands))
    ]
    vmem = pl.BlockSpec(memory_space=pltpu.VMEM)
    loaded = [
        pltpu.VMEM(a.shape, a.dtype) for i, a in enumerate(operands) if i not in in_smem
    ]
    dma = pltpu.SemaphoreType.DMA
    scratch = (
        [pltpu.SMEM(operands[i].shape, operands[i].dtype) for i in in_smem]
        + [loaded[0], loaded[0]]
        + loaded[1:]
        + [
            pltpu.VMEM((seqs + PAD, qc + 2 * kcols + 2 * LANES), F32),
            pltpu.VMEM((seqs + PAD, qc + 2 * kcols + 2 * LANES), F32),
            pltpu.VMEM((seqs, groups, HEAD), F32),
            pltpu.VMEM((seqs * groups, BATCH * HEAD), BF16),
            pltpu.VMEM((seqs * groups, positions), F32),
            pltpu.VMEM((seqs * groups, positions), BF16),
            pltpu.VMEM((seqs, groups, HEAD), F32),
            pltpu.VMEM((CHUNKS, 2, seqs // CHUNKS, half), BF16),
            pltpu.VMEM((CHUNKS, 2, seqs // CHUNKS, half), BF16),
            pltpu.VMEM((seqs, half), BF16),
            pltpu.VMEM((2 * top, seqs), F32),
            pltpu.VMEM((planes, 2 * top, seqs), F32),
            pltpu.VMEM((planes, plane * cap, seqs), BF16),
            pltpu.VMEM((planes, seqs, 2 * plane * cap), F32),
            pltpu.VMEM((CHUNKS, seqs // CHUNKS, half), BF16),
            pltpu.VMEM((planes, CHUNKS, seqs // CHUNKS, half), BF16),
            pltpu.VMEM((planes, plane, cap, half), BF16),
            pltpu.VMEM((planes, plane, cap, half), BF16),
            pltpu.VMEM((planes, plane, cap, half), BF16),
            pltpu.VMEM((most, hidden), F32),
            pltpu.VMEM((most, hidden), F32),
            pltpu.VMEM((most, hidden), BF16),
            pltpu.VMEM((tiles, planes, plane * cap, COL_BLOCK), BF16),
            pltpu.VMEM((tiles, planes, plane * cap, COL_BLOCK), BF16),
            pltpu.VMEM((tiles, planes, plane * cap, COL_BLOCK), BF16),
            pltpu.VMEM((planes, plane, backs, cap, BACK_BLOCK), BF16),
            pltpu.VMEM((planes, plane, backs, cap, BACK_BLOCK), BF16),
            pltpu.VMEM((planes, backs, seqs, BACK_BLOCK), BF16),
            pltpu.VMEM((planes, backs, seqs, BACK_BLOCK), BF16),
            pltpu.VMEM((seqs, half), F32),
            dma((planes + 1 + tiles + 2 * backs,)),
            dma((2,)),
            dma((2 + CHUNKS,)),
            dma((1,)),
            dma((1,)),
            dma((1,)),
            dma((planes,)),
            dma((1,)),
            dma((1,)),
            dma((1,)),
            dma((planes,)),
            dma((1,)),
            dma((planes,)),
            dma((1,)),
            dma((1 + 2 * tiles,)),
            dma((1,)),
            dma((1 + tiles + 2 * backs,)),
        ]
    )
    shapes = ((seqs, half), (seqs, kcols), (seqs, kcols))
    results = pl.pallas_call(
        functools.partial(kernel, n, cap),
        out_shape=tuple(pltpu.VMEM(shape, BF16) for shape in shapes),
        in_specs=in_specs,
        out_specs=(vmem, vmem, vmem),
        scratch_shapes=scratch,
        compiler_params=pltpu.CompilerParams(
            collective_id=0, has_side_effects=True, vmem_limit_bytes=VMEM_BYTES
        ),
    )(*operands)
    return pl.pallas_call(
        publish,
        out_shape=tuple(jax.ShapeDtypeStruct(shape, BF16) for shape in shapes),
        in_specs=[vmem] * len(shapes),
        out_specs=tuple([pl.BlockSpec(memory_space=pl.ANY)] * len(shapes)),
        scratch_shapes=[dma((len(shapes),))],
    )(*(pltpu.with_memory_space_constraint(r, pltpu.VMEM) for r in results))


def solution(mesh):
    in_specs = (
        P("ep", "tp"),
        P("tp"),
        P("tp", None),
        P("tp", None),
        P("tp", None),
        P("tp"),
        P("ep", None, "tp"),
        P("ep", None, "tp"),
        P("ep"),
        P("tp", None),
        P("tp"),
        P("ep", None),
        P("ep", None),
        P("ep", None, "tp"),
        P("ep", None, "tp"),
        P("ep", "tp", None),
    )
    out_specs = (P("ep", "tp"), P("ep", "tp"), P("ep", "tp"))
    return jax.shard_map(local, mesh=mesh, in_specs=in_specs, out_specs=out_specs, check_vma=False)
```

```python
import functools

import jax
import jax.numpy as jnp
from jax import lax
from jax.experimental import pallas as pl
from jax.experimental.pallas import tpu as pltpu
from jax.sharding import PartitionSpec as P

HEAD = 64
LN_EPS = 1e-05
SWIGLU_ALPHA = 1.702
SWIGLU_LIMIT = 7.0
MESH = pl.DeviceIdType.MESH
F32 = jnp.float32
BF16 = jnp.bfloat16
DEAD = -1e30
POS_BLOCK = 256
COL_BLOCK = 512
GATE_BLOCK = 1024
BACK_BLOCK = 256
PAD = 16
BATCH = 4
CHUNKS = 2
VMEM_BYTES = 63 * 1024 * 1024
LANES = 128


def dot(a, b):
    return jnp.dot(a, b, preferred_element_type=F32)


def kernel(
    n,
    cap,
    tok_hbm,
    g1_hbm,
    wq_hbm,
    wk_hbm,
    wv_hbm,
    bias_hbm,
    kc_hbm,
    vc_hbm,
    lens_hbm,
    wo_hbm,
    g2_hbm,
    ids_hbm,
    logits_hbm,
    gate_hbm,
    up_hbm,
    down_hbm,
    out_ref,
    nk_ref,
    nv_ref,
    bias_ref,
    lens_ref,
    x_own,
    x_peer,
    g1,
    wq,
    wk,
    wv,
    kc,
    vc,
    wo,
    g2,
    ids,
    logits,
    gate,
    up,
    down,
    proj_send,
    proj_recv,
    q_rows,
    q_wide,
    z_ref,
    w_ref,
    att_ref,
    part_send,
    part_recv,
    res_ref,
    route_send,
    route_recv,
    tables,
    mixing,
    rows_ref,
    rows_recv,
    disp,
    recv_own,
    recv_peer,
    gate_acc,
    up_acc,
    act_ref,
    down_send,
    down_recv,
    down_own,
    back_send,
    back_recv,
    sum_send,
    sum_recv,
    total_ref,
    load_sem,
    one_send,
    one_recv,
    route_send_sem,
    route_recv_sem,
    rows_send_sem,
    rows_recv_sem,
    sum_send_sem,
    sum_recv_sem,
    disp_send_sem,
    disp_recv_sem,
    fwd_send_sem,
    fwd_recv_sem,
    down_send_sem,
    down_recv_sem,
    back_send_sem,
    back_recv_sem,
):
    ep = lax.axis_index("ep")
    tp = lax.axis_index("tp")
    other = 1 - tp
    seqs, half = x_own.shape
    width = 2 * half

    loads = []
    pairs = (
        (tok_hbm, x_own),
        (g1_hbm, g1),
        (wq_hbm, wq),
        (wk_hbm, wk),
        (wv_hbm, wv),
        (kc_hbm, kc),
        (vc_hbm, vc),
        (wo_hbm, wo),
        (g2_hbm, g2),
        (ids_hbm, ids),
        (logits_hbm, logits),
        (gate_hbm, gate),
        (up_hbm, up),
        (down_hbm, down),
        (bias_hbm, bias_ref),
        (lens_hbm, lens_ref),
    )
    for i, (src, dst) in enumerate(pairs):
        slot = (10, 11, 12, 11, 12)[i - 11] if i > 10 else i
        loads.append(pltpu.make_async_copy(src, dst, load_sem.at[slot]))
    for i in (0, 1, 2, 3, 4, 14, 15, 9, 10, 8, 5, 6, 7):
        loads[i].start()

    def tally(ref, sem):
        return pltpu.make_async_remote_copy(
            src_ref=ref,
            dst_ref=ref,
            send_sem=sem,
            recv_sem=sem,
            device_id=(ep, other),
            device_id_type=MESH,
        )

    def peer_copy(src, dst, i):
        return pltpu.make_async_remote_copy(
            src_ref=src,
            dst_ref=dst,
            send_sem=one_send.at[min(i, 1)],
            recv_sem=one_recv.at[i],
            device_id=(ep, other),
            device_id_type=MESH,
        )

    barrier = pltpu.get_barrier_semaphore()
    pl.semaphore_signal(barrier, inc=1, device_id=(ep, other), device_id_type=MESH)

    planes = tables.shape[0]
    plane = n // planes
    level = ep // plane
    spot = ep % plane

    def column(i):
        return lax.rem(level + i, planes) * plane + spot

    def beside(i):
        return level * plane + lax.rem(spot + i, plane)

    if planes == 4:
        inner = lax.rem((level + 1) // 2, 2)
        partners = (
            level,
            lax.rem(level + 2, 4),
            level + 1 - 2 * lax.rem(level, 2),
            3 - level,
        )
        teams = ((0,), (1,), (2, 3))
        eager = (1, 3, 2)
    else:
        partners = (level,)
        inner = 0
        teams = ((0,),)
        eager = ()

    def greet_column(i, carry):
        pl.semaphore_signal(barrier, inc=1, device_id=(column(i), tp), device_id_type=MESH)
        return carry

    def greet_beside(i, carry):
        pl.semaphore_signal(barrier, inc=1, device_id=(beside(i), tp), device_id_type=MESH)
        return carry

    lax.fori_loop(1, planes, greet_column, 0)
    lax.fori_loop(1, plane, greet_beside, 0)
    loads[0].wait()
    loads[1].wait()
    mine = x_own[...].astype(F32)
    mean_own = jnp.sum(mine, axis=1, keepdims=True) / half
    centred = mine - mean_own
    square_own = jnp.sum(centred * centred, axis=1, keepdims=True)
    gain = g1[...]
    gain_hi = gain.astype(BF16)
    gain_lo = (gain - gain_hi.astype(F32)).astype(BF16)
    pad_row = lax.broadcasted_iota(jnp.int32, (PAD, half), 0)
    gains = jnp.where(
        pad_row == 0, gain_hi.astype(F32), jnp.where(pad_row == 1, gain_lo.astype(F32), 0.0)
    )
    stacked = jnp.concatenate([centred * gain, gains], axis=0).astype(BF16)
    for i in (2, 3, 4):
        loads[i].wait()
    pq = dot(stacked, wq[...])
    pk = dot(stacked, wk[...])
    pv = dot(stacked, wv[...])
    qc = pq.shape[1] // 2
    kcols = pk.shape[1] // 2
    first = tp == 0
    used = qc + 2 * kcols
    proj_send[:, :qc] = jnp.where(first, pq[:, qc:], pq[:, :qc])
    proj_send[:, qc : qc + kcols] = jnp.where(first, pk[:, kcols:], pk[:, :kcols])
    proj_send[:, qc + kcols : used] = jnp.where(first, pv[:, kcols:], pv[:, :kcols])
    proj_send[:seqs, used : used + LANES] = jnp.broadcast_to(mean_own, (seqs, LANES))
    proj_send[:seqs, used + LANES :] = jnp.broadcast_to(square_own, (seqs, LANES))
    pl.semaphore_wait(barrier, planes + plane - 1)

    proj_copy = peer_copy(proj_send, proj_recv, 1)
    proj_copy.start()
    loads[9].wait()
    loads[10].wait()
    top = ids.shape[0]
    route_send[:top] = ids[...].astype(F32)
    route_send[top:] = logits[...]

    def route_copy(i):
        to = partners[i]
        return pltpu.make_async_remote_copy(
            src_ref=route_send,
            dst_ref=route_recv.at[level],
            send_sem=route_send_sem.at[0],
            recv_sem=route_recv_sem.at[0],
            device_id=(to * plane + spot, tp),
            device_id_type=MESH,
        )

    for i in eager:
        route_copy(i).start()
    tok_copy = peer_copy(x_own, x_peer, 0)
    tok_copy.start()

    def stats(a, b):
        total = jnp.sum(a, axis=1, keepdims=True) + jnp.sum(b, axis=1, keepdims=True)
        square = jnp.sum(a * a, axis=1, keepdims=True) + jnp.sum(b * b, axis=1, keepdims=True)
        mean = total / width
        return mean, lax.rsqrt(square / width - mean * mean + LN_EPS)

    group = plane * cap
    slot_row = lax.broadcasted_iota(jnp.int32, (group, seqs), 0)
    slot_expert = slot_row // cap
    slot_rank = (slot_row - slot_expert * cap).astype(F32)
    slot_expert = (slot_expert + level * plane).astype(F32)
    earlier = (
        lax.broadcasted_iota(jnp.int32, (seqs, seqs), 0)
        < lax.broadcasted_iota(jnp.int32, (seqs, seqs), 1)
    )
    earlier = jnp.where(earlier, 1.0, 0.0).astype(BF16)

    def make_tables(k):
        route = route_send[...] if k == 0 else route_recv[partners[k]]
        raw = jnp.exp(route[top:])
        probs = raw / jnp.sum(raw, axis=0, keepdims=True)
        hot = jnp.zeros((group, seqs), F32)
        prob_hot = jnp.zeros((group, seqs), F32)
        for i in range(top):
            match = jnp.abs(route[i : i + 1] - slot_expert) < 0.5
            hot = hot + jnp.where(match, 1.0, 0.0)
            prob_hot = prob_hot + jnp.where(match, probs[i : i + 1, :], 0.0)
        rank = dot(hot.astype(BF16), earlier)
        chosen = (hot > 0.5) & (jnp.abs(rank - slot_rank) < 0.5)
        weight = jnp.where(chosen, prob_hot, 0.0)
        tables[k] = jnp.where(chosen, 1.0, 0.0).astype(BF16)
        weight = weight.T
        weight_hi = weight.astype(BF16)
        mixing[k, :, :group] = weight_hi.astype(F32)
        mixing[k, :, group:] = weight - weight_hi.astype(F32)

    groups = qc // HEAD
    loads[14].wait()
    loads[15].wait()
    bias = jnp.zeros((groups, 1), F32)
    head_row = lax.broadcasted_iota(jnp.int32, (groups, 1), 0)
    for h in range(groups):
        bias = bias + jnp.where(head_row == h, bias_ref[h], 0.0)

    own_q = jnp.where(first, pq[:, :qc], pq[:, qc:])
    own_k = jnp.where(first, pk[:, :kcols], pk[:, kcols:])
    own_v = jnp.where(first, pv[:, :kcols], pv[:, kcols:])
    proj_copy.wait()
    mean_peer = proj_recv[:seqs, used : used + 1]
    square_peer = proj_recv[:seqs, used + LANES : used + LANES + 1]
    apart = (mean_own - mean_peer) * 0.5
    scale = lax.rsqrt((square_own + square_peer) / width + apart * apart + LN_EPS)

    def joined(own, lo, hi):
        tilt = (own[seqs : seqs + 1] + own[seqs + 1 : seqs + 2]) - (
            proj_recv[seqs : seqs + 1, lo:hi] + proj_recv[seqs + 1 : seqs + 2, lo:hi]
        )
        return (scale * (own[:seqs] + proj_recv[:seqs, lo:hi] + apart * tilt)).astype(BF16)

    query = joined(own_q, 0, qc).astype(F32) * HEAD ** (-0.5)
    nk_ref[...] = joined(own_k, qc, qc + kcols)
    nv_ref[...] = joined(own_v, qc + kcols, used)
    for h in range(groups):
        q_rows[:, h, :] = query[:, h * HEAD : (h + 1) * HEAD]
    flat = q_rows[...].reshape(seqs * groups, HEAD).astype(BF16)
    wide_row = lax.broadcasted_iota(jnp.int32, (seqs * groups, BATCH * HEAD), 0)
    wide_col = lax.broadcasted_iota(jnp.int32, (seqs * groups, BATCH * HEAD), 1)
    q_wide[...] = jnp.where(
        lax.rem(wide_row // groups, BATCH) == wide_col // HEAD,
        jnp.concatenate([flat] * BATCH, axis=1),
        jnp.zeros((), BF16),
    )

    positions = kc.shape[2]
    after = (
        lax.broadcasted_iota(jnp.int32, (POS_BLOCK, POS_BLOCK), 0)
        > lax.broadcasted_iota(jnp.int32, (POS_BLOCK, POS_BLOCK), 1)
    )
    after = jnp.where(after, 1.0, 0.0).astype(BF16)
    chunk = seqs // CHUNKS
    step_rows = BATCH * groups
    place = lax.broadcasted_iota(jnp.int32, (step_rows, positions), 1)
    step_seq = lax.broadcasted_iota(jnp.int32, (step_rows, 1), 0) // groups
    step_bias = jnp.concatenate([bias] * BATCH, axis=0)

    def score(c):
        for i in range(c * chunk // BATCH, (c + 1) * chunk // BATCH):
            rows = slice(i * step_rows, (i + 1) * step_rows)
            keys = kc[i * BATCH : (i + 1) * BATCH].reshape(BATCH * HEAD, positions)
            length = jnp.zeros((step_rows, 1), jnp.int32)
            for j in range(BATCH):
                length = jnp.where(step_seq == j, lens_ref[i * BATCH + j], length)
            s = dot(q_wide[rows, :], keys) + step_bias
            z_ref[rows, :] = jnp.where(place < length, s, DEAD)

    def spend(c):
        count = chunk * groups
        rows = slice(c * count, (c + 1) * count)
        beyond = jnp.zeros((count, 1), F32)
        for b in reversed(range(positions // POS_BLOCK)):
            cols = slice(b * POS_BLOCK, (b + 1) * POS_BLOCK)
            z = z_ref[rows, cols]
            tail = jnp.log(1.0 + jnp.exp(-jnp.abs(z)))
            spent = jnp.maximum(z, 0.0) + tail
            hi = spent.astype(BF16)
            lo = (spent - hi.astype(F32)).astype(BF16)
            sums = dot(jnp.concatenate([hi, lo], axis=0), after)
            inside = sums[:count] + sums[count:]
            w_ref[rows, cols] = jnp.exp(
                jnp.minimum(z, 0.0) - tail - (inside + beyond)
            ).astype(BF16)
            beyond = beyond + inside[:, :1] + spent[:, :1]

    def read(c):
        for i in range(c * chunk // BATCH, (c + 1) * chunk // BATCH):
            weights = w_ref[i * step_rows : (i + 1) * step_rows, :]
            values = vc[i * BATCH : (i + 1) * BATCH].reshape(BATCH * HEAD, positions)
            mixed = lax.dot_general(
                weights, values, (((1,), (1,)), ((), ())), preferred_element_type=F32
            )
            for j in range(BATCH):
                att_ref[i * BATCH + j] = mixed[
                    j * groups : (j + 1) * groups, j * HEAD : (j + 1) * HEAD
                ]

    def part_copy(c):
        return peer_copy(part_send.at[c], part_recv.at[c], 2 + c)

    def project(c):
        mine = slice(c * chunk, (c + 1) * chunk)
        attended = jnp.concatenate([att_ref[mine, h, :] for h in range(groups)], axis=1)
        part = dot(attended.astype(BF16), wo[...]).astype(BF16)
        part_send[c, 0] = part[:, :half]
        part_send[c, 1] = part[:, half:]
        part_copy(c).start()

    def rows_copy(to, c):
        return pltpu.make_async_remote_copy(
            src_ref=rows_ref.at[c],
            dst_ref=rows_recv.at[level, c],
            send_sem=rows_send_sem.at[0],
            recv_sem=rows_recv_sem.at[level],
            device_id=(to * plane + spot, tp),
            device_id_type=MESH,
        )

    def relay_copy(c):
        far = partners[1]
        return pltpu.make_async_remote_copy(
            src_ref=rows_recv.at[far, c],
            dst_ref=rows_recv.at[far, c],
            send_sem=rows_send_sem.at[0],
            recv_sem=rows_recv_sem.at[far],
            device_id=(partners[2] * plane + spot, tp),
            device_id_type=MESH,
        )

    def settle(c):
        at = slice(c * chunk, (c + 1) * chunk)
        part_copy(c).wait()
        res_own = (
            x_own[at, :].astype(F32)
            + (part_send[c, tp].astype(F32) + part_recv[c, tp].astype(F32))
        ).astype(BF16)
        res_other = (
            x_peer[at, :].astype(F32)
            + (part_send[c, other].astype(F32) + part_recv[c, other].astype(F32))
        ).astype(BF16)
        res_ref[at, :] = res_own
        mine = res_own.astype(F32)
        mean, scale = stats(mine, res_other.astype(F32))
        rows_ref[c] = ((mine - mean) * scale * g2[...]).astype(BF16)
        if planes > 1:
            rows_copy(partners[1], c).start()

            @pl.when(inner == 1)
            def _():
                rows_copy(partners[3], c).start()

            rows_copy(partners[2], c).start()

    loads[5].wait()
    for c in range(CHUNKS):
        score(c)
        spend(c)
        if c == 0:
            loads[6].wait()
            for i in (11, 12, 13):
                loads[i].start()
            loads[7].wait()
            loads[8].wait()
            tok_copy.wait()
        else:
            settle(c - 1)
        read(c)
        project(c)
    for k in range(planes):
        if k == 1:
            tally(route_recv.at[pl.ds(0, planes - 1)], route_recv_sem.at[0]).wait_recv()
        make_tables(k)
    settle(CHUNKS - 1)

    def beside_copy(src, dst, send_sem, recv_sem, j):
        to = lax.rem(spot + j, plane)
        return pltpu.make_async_remote_copy(
            src_ref=src(to),
            dst_ref=dst(spot),
            send_sem=send_sem,
            recv_sem=recv_sem,
            device_id=(level * plane + to, tp),
            device_id_type=MESH,
        )

    def disp_copy(k, j):
        return beside_copy(
            lambda to: disp.at[k, to],
            lambda giver: recv_own.at[k, giver],
            disp_send_sem.at[0],
            disp_recv_sem.at[k],
            j,
        )

    def disp_keep(k):
        return pltpu.make_async_copy(disp.at[k, spot], recv_own.at[k, spot], load_sem.at[k])

    def fwd_copy(k):
        return pltpu.make_async_remote_copy(
            src_ref=recv_own.at[k],
            dst_ref=recv_peer.at[k],
            send_sem=fwd_send_sem.at[0],
            recv_sem=fwd_recv_sem.at[k],
            device_id=(ep, other),
            device_id_type=MESH,
        )

    def place_rows(k):
        if k > 0:
            rows = rows_recv[partners[k]].reshape(seqs, half)
        else:
            rows = rows_ref[...].reshape(seqs, half)
        placed = dot(tables[k], rows).astype(BF16)
        disp[k] = placed.reshape(plane, cap, half)
        for j in range(1, plane):
            disp_copy(k, j).start()
        disp_keep(k).start()

    def receive_rows(k):
        source = partners[k]
        tally(rows_recv.at[source], rows_recv_sem.at[source]).wait_recv()

    def gather(k):
        disp_keep(k).wait()
        tally(recv_own.at[k, pl.ds(0, plane - 1)], disp_recv_sem.at[k]).wait_recv()
        fwd_copy(k).start()

    hidden = gate.shape[1]
    own_depth = pl.ds(pl.multiple_of(tp * half, half), half)
    peer_depth = pl.ds(pl.multiple_of(other * half, half), half)
    def blocks_of(team):
        count = len(team) * group
        size = min(count, 256)
        return [slice(i * size, (i + 1) * size) for i in range(count // size)]

    def rows_of(ref, team, at):
        rows = ref[team[0] : team[-1] + 1].reshape(len(team) * plane, cap, half)
        return rows[at.start // cap : at.stop // cap].reshape(at.stop - at.start, half)

    def swiglu(g, u):
        c = jnp.minimum(g, SWIGLU_LIMIT)
        linear = jnp.clip(u, -SWIGLU_LIMIT, SWIGLU_LIMIT)
        return (c * jax.nn.sigmoid(SWIGLU_ALPHA * c) * (linear + 1.0)).astype(BF16)

    def first_half(team):
        def body(i, carry):
            cols = pl.ds(pl.multiple_of(i * GATE_BLOCK, GATE_BLOCK), GATE_BLOCK)
            for at in blocks_of(team):
                rows = rows_of(recv_own, team, at)
                gate_acc[at, cols] = dot(rows, gate[own_depth, cols])
                up_acc[at, cols] = dot(rows, up[own_depth, cols])
            return carry

        lax.fori_loop(0, hidden // GATE_BLOCK, body, 0)

    def second_half(team):
        def body(i, carry):
            cols = pl.ds(pl.multiple_of(i * GATE_BLOCK, GATE_BLOCK), GATE_BLOCK)
            for at in blocks_of(team):
                rows = rows_of(recv_peer, team, at)
                g = gate_acc[at, cols] + dot(rows, gate[peer_depth, cols])
                u = up_acc[at, cols] + dot(rows, up[peer_depth, cols])
                act_ref[at, cols] = swiglu(g, u)
            return carry

        lax.fori_loop(0, hidden // GATE_BLOCK, body, 0)

    def whole_depth(team):
        def body(i, carry):
            cols = pl.ds(pl.multiple_of(i * GATE_BLOCK, GATE_BLOCK), GATE_BLOCK)
            for at in blocks_of(team):
                mine = rows_of(recv_own, team, at)
                theirs = rows_of(recv_peer, team, at)
                g = dot(mine, gate[own_depth, cols]) + dot(theirs, gate[peer_depth, cols])
                u = dot(mine, up[own_depth, cols]) + dot(theirs, up[peer_depth, cols])
                act_ref[at, cols] = swiglu(g, u)
            return carry

        lax.fori_loop(0, hidden // GATE_BLOCK, body, 0)

    tiles = half // COL_BLOCK
    all_tiles = pl.ds(0, tiles)
    one_tile = [pl.ds(t, 1) for t in range(tiles)]
    backs = half // BACK_BLOCK
    all_backs = pl.ds(0, backs)
    one_back = [pl.ds(b, 1) for b in range(backs)]
    some_backs = [pl.ds(t * backs // tiles, backs // tiles) for t in range(tiles)]

    def down_copy(p, at):
        team = teams[p]
        ks = pl.ds(team[0], len(team))
        slot = p + at.start // at.size + (tiles - 1 if p == 2 else 0)
        return pltpu.make_async_remote_copy(
            src_ref=down_send.at[at, ks],
            dst_ref=down_recv.at[at, ks],
            send_sem=down_send_sem.at[0],
            recv_sem=down_recv_sem.at[slot],
            device_id=(ep, other),
            device_id_type=MESH,
        )

    def down_tile(ref, p, side, t):
        team = teams[p]
        cols = pl.ds(pl.multiple_of(side * half + t * COL_BLOCK, COL_BLOCK), COL_BLOCK)
        for at in blocks_of(team):
            value = dot(act_ref[at, :], down[:, cols]).astype(BF16)
            size = at.stop - at.start
            if size <= group:
                k, begin = team[0] + at.start // group, at.start % group
                ref[t, k, begin : begin + size, :] = value
            else:
                k = team[0] + at.start // group
                ref[t, k : k + size // group] = value.reshape(size // group, group, COL_BLOCK)

    def down_other(p, parts):
        for at in parts:
            for t in range(at.start, at.start + at.size):
                down_tile(down_send, p, other, t)
            down_copy(p, at).start()

    def back_slot(k, at):
        base = (0, 1, 1 + tiles, 1 + tiles + backs)[k]
        return base + at.start // at.size

    def back_copy(k, at, j):
        return beside_copy(
            lambda to: back_send.at[k, to, at],
            lambda giver: back_recv.at[k, giver, at],
            back_send_sem.at[0],
            back_recv_sem.at[back_slot(k, at)],
            j,
        )

    def back_keep(k, at):
        return pltpu.make_async_copy(
            back_send.at[k, spot, at],
            back_recv.at[k, spot, at],
            load_sem.at[planes + back_slot(k, at)],
        )

    def send_back(k, at):
        for j in range(1, plane):
            back_copy(k, at, j).start()
        back_keep(k, at).start()

    def down_join(p, t):
        for k in teams[p]:
            total = (down_own[t, k].astype(F32) + down_recv[t, k].astype(F32)).astype(BF16)
            for i in range(COL_BLOCK // BACK_BLOCK):
                piece = total[:, i * BACK_BLOCK : (i + 1) * BACK_BLOCK]
                at = t * (COL_BLOCK // BACK_BLOCK) + i
                back_send[k, :, at] = piece.reshape(plane, cap, BACK_BLOCK)

    def down_mine(p):
        for t in range(tiles):
            down_tile(down_own, p, tp, t)

    def join_whole(p):
        down_copy(p, all_tiles).wait_recv()
        for t in range(tiles):
            down_join(p, t)
        for k in teams[p]:
            send_back(k, all_backs)

    def join_tiles(p):
        for t in range(tiles):
            down_tile(down_own, p, tp, t)
            down_copy(p, one_tile[t]).wait_recv()
            down_join(p, t)
            for b in range(t * backs // tiles, (t + 1) * backs // tiles):
                send_back(teams[p][-1], one_back[b])
        for k in reversed(teams[p][:-1]):
            for b in range(backs):
                send_back(k, one_back[b])

    def sum_copy(k, t):
        to = partners[k]
        return pltpu.make_async_remote_copy(
            src_ref=sum_send.at[to, t],
            dst_ref=sum_recv.at[level, t],
            send_sem=sum_send_sem.at[0],
            recv_sem=sum_recv_sem.at[0],
            device_id=(to * plane + spot, tp),
            device_id_type=MESH,
        )

    def combine(k, at):
        back_keep(k, at).wait()
        arrived = back_recv.at[k, pl.ds(0, plane - 1), at]
        tally(arrived, back_recv_sem.at[back_slot(k, at)]).wait_recv()
        to = partners[k]
        mixes = []
        for t in range(at.start, at.start + at.size):
            back = back_recv[k, :, t].reshape(group, BACK_BLOCK)
            mixes.append(dot(mixing[k].astype(BF16), jnp.concatenate([back, back], axis=0)))
        for t, mixed in zip(range(at.start, at.start + at.size), mixes):
            cols = slice(t * BACK_BLOCK, (t + 1) * BACK_BLOCK)
            if k == 0:
                total_ref[:, cols] = res_ref[:, cols].astype(F32) + mixed
            else:
                sum_send[to, t] = mixed.astype(BF16)
        if k > 0:
            for t in range(at.start, at.start + at.size):
                sum_copy(k, t).start()

    def run_far():
        whole_depth(teams[2])
        down_other(2, one_tile)
        join_tiles(2)

    place_rows(0)
    if planes > 1:
        receive_rows(1)

        @pl.when(inner == 1)
        def _():
            for c in range(CHUNKS):
                relay_copy(c).start()

        place_rows(1)
    gather(0)
    if planes > 1:
        receive_rows(2)
        place_rows(2)
    for i in (11, 12, 13):
        loads[i].wait()
    first_half(teams[0])
    fwd_copy(0).wait_recv()
    second_half(teams[0])
    down_other(0, [all_tiles])
    if planes > 1:
        receive_rows(3)
        place_rows(3)
    down_mine(0)
    join_whole(0)
    if planes > 1:
        gather(1)
        first_half(teams[1])
        fwd_copy(1).wait_recv()
        second_half(teams[1])
        gather(2)
        down_other(1, one_tile)
        gather(3)
        down_mine(1)
        for t in range(tiles):
            down_copy(1, one_tile[t]).wait_recv()
            down_join(1, t)
            send_back(1, some_backs[t])
        fwd_copy(2).wait_recv()
        fwd_copy(3).wait_recv()
        run_far()
        tally(route_recv.at[pl.ds(0, planes - 1)], route_send_sem.at[0]).wait_send()

        @pl.when(inner == 1)
        def _():
            tally(rows_recv, rows_send_sem.at[0]).wait_send()

        @pl.when(inner == 0)
        def _():
            tally(rows_recv.at[pl.ds(0, 2)], rows_send_sem.at[0]).wait_send()

    tally(disp.at[:, pl.ds(0, plane - 1)], disp_send_sem.at[0]).wait_send()
    tally(recv_own, fwd_send_sem.at[0]).wait_send()
    tally(down_send, down_send_sem.at[0]).wait_send()
    if planes > 1:
        for at in some_backs:
            combine(1, at)
    combine(0, all_backs)
    if planes > 1:
        for k in (3, 2):
            for b in range(backs):
                combine(k, one_back[b])
    tally(back_send.at[:, pl.ds(0, plane - 1)], back_send_sem.at[0]).wait_send()
    if planes > 1:
        tally(sum_recv.at[pl.ds(0, planes - 1)], sum_recv_sem.at[0]).wait_recv()
    for t in range(backs):
        cols = slice(t * BACK_BLOCK, (t + 1) * BACK_BLOCK)
        total = total_ref[:, cols]
        for k in range(1, planes):
            total = total + sum_recv[partners[k], t].astype(F32)
        out_ref[:, cols] = total.astype(BF16)

    if planes > 1:
        tally(sum_send.at[pl.ds(0, planes - 1)], sum_send_sem.at[0]).wait_send()


def publish(*refs):
    sems = refs[-1]
    count = len(refs) // 2
    copies = []
    for i in range(count):
        copy = pltpu.make_async_copy(refs[i], refs[count + i], sems.at[i])
        copy.start()
        copies.append(copy)
    for copy in copies:
        copy.wait()


def local(
    tokens,
    norm1_gain,
    w_query,
    w_key,
    w_value,
    head_bias,
    key_cache,
    value_cache,
    seq_lengths,
    w_out,
    norm2_gain,
    route_ids,
    route_logits,
    expert_gate,
    expert_up,
    expert_down,
):
    n = lax.axis_size("ep")
    seqs, half = tokens.shape
    top = route_ids.shape[1]
    experts = n * expert_gate.shape[0]
    capacity = max(2, 2 * seqs * top // experts)
    cap = -(-capacity // 16) * 16
    planes = 4 if n % 4 == 0 else 1
    plane = n // planes
    qc = w_query.shape[1] // 2
    kcols = w_key.shape[1] // 2
    groups = qc // HEAD
    positions = key_cache.shape[1]
    hidden = expert_gate.shape[2]
    tiles = half // COL_BLOCK
    backs = half // BACK_BLOCK
    most = plane * cap * (2 if planes == 4 else 1)
    keys = jnp.swapaxes(key_cache, 1, 2)
    values = jnp.swapaxes(value_cache, 1, 2)
    operands = (
        tokens,
        norm1_gain.reshape(1, -1),
        w_query,
        w_key,
        w_value,
        head_bias,
        keys,
        values,
        seq_lengths,
        w_out,
        norm2_gain.reshape(1, -1),
        route_ids.T,
        route_logits.T,
        expert_gate.reshape(expert_gate.shape[1:]),
        expert_up.reshape(expert_up.shape[1:]),
        expert_down.reshape(expert_down.shape[1:]),
    )
    in_smem = (5, 8)
    in_specs = [
        pl.BlockSpec(memory_space=pl.ANY) for i in range(len(operands))
    ]
    vmem = pl.BlockSpec(memory_space=pltpu.VMEM)
    loaded = [
        pltpu.VMEM(a.shape, a.dtype) for i, a in enumerate(operands) if i not in in_smem
    ]
    dma = pltpu.SemaphoreType.DMA
    scratch = (
        [pltpu.SMEM(operands[i].shape, operands[i].dtype) for i in in_smem]
        + [loaded[0], loaded[0]]
        + loaded[1:]
        + [
            pltpu.VMEM((seqs + PAD, qc + 2 * kcols + 2 * LANES), F32),
            pltpu.VMEM((seqs + PAD, qc + 2 * kcols + 2 * LANES), F32),
            pltpu.VMEM((seqs, groups, HEAD), F32),
            pltpu.VMEM((seqs * groups, BATCH * HEAD), BF16),
            pltpu.VMEM((seqs * groups, positions), F32),
            pltpu.VMEM((seqs * groups, positions), BF16),
            pltpu.VMEM((seqs, groups, HEAD), F32),
            pltpu.VMEM((CHUNKS, 2, seqs // CHUNKS, half), BF16),
            pltpu.VMEM((CHUNKS, 2, seqs // CHUNKS, half), BF16),
            pltpu.VMEM((seqs, half), BF16),
            pltpu.VMEM((2 * top, seqs), F32),
            pltpu.VMEM((planes, 2 * top, seqs), F32),
            pltpu.VMEM((planes, plane * cap, seqs), BF16),
            pltpu.VMEM((planes, seqs, 2 * plane * cap), F32),
            pltpu.VMEM((CHUNKS, seqs // CHUNKS, half), BF16),
            pltpu.VMEM((planes, CHUNKS, seqs // CHUNKS, half), BF16),
            pltpu.VMEM((planes, plane, cap, half), BF16),
            pltpu.VMEM((planes, plane, cap, half), BF16),
            pltpu.VMEM((planes, plane, cap, half), BF16),
            pltpu.VMEM((most, hidden), F32),
            pltpu.VMEM((most, hidden), F32),
            pltpu.VMEM((most, hidden), BF16),
            pltpu.VMEM((tiles, planes, plane * cap, COL_BLOCK), BF16),
            pltpu.VMEM((tiles, planes, plane * cap, COL_BLOCK), BF16),
            pltpu.VMEM((tiles, planes, plane * cap, COL_BLOCK), BF16),
            pltpu.VMEM((planes, plane, backs, cap, BACK_BLOCK), BF16),
            pltpu.VMEM((planes, plane, backs, cap, BACK_BLOCK), BF16),
            pltpu.VMEM((planes, backs, seqs, BACK_BLOCK), BF16),
            pltpu.VMEM((planes, backs, seqs, BACK_BLOCK), BF16),
            pltpu.VMEM((seqs, half), F32),
            dma((planes + 1 + tiles + 2 * backs,)),
            dma((2,)),
            dma((2 + CHUNKS,)),
            dma((1,)),
            dma((1,)),
            dma((1,)),
            dma((planes,)),
            dma((1,)),
            dma((1,)),
            dma((1,)),
            dma((planes,)),
            dma((1,)),
            dma((planes,)),
            dma((1,)),
            dma((1 + 2 * tiles,)),
            dma((1,)),
            dma((1 + tiles + 2 * backs,)),
        ]
    )
    shapes = ((seqs, half), (seqs, kcols), (seqs, kcols))
    results = pl.pallas_call(
        functools.partial(kernel, n, cap),
        out_shape=tuple(pltpu.VMEM(shape, BF16) for shape in shapes),
        in_specs=in_specs,
        out_specs=(vmem, vmem, vmem),
        scratch_shapes=scratch,
        compiler_params=pltpu.CompilerParams(
            collective_id=0, has_side_effects=True, vmem_limit_bytes=VMEM_BYTES
        ),
    )(*operands)
    return pl.pallas_call(
        publish,
        out_shape=tuple(jax.ShapeDtypeStruct(shape, BF16) for shape in shapes),
        in_specs=[vmem] * len(shapes),
        out_specs=tuple([pl.BlockSpec(memory_space=pl.ANY)] * len(shapes)),
        scratch_shapes=[dma((len(shapes),))],
    )(*(pltpu.with_memory_space_constraint(r, pltpu.VMEM) for r in results))


def solution(mesh):
    in_specs = (
        P("ep", "tp"),
        P("tp"),
        P("tp", None),
        P("tp", None),
        P("tp", None),
        P("tp"),
        P("ep", None, "tp"),
        P("ep", None, "tp"),
        P("ep"),
        P("tp", None),
        P("tp"),
        P("ep", None),
        P("ep", None),
        P("ep", None, "tp"),
        P("ep", None, "tp"),
        P("ep", "tp", None),
    )
    out_specs = (P("ep", "tp"), P("ep", "tp"), P("ep", "tp"))
    return jax.shard_map(local, mesh=mesh, in_specs=in_specs, out_specs=out_specs, check_vma=False)
```
